512 devices in a mesh: rep: 2 (over z_hi), fs: 32 (over z_lo, y), tp: 8 (over x, core).
Axes of the slice: x: 4, y: 4, z: 16 (z_hi: 2, z_lo: 8; z = z_hi * 8 + z_lo), core: 2. Of those that a mesh axis runs over, the one named last changes fastest.
Arguments:
- tokens: bfloat16 [32768, 2048], P(('rep', 'fs')), may hold values from -6 to 6
- gate_outer: bfloat16 [2048, 1024], P('fs', 'tp'), may hold values from -0.125 to 0.125
- gate_inner: bfloat16 [2048, 1024], P('fs', 'tp'), may hold values from -0.125 to 0.125
- conv_input: bfloat16 [2048, 1024], P('fs', 'tp'), may hold values from -0.125 to 0.125
- mixer_output: bfloat16 [2048, 1024], P('fs', 'tp'), may hold values from -0.1875 to 0.1875
- conv_taps: float32 [3, 1024], P(None, 'tp'), may hold values from -3 to 3
- mixer_gain: float32 [2048], replicated, may hold values from 0.1 to 1.9
- mixer_shift: float32 [2048], replicated, may hold values from -3 to 3
- up_weight: bfloat16 [2048, 8192], P('fs', 'tp'), may hold values from -0.125 to 0.125
- down_weight: bfloat16 [2048, 8192], P('fs', 'tp'), may hold values from -0.0625 to 0.0625
- channel_gain: float32 [2048], replicated, may hold values from 0.1 to 1.9
- channel_shift: float32 [2048], replicated, may hold values from -3 to 3
Outputs:
- mixed: bfloat16 [32768, 2048], P(('rep', 'fs'))
The draws below stay inside these ranges and needn't reach their ends.
All inputs are finite; a program needn't handle non-finite values.
Results may differ from the reference program's by a relative error of at most 0.014.
Values may be sent and summed in bfloat16 or wider, within the bound.
A program may use at most 64 MiB of HBM per device.

```python
import jax
import jax.numpy as jnp
from jax import lax

D = 2048
C = 1024
FF = 8192
TAPS = 3
LEN = 512
SEQS = 64
TOKENS = 32768
N_TP = 8


def levels(rng, dims, shards, least, top_value):
    loudness = 1.0
    for axis_at, parts in shards:
        steps = jax.random.uniform(jax.random.fold_in(jax.random.fold_in(rng, 6), axis_at), (parts,), jnp.float32, least / len(shards), top_value / len(shards))
        loudness = loudness * jnp.repeat(jnp.exp(steps), dims[axis_at] // parts).reshape((-1,) + (1,) * (len(dims) - 1 - axis_at))
    return loudness


def bell_draw(own_key, dims, deviation, most, pieces=(), dtype=jnp.bfloat16):
    drawn = jax.random.normal(own_key, dims, jnp.float32) * deviation
    if len(pieces) > 0:
        drawn = levels(own_key, dims, pieces, -0.22, 0.18) * drawn
    return jnp.clip(drawn, min=-most, max=most).astype(dtype)


def setup_inputs(seed: int = 0) -> dict:
    arg_keys = jax.random.split(jax.random.key(seed), 13)
    return {
        "tokens": bell_draw(arg_keys[0], (TOKENS, D), 1.0, 6.0, ((0, 64),)),
        "gate_outer": bell_draw(arg_keys[1], (D, C), D ** -0.5, 0.125, ((0, 32), (1, 8))),
        "gate_inner": bell_draw(arg_keys[2], (D, C), D ** -0.5, 0.125, ((0, 32), (1, 8))),
        "conv_input": bell_draw(arg_keys[3], (D, C), D ** -0.5, 0.125, ((0, 32), (1, 8))),
        "mixer_output": bell_draw(arg_keys[4], (D, C), C ** -0.5, 0.1875, ((0, 32), (1, 8))),
        "conv_taps": bell_draw(arg_keys[5], (TAPS, C), 0.6, 3.0, ((1, 8),), jnp.float32),
        "mixer_gain": jnp.clip(1.0 + 0.18 * jax.random.normal(arg_keys[6], (D,), jnp.float32), 0.1, 1.9),
        "mixer_shift": bell_draw(arg_keys[7], (D,), 0.5, 3.0, (), jnp.float32),
        "up_weight": bell_draw(arg_keys[8], (D, FF), D ** -0.5, 0.125, ((0, 32), (1, 8))),
        "down_weight": bell_draw(arg_keys[9], (D, FF), FF ** -0.5, 0.0625, ((0, 32), (1, 8))),
        "channel_gain": jnp.clip(1.0 + 0.18 * jax.random.normal(arg_keys[10], (D,), jnp.float32), 0.1, 1.9),
        "channel_shift": bell_draw(arg_keys[11], (D,), 0.5, 3.0, (), jnp.float32),
    }


residual_scale = 8.0 ** 0.25
norm_epsilon = 1e-05

def layer_norm(values, gain, shift):
    row_mean = lax.optimization_barrier(jnp.mean(values, -1, keepdims=True))
    centered = values - row_mean
    variance = lax.optimization_barrier(jnp.mean(centered * centered, -1, keepdims=True))
    return centered * lax.rsqrt(variance + norm_epsilon) * gain + shift

def blockwise_sum(left, right_t):
    block_width = left.shape[1] // N_TP
    totals = jnp.zeros((left.shape[0], right_t.shape[0]), jnp.float32)
    for block_index in range(N_TP):
        lower = block_index * block_width
        product = lax.dot_general(left[:, lower:lower + block_width], right_t[:, lower:lower + block_width], (((1,), (1,)), ((), ())), preferred_element_type=jnp.float32)
        totals = totals + lax.optimization_barrier(product.astype(jnp.bfloat16)).astype(jnp.float32)
    return totals

def reference(tokens, gate_outer, gate_inner, conv_input, mixer_output, conv_taps, mixer_gain, mixer_shift, up_weight, down_weight, channel_gain, channel_shift):

    def one_sequence(seq_rows):
        outer_gate = jnp.dot(seq_rows, gate_outer, preferred_element_type=jnp.float32)
        inner_gate = jnp.dot(seq_rows, gate_inner, preferred_element_type=jnp.float32)
        conv_values = jnp.dot(seq_rows, conv_input, preferred_element_type=jnp.float32)
        product = inner_gate * conv_values
        padded = jnp.pad(product, ((TAPS - 1, 0), (0, 0)))
        result = jnp.zeros_like(product)
        for tap_index in range(TAPS):
            result = result + conv_taps[tap_index] * padded[tap_index:tap_index + LEN]
        conv_out = (outer_gate * result).astype(jnp.bfloat16)
        mixer_sum = blockwise_sum(conv_out, mixer_output)
        first = layer_norm(residual_scale * seq_rows.astype(jnp.float32) + mixer_sum, mixer_gain, mixer_shift).astype(jnp.bfloat16)
        up_product = jnp.dot(first, up_weight, preferred_element_type=jnp.float32)
        hidden = jnp.square(jax.nn.relu(up_product)).astype(jnp.bfloat16)
        channel_sum = blockwise_sum(hidden, down_weight)
        return layer_norm(residual_scale * first.astype(jnp.float32) + channel_sum, channel_gain, channel_shift).astype(jnp.bfloat16)
    sequences = tokens.reshape(SEQS, LEN, D)
    outputs = lax.map(one_sequence, sequences)
    return outputs.reshape(TOKENS, D)
```

```python
import functools

import jax
import jax.numpy as jnp
from jax import lax
from jax.experimental import pallas as pl
from jax.experimental.pallas import tpu as pltpu
from jax.sharding import PartitionSpec as P

residual_scale = 8.0**0.25
norm_epsilon = 1e-05

NZ, NY, NX = 8, 4, 4
SEQ, WIDTH = 512, 2048
ROWS = 64
GROUP = 256
CHUNKS, CHUNK = 8, 256
ARRIVAL = (0, 1, -1, 2, -2, 3, -3, 4)

LINK_RATE, LINK_LAT = 46.6e3, 1.9
PAIR_RATE, PAIR_LAT = 500e3, 1.1
BACKLOG = 1.0


class Op:
    def __init__(self, name, deps, emit, prio, dur=0.0, link=None, nbytes=0, wait=None, latency=0.0):
        self.name, self.deps, self.emit, self.prio = name, deps, emit, prio
        self.dur, self.link, self.nbytes, self.wait = dur, link, nbytes, wait
        self.latency = latency


def plan(ops):
    done, link_free, order, now = {}, {}, [], 0.0
    left = list(ops)
    while left:
        best = None
        for at, op in enumerate(left):
            if any(d not in done for d in op.deps):
                continue
            ready = max([done[d] for d in op.deps], default=0.0)
            if op.link is not None:
                ready = max(ready, link_free.get(op.link, 0.0) - BACKLOG)
            key = (max(ready, now), op.prio, at)
            if best is None or key < best[0]:
                best = (key, op)
        (start, _, _), op = best
        left.remove(op)
        now = start + (op.dur if op.link is None else 0.02)
        if op.link is None:
            done[op.name] = now + op.latency
        else:
            rate, lat = (PAIR_RATE, PAIR_LAT) if op.link == "c" else (LINK_RATE, LINK_LAT)
            begin = max(now, link_free.get(op.link, 0.0))
            link_free[op.link] = begin + op.nbytes / rate
            done[op.name] = link_free[op.link] + lat
        order.append((start, op))
    return order, done


def layer_kernel(
    tok_hbm, go_hbm, gi_hbm, ci_hbm, mo_hbm, up_hbm, dn_hbm, taps, mgain, mshift, cgain, cshift,
    out_hbm,
    tok, wm, wu, wd, proj, prod, conv, ps, so, dr, rl, fr, fd, v, first, hid, res,
    send_sems, recv_sems, load_sems, store_sems,
    report=None,
):
    f32, bf16 = jnp.float32, jnp.bfloat16
    rep, fs, tp = lax.axis_index("rep"), lax.axis_index("fs"), lax.axis_index("tp")
    zl, y = lax.div(fs, NY), lax.rem(fs, NY)
    x, c = lax.div(tp, 2), lax.rem(tp, 2)
    z = rep * NZ + zl

    def mod(v, n):
        return lax.rem(v + 2 * n, n)

    def device(dz=0, dy=0, dx=0, dc=0):
        zz = mod(z + dz, 2 * NZ)
        return (
            lax.div(zz, NZ),
            lax.rem(zz, NZ) * NY + mod(y + dy, NY),
            mod(x + dx, NX) * 2 + lax.rem(c + dc, 2),
        )

    peer = {
        "z+": device(dz=1), "z-": device(dz=-1), "y+": device(dy=1), "y-": device(dy=-1),
        "x+": device(dx=1), "x-": device(dx=-1), "c": device(dc=1),
    }
    sign = {"+": 1, "-": -1}

    ops = []
    sends = []

    def send(name, link, deps, src, dst, landed, nbytes, prio):
        index = len(sends)

        def copy(s, d):
            return pltpu.make_async_remote_copy(
                src_ref=s, dst_ref=d, send_sem=send_sems.at[index], recv_sem=recv_sems.at[index],
                device_id=peer[link], device_id_type=pl.DeviceIdType.MESH,
            )

        sends.append((name, lambda: copy(src(), dst()).wait_send()))
        ops.append(Op(
            name, deps, lambda: copy(src(), dst()).start(), prio, link=link, nbytes=nbytes,
            wait=lambda: copy(landed(), landed()).wait_recv(),
        ))

    def compute(name, deps, emit, prio, dur):
        ops.append(Op(name, deps, emit, prio, dur=dur))

    loads = []

    def load(name, src, dst):
        index = len(loads)
        op = Op(name, [], lambda: None, 0, latency=0.5)
        op.wait = lambda: pltpu.make_async_copy(src(), dst(), load_sems.at[index]).wait()
        loads.append(lambda: pltpu.make_async_copy(src(), dst(), load_sems.at[index]).start())
        ops.append(op)

    def own(w, c0, n):
        return lambda: w.at[zl, pl.ds(pl.multiple_of(y * ROWS, ROWS), ROWS), pl.ds(c0, n)]

    load("load.m0", lambda: go_hbm, own(wm, 0, 128))
    load("load.m1", lambda: gi_hbm, own(wm, 128, 128))
    load("load.m2", lambda: ci_hbm, own(wm, 256, 128))
    load("load.m3", lambda: mo_hbm, own(wm, 384, 128))
    load("load.u", lambda: up_hbm, own(wu, 0, 1024))
    load("load.d", lambda: dn_hbm, own(wd, 0, 1024))
    load("load.t", lambda: tok_hbm, lambda: tok)

    def block(w, dz, dy, c0, n, half=None):
        rows, off = (ROWS, 0) if half is None else (ROWS // 2, half * ROWS // 2)

        def view():
            start = pl.multiple_of(mod(y + dy, NY) * ROWS + off, ROWS // 2)
            return w.at[mod(zl + dz, NZ), pl.ds(start, rows), pl.ds(c0, n)]

        return view

    def slab(w, dz, c0, n, half=None):
        rows, off = (GROUP, 0) if half is None else (GROUP // 2, half * GROUP // 2)
        return lambda: w.at[mod(zl + dz, NZ), pl.ds(off, rows), pl.ds(c0, n)]

    ready = {}

    def y_first(tag, w, c0, n, deps, prio):
        size = ROWS * n * 2
        for d in "+-":
            s = sign[d]
            b = block(w, 0, 0, c0, n)
            send(f"{tag}.Y1{d}", "y" + d, deps, b, b, block(w, 0, -s, c0, n), size, prio)
        for d, half in (("+", 0), ("-", 1)):
            s = sign[d]
            b = block(w, 0, -s, c0, n, half)
            send(f"{tag}.Y2{d}", "y" + d, [f"{tag}.Y1{d}"], b, b, block(w, 0, -2 * s, c0, n, half), size // 2, prio)
        group = [f"{tag}.Y{h}{d}" for h in (1, 2) for d in "+-"]
        ready[tag[0], 0] = ready.get((tag[0], 0), []) + group
        for d, half in (("+", 0), ("-", 1)):
            s = sign[d]
            for h in (1, 2, 3, 4):
                part = half if h == 4 else None
                b = slab(w, -s * (h - 1), c0, n, part)
                before = deps + group if h == 1 else [f"{tag}.Z{h - 1}{d}"]
                send(f"{tag}.Z{h}{d}", "z" + d, before, b, b, slab(w, -s * h, c0, n, part),
                     NY * size // (1 if part is None else 2), prio)
                dist = 4 if h == 4 else -s * h
                ready[tag[0], dist] = ready.get((tag[0], dist), []) + [f"{tag}.Z{h}{d}"]

    def z_first(tag, w, c0, n, deps, prio):
        size = ROWS * n * 2
        for d, half in (("+", 0), ("-", 1)):
            s = sign[d]
            for h in (1, 2, 3, 4):
                part = half if h == 4 else None
                b = block(w, -s * (h - 1), 0, c0, n, part)
                before = deps if h == 1 else [f"{tag}.Z{h - 1}{d}"]
                send(f"{tag}.Z{h}{d}", "z" + d, before, b, b, block(w, -s * h, 0, c0, n, part),
                     size // (1 if part is None else 2), prio)
        for dist in ARRIVAL:
            here = {0: deps, 4: [f"{tag}.Z4+", f"{tag}.Z4-"]}.get(
                dist, [f"{tag}.Z{abs(dist)}{'-' if dist > 0 else '+'}"])
            for d, half in (("+", 0), ("-", 1)):
                s = sign[d]
                b = block(w, dist, 0, c0, n)
                send(f"{tag}.Y1{d}{dist}", "y" + d, here, b, b, block(w, dist, -s, c0, n), size, prio)
                b = block(w, dist, -s, c0, n, half)
                send(f"{tag}.Y2{d}{dist}", "y" + d, [f"{tag}.Y1{d}{dist}"], b, b,
                     block(w, dist, -2 * s, c0, n, half), size // 2, prio)
            names = here + [f"{tag}.Y{h}{d}{dist}" for h in (1, 2) for d in "+-"]
            ready[tag[0], dist] = ready.get((tag[0], dist), []) + names

    mixer_loads = ["load.m0", "load.m1", "load.m2", "load.m3"]
    y_first("my", wm, 0, 256, ["load.m0", "load.m1"], 1)
    z_first("mz", wm, 256, 256, ["load.m2", "load.m3"], 1)
    y_first("uy", wu, 0, 384, ["load.u"], 3)
    z_first("uz", wu, 384, 640, ["load.u"], 3)
    y_first("dy", wd, 0, 384, ["load.d"], 5)
    z_first("dz", wd, 384, 640, ["load.d"], 5)

    def project():
        def step(i, _):
            rows = pl.ds(pl.multiple_of(i * 128, 128), 128)
            proj[rows, :] = jnp.dot(
                tok[rows, :], wm[:, :, 0:384].reshape(WIDTH, 384), preferred_element_type=f32)
            return 0

        lax.fori_loop(0, SEQ // 128, step, 0)
        prod[0:8, :] = jnp.zeros((8, 128), f32)
        prod[8:, :] = proj[:, 128:256] * proj[:, 256:384]
        total = taps[0:1, :] * prod[6:6 + SEQ, :]
        total = total + taps[1:2, :] * prod[7:7 + SEQ, :]
        total = total + taps[2:3, :] * prod[8:8 + SEQ, :]
        conv[...] = (proj[:, 0:128] * total).astype(bf16)

    mixer_ready = [n for dist in ARRIVAL for n in ready["m", dist]]
    compute("project", ["load.t"] + mixer_loads + mixer_ready, project, 0, 3.0)

    half_rows = lambda which: pl.ds(pl.multiple_of(which * GROUP, GROUP), GROUP)
    nt = (((1,), (1,)), ((), ()))

    def product(phase, k, left, right):
        weight = right()
        ps[phase, k] = lax.dot_general(
            left[half_rows(1 - c), :], weight, nt, preferred_element_type=f32).astype(bf16)
        so[phase, k] = lax.dot_general(
            left[half_rows(c), :], weight, nt, preferred_element_type=f32).astype(bf16)

    def rows_of(dx):
        return pl.ds(pl.multiple_of(mod(x + dx, NX) * ROWS, ROWS), ROWS)

    def own_rows():
        return pl.ds(pl.multiple_of((c * NX + x) * ROWS, ROWS), ROWS)

    def sum_chunk(phase, k, column, residual, prio):
        t = f"s{phase}.{k}"
        d, e = ("+", "-") if k % 2 == 0 else ("-", "+")
        s = sign[d]
        send(f"{t}.pair", "c", [f"{t}.product"], lambda: ps.at[phase, k], lambda: dr.at[phase, k],
             lambda: dr.at[phase, k], GROUP * CHUNK * 2, prio)

        def add_pair():
            so[phase, k] = (so[phase, k].astype(f32) + dr[phase, k].astype(f32)).astype(bf16)

        compute(f"{t}.add", [f"{t}.product", f"{t}.pair"], add_pair, prio, 0.15)
        size = ROWS * CHUNK * 2
        at = lambda dx: (lambda: so.at[phase, k, rows_of(dx), :])
        slot = lambda ref: (lambda: ref.at[phase, k])
        send(f"{t}.relay", "x" + d, [f"{t}.add"], at(2), slot(rl), slot(rl), size, prio)
        send(f"{t}.direct", "x" + e, [f"{t}.add"], at(-s), slot(fd), slot(fd), size, prio)

        def add_relay():
            so[phase, k, rows_of(s), :] = (
                so[phase, k, rows_of(s), :].astype(f32) + rl[phase, k].astype(f32)).astype(bf16)

        compute(f"{t}.radd", [f"{t}.add", f"{t}.relay"], add_relay, prio, 0.05)
        send(f"{t}.final", "x" + d, [f"{t}.radd"], at(s), slot(fr), slot(fr), size, prio)

        def finish():
            columns = pl.ds(pl.multiple_of(column() * CHUNK, CHUNK), CHUNK)
            total = so[phase, k, rows_of(0), :].astype(f32) + fr[phase, k].astype(f32)
            total = total + fd[phase, k].astype(f32)
            v[:, columns] = residual_scale * residual[own_rows(), columns].astype(f32) + total

        compute(f"{t}.finish", [f"{t}.add", f"{t}.final", f"{t}.direct"], finish, prio, 0.05)

    def norm(phase, gain, shift, dest):
        def emit():
            values = v[...]
            mean = jnp.mean(values, -1, keepdims=True)
            centered = values - mean
            variance = jnp.mean(centered * centered, -1, keepdims=True)
            scaled = centered * lax.rsqrt(variance + norm_epsilon)
            dest[own_rows(), :] = (scaled * gain[...] + shift[...]).astype(bf16)

        compute(f"norm{phase}", [f"s{phase}.{k}.finish" for k in range(CHUNKS)], emit, 0, 0.7)

    HALF = WIDTH // 2

    def gather(phase, ref):
        def at(dx, h, other=False):
            def view():
                core = 1 - c if other else c
                rows = pl.ds(pl.multiple_of((core * NX + mod(x + dx, NX)) * ROWS, ROWS), ROWS)
                return ref.at[rows, :] if h is None else ref.at[rows, pl.ds(h * HALF, HALF)]
            return view

        t, size, landed = f"g{phase}", ROWS * HALF * 2, []
        start = [f"norm{phase}"]
        for d, first_half in (("+", 0), ("-", 1)):
            for h in (first_half, 1 - first_half):
                send(f"{t}.A{d}{h}", "x" + d, start, at(0, h), at(0, h), at(-sign[d], h), size, 0)
                landed.append((f"{t}.A{d}{h}", at(-sign[d], h)))
        send(f"{t}.P", "c", start, at(0, None), at(0, None), at(0, None, True), 2 * size, 0)
        landed.append((f"{t}.P", at(0, None, True)))
        for d, h in (("+", 0), ("-", 1)):
            b = at(-sign[d], h)
            send(f"{t}.B{d}", "x" + d, [f"{t}.A{d}{h}"], b, b, at(2, h), size, 0)
            landed.append((f"{t}.B{d}", at(2, h)))
        for name, dx, h in ((f"{t}.A+0", -1, 0), (f"{t}.A-1", 1, 1), (f"{t}.A+1", -1, 1),
                            (f"{t}.A-0", 1, 0), (f"{t}.B+", 2, 0), (f"{t}.B-", 2, 1)):
            send(f"{name}.P", "c", [name], at(dx, h), at(dx, h), at(dx, h, True), size, 0)
            landed.append((f"{name}.P", at(dx, h, True)))
        return landed, at(0, None)

    for k in range(CHUNKS):
        compute(f"s0.{k}.product", ["project"],
                functools.partial(product, 0, k, conv, lambda k=k: wm[k, :, 384:512]), 1, 0.25)
        sum_chunk(0, k, lambda k=k: k, tok, 0)
    norm(0, mgain, mshift, first)
    landed0, _ = gather(0, first)

    def hidden(n):
        columns = pl.ds(n * 256, 256)
        for r in range(2):
            rows = pl.ds(r * 256, 256)
            up = jnp.dot(first[rows, :], wu[:, :, columns].reshape(WIDTH, 256), preferred_element_type=f32)
            hid[rows, columns] = jnp.square(jnp.maximum(up, 0.0)).astype(bf16)

    up_ready = ["load.u"] + [n for dist in ARRIVAL for n in ready["u", dist]]
    for n in range(4):
        compute(f"hidden{n}", ["norm0"] + [name for name, _ in landed0] + up_ready,
                functools.partial(hidden, n), 2, 1.0)
    for k, dist in enumerate(ARRIVAL):
        group = lambda dist=dist: mod(zl + dist, NZ)
        compute(f"s1.{k}.product", [f"hidden{n}" for n in range(4)] + ["load.d"] + ready["d", dist],
                functools.partial(product, 1, k, hid, lambda group=group: wd[group()]), 1, 0.6)
        sum_chunk(1, k, group, first, 0)
    norm(1, cgain, cshift, res)
    landed1, mine = gather(1, res)

    stores = []

    def store(name, deps, view):
        index = len(stores)

        def copy():
            source = view()
            return pltpu.make_async_copy(source, out_view(view), store_sems.at[index])

        stores.append(copy)
        ops.append(Op(name, deps, lambda: copy().start(), 2, dur=0.02))

    def out_view(view):
        return view(out_hbm)

    def place(dx, h, other):
        def view(ref=res):
            core = 1 - c if other else c
            rows = pl.ds(pl.multiple_of((core * NX + mod(x + dx, NX)) * ROWS, ROWS), ROWS)
            return ref.at[rows, :] if h is None else ref.at[rows, pl.ds(h * HALF, HALF)]
        return view

    store("out.own", ["norm1"], place(0, None, False))
    store("out.P", ["g1.P"], place(0, None, True))
    for name, dx, h in (("g1.A+0", -1, 0), ("g1.A-1", 1, 1), ("g1.A+1", -1, 1),
                        ("g1.A-0", 1, 0), ("g1.B+", 2, 0), ("g1.B-", 2, 1)):
        store(f"out.{name}", [name], place(dx, h, False))
        store(f"out.{name}.P", [f"{name}.P"], place(dx, h, True))

    order, done = plan(ops)
    if report is not None:
        report(order, done, len(sends), len(loads), len(stores))

    for start_load in loads:
        start_load()
    barrier = pltpu.get_barrier_semaphore()
    for link in peer:
        pl.semaphore_signal(barrier, inc=1, device_id=peer[link], device_id_type=pl.DeviceIdType.MESH)
    pl.semaphore_wait(barrier, len(peer))

    by_name = {op.name: op for op in ops}
    waited = set()

    def need(name):
        op = by_name[name]
        if op.wait is not None and name not in waited:
            waited.add(name)
            op.wait()

    for _, op in order:
        for name in op.deps:
            need(name)
        op.emit()
    for op in ops:
        need(op.name)
    for _, wait in sends:
        wait()
    for copy in stores:
        copy().wait()


N_SENDS, N_LOADS, N_STORES = 256, 7, 14


def count_ops():
    return N_SENDS, N_LOADS, N_STORES


def local(tokens, gate_outer, gate_inner, conv_input, mixer_output, conv_taps, mixer_gain,
          mixer_shift, up_weight, down_weight, channel_gain, channel_shift):
    bf16, f32 = jnp.bfloat16, jnp.float32
    vmem, hbm = pl.BlockSpec(memory_space=pltpu.VMEM), pl.BlockSpec(memory_space=pl.ANY)
    return pl.pallas_call(
        layer_kernel,
        out_shape=jax.ShapeDtypeStruct((SEQ, WIDTH), bf16),
        in_specs=[hbm] * 7 + [vmem] * 5,
        out_specs=hbm,
        scratch_shapes=[
            pltpu.VMEM((SEQ, WIDTH), bf16),
            pltpu.VMEM((NZ, GROUP, 512), bf16),
            pltpu.VMEM((NZ, GROUP, 1024), bf16),
            pltpu.VMEM((NZ, GROUP, 1024), bf16),
            pltpu.VMEM((SEQ, 384), f32),
            pltpu.VMEM((SEQ + 8, 128), f32),
            pltpu.VMEM((SEQ, 128), bf16),
            pltpu.VMEM((2, CHUNKS, GROUP, CHUNK), bf16),
            pltpu.VMEM((2, CHUNKS, GROUP, CHUNK), bf16),
            pltpu.VMEM((2, CHUNKS, GROUP, CHUNK), bf16),
            pltpu.VMEM((2, CHUNKS, ROWS, CHUNK), bf16),
            pltpu.VMEM((2, CHUNKS, ROWS, CHUNK), bf16),
            pltpu.VMEM((2, CHUNKS, ROWS, CHUNK), bf16),
            pltpu.VMEM((ROWS, WIDTH), f32),
            pltpu.VMEM((SEQ, WIDTH), bf16),
            pltpu.VMEM((SEQ, 1024), bf16),
            pltpu.VMEM((SEQ, WIDTH), bf16),
            pltpu.SemaphoreType.DMA((N_SENDS,)),
            pltpu.SemaphoreType.DMA((N_SENDS,)),
            pltpu.SemaphoreType.DMA((N_LOADS,)),
            pltpu.SemaphoreType.DMA((N_STORES,)),
        ],
        compiler_params=pltpu.CompilerParams(
            collective_id=0, has_side_effects=True, vmem_limit_bytes=60 * 2**20),
    )(tokens, gate_outer, gate_inner, conv_input, mixer_output, up_weight, down_weight, conv_taps,
      mixer_gain.reshape(1, -1), mixer_shift.reshape(1, -1), channel_gain.reshape(1, -1),
      channel_shift.reshape(1, -1))


def solution(mesh):
    weights = P("fs", "tp")
    in_specs = (
        P(("rep", "fs"), None), weights, weights, weights, weights, P(None, "tp"), P(), P(),
        weights, weights, P(), P(),
    )
    out_specs = P(("rep", "fs"), None)
    return jax.shard_map(local, mesh=mesh, in_specs=in_specs, out_specs=out_specs, check_vma=False)
```

```python
import functools

import jax
import jax.numpy as jnp
from jax import lax
from jax.experimental import pallas as pl
from jax.experimental.pallas import tpu as pltpu
from jax.sharding import PartitionSpec as P

residual_scale = 8.0**0.25
norm_epsilon = 1e-05

NZ, NY, NX = 8, 4, 4
SEQ, WIDTH = 512, 2048
ROWS = 64
GROUP = 256
PARTS = 2
PART = SEQ // PARTS
CORE_ROWS, OWN = PART // 2, PART // 8
CHUNKS, CHUNK = 4, 512
ARRIVAL = (0, 1, -1, 2, -2, 3, -3, 4)

LINK_RATE, LINK_LAT = 46.6e3, 1.9
PAIR_RATE, PAIR_LAT = 500e3, 1.1
BACKLOG = 1.0


PIECES = (
    ("m0", "y", 128, 1), ("m1", "y", 128, 1), ("m2", "z", 256, 1),
    ("u0", "y", 128, 4), ("u1", "y", 256, 4), ("u2", "z", 384, 4), ("u3", "z", 256, 4),
    ("d0", "y", 128, 5), ("d1", "y", 256, 5), ("d2", "z", 384, 5), ("d3", "z", 256, 5),
)
NOT_BEFORE = {4: 0.0, 5: 0.0}


class Op:
    def __init__(self, name, deps, emit, prio, dur=0.0, link=None, nbytes=0, wait=None, latency=0.0):
        self.name, self.deps, self.emit, self.prio = name, deps, emit, prio
        self.dur, self.link, self.nbytes, self.wait = dur, link, nbytes, wait
        self.latency = latency


def plan(ops):
    done, link_free, order, now = {}, {}, [], 0.0
    left = list(ops)
    while left:
        best = None
        for at, op in enumerate(left):
            if any(d not in done for d in op.deps):
                continue
            ready = max([done[d] for d in op.deps], default=NOT_BEFORE.get(op.prio, 0.0))
            ready = max(ready, NOT_BEFORE.get(op.prio, 0.0))
            if op.link is not None:
                ready = max(ready, link_free.get(op.link, 0.0) - (BACKLOG if op.prio >= 3 else 3 * BACKLOG))
            key = (max(ready, now), op.prio, at)
            if best is None or key < best[0]:
                best = (key, op)
        (start, _, _), op = best
        left.remove(op)
        now = start + (op.dur if op.link is None else 0.03)
        if op.link is None:
            done[op.name] = now + op.latency
        else:
            rate, lat = (PAIR_RATE, PAIR_LAT) if op.link == "c" else (LINK_RATE, LINK_LAT)
            begin = max(now, link_free.get(op.link, 0.0))
            link_free[op.link] = begin + op.nbytes / rate
            done[op.name] = link_free[op.link] + lat
        order.append((start, op))
    return order, done


def layer_kernel(
    tok_hbm, go_hbm, gi_hbm, ci_hbm, mo_hbm, up_hbm, dn_hbm, taps, mgain, mshift, cgain, cshift,
    out_hbm,
    tok, wm, wu, wd, proj, prod, conv, pp, so, dr, rl, fr, fd, v, first, hid, res,
    send_sems, recv_sems, load_sems, store_sems,
    report=None,
):
    f32, bf16 = jnp.float32, jnp.bfloat16
    rep, fs, tp = lax.axis_index("rep"), lax.axis_index("fs"), lax.axis_index("tp")
    zl, y = lax.div(fs, NY), lax.rem(fs, NY)
    x, c = lax.div(tp, 2), lax.rem(tp, 2)
    z = rep * NZ + zl

    def mod(v, n):
        return lax.rem(v + 2 * n, n)

    def device(dz=0, dy=0, dx=0, dc=0):
        zz = mod(z + dz, 2 * NZ)
        return (
            lax.div(zz, NZ),
            lax.rem(zz, NZ) * NY + mod(y + dy, NY),
            mod(x + dx, NX) * 2 + lax.rem(c + dc, 2),
        )

    peer = {
        "z+": device(dz=1), "z-": device(dz=-1), "y+": device(dy=1), "y-": device(dy=-1),
        "x+": device(dx=1), "x-": device(dx=-1), "c": device(dc=1),
    }
    sign = {"+": 1, "-": -1}

    ops = []
    sends = []

    def send(name, link, deps, src, dst, landed, nbytes, prio):
        index = len(sends)

        def copy(s, d):
            return pltpu.make_async_remote_copy(
                src_ref=s, dst_ref=d, send_sem=send_sems.at[index], recv_sem=recv_sems.at[index],
                device_id=peer[link], device_id_type=pl.DeviceIdType.MESH,
            )

        sends.append((name, lambda: copy(src(), dst()).wait_send()))
        ops.append(Op(
            name, deps, lambda: copy(src(), dst()).start(), prio, link=link, nbytes=nbytes,
            wait=lambda: copy(landed(), landed()).wait_recv(),
        ))

    def compute(name, deps, emit, prio, dur):
        ops.append(Op(name, deps, emit, prio, dur=dur))

    loads = []

    def load(name, src, dst):
        index = len(loads)
        op = Op(name, [], lambda: None, 0, latency=0.5)
        op.wait = lambda: pltpu.make_async_copy(src(), dst(), load_sems.at[index]).wait()
        loads.append(lambda: pltpu.make_async_copy(src(), dst(), load_sems.at[index]).start())
        ops.append(op)

    def own(w, c0, n):
        return lambda: w.at[zl, pl.ds(pl.multiple_of(y * ROWS, ROWS), ROWS), pl.ds(c0, n)]

    load("load.m0", lambda: go_hbm, own(wm, 0, 128))
    load("load.m1", lambda: gi_hbm, own(wm, 128, 128))
    load("load.m2", lambda: ci_hbm, own(wm, 256, 128))
    load("load.m3", lambda: mo_hbm, own(wm, 384, 128))
    load("load.u", lambda: up_hbm, own(wu, 0, 1024))
    load("load.d", lambda: dn_hbm, own(wd, 0, 1024))
    load("load.t", lambda: tok_hbm, lambda: tok)

    def block(w, dz, dy, c0, n, half=None):
        rows, off = (ROWS, 0) if half is None else (ROWS // 2, half * ROWS // 2)

        def view():
            start = pl.multiple_of(mod(y + dy, NY) * ROWS + off, ROWS // 2)
            return w.at[mod(zl + dz, NZ), pl.ds(start, rows), pl.ds(c0, n)]

        return view

    def slab(w, dz, c0, n, half=None):
        rows, off = (GROUP, 0) if half is None else (GROUP // 2, half * GROUP // 2)
        return lambda: w.at[mod(zl + dz, NZ), pl.ds(off, rows), pl.ds(c0, n)]

    ready = {}

    def y_first(tag, w, c0, n, deps, prio):
        size = ROWS * n * 2
        for d in "+-":
            s = sign[d]
            b = block(w, 0, 0, c0, n)
            send(f"{tag}.Y1{d}", "y" + d, deps, b, b, block(w, 0, -s, c0, n), size, prio)
        for d, half in (("+", 0), ("-", 1)):
            s = sign[d]
            b = block(w, 0, -s, c0, n, half)
            send(f"{tag}.Y2{d}", "y" + d, [f"{tag}.Y1{d}"], b, b, block(w, 0, -2 * s, c0, n, half), size // 2, prio)
        group = [f"{tag}.Y{h}{d}" for h in (1, 2) for d in "+-"]
        ready[tag[0], 0] = ready.get((tag[0], 0), []) + group
        for d, half in (("+", 0), ("-", 1)):
            s = sign[d]
            for h in (1, 2, 3, 4):
                part = half if h == 4 else None
                b = slab(w, -s * (h - 1), c0, n, part)
                before = deps + group if h == 1 else [f"{tag}.Z{h - 1}{d}"]
                send(f"{tag}.Z{h}{d}", "z" + d, before, b, b, slab(w, -s * h, c0, n, part),
                     NY * size // (1 if part is None else 2), prio)
                dist = 4 if h == 4 else -s * h
                ready[tag[0], dist] = ready.get((tag[0], dist), []) + [f"{tag}.Z{h}{d}"]

    def z_first(tag, w, c0, n, deps, prio):
        size = ROWS * n * 2
        for d, half in (("+", 0), ("-", 1)):
            s = sign[d]
            for h in (1, 2, 3, 4):
                part = half if h == 4 else None
                b = block(w, -s * (h - 1), 0, c0, n, part)
                before = deps if h == 1 else [f"{tag}.Z{h - 1}{d}"]
                send(f"{tag}.Z{h}{d}", "z" + d, before, b, b, block(w, -s * h, 0, c0, n, part),
                     size // (1 if part is None else 2), prio)
        for dist in ARRIVAL:
            here = {0: deps, 4: [f"{tag}.Z4+", f"{tag}.Z4-"]}.get(
                dist, [f"{tag}.Z{abs(dist)}{'-' if dist > 0 else '+'}"])
            for d, half in (("+", 0), ("-", 1)):
                s = sign[d]
                b = block(w, dist, 0, c0, n)
                send(f"{tag}.Y1{d}{dist}", "y" + d, here, b, b, block(w, dist, -s, c0, n), size, prio)
                b = block(w, dist, -s, c0, n, half)
                send(f"{tag}.Y2{d}{dist}", "y" + d, [f"{tag}.Y1{d}{dist}"], b, b,
                     block(w, dist, -2 * s, c0, n, half), size // 2, prio)
            names = here + [f"{tag}.Y{h}{d}{dist}" for h in (1, 2) for d in "+-"]
            ready[tag[0], dist] = ready.get((tag[0], dist), []) + names

    seen = []
    mixer_loads = ["load.m0", "load.m1", "load.m2", "load.m3"]
    column, loads_of = 0, {"m": mixer_loads, "u": ["load.u"], "d": ["load.d"]}
    for tag, way, n, prio in PIECES:
        w = {"m": wm, "u": wu, "d": wd}[tag[0]]
        if tag[0] not in [t[0] for t in seen]:
            column = 0
        seen.append(tag)
        way = y_first if way == "y" else z_first
        way(tag, w, column, n, loads_of[tag[0]], prio)
        column += n

    def project(first_one, dists):
        def emit():
            for at, dist in enumerate(dists):
                g = mod(zl + dist, NZ)
                term = jnp.dot(
                    tok[:, pl.ds(pl.multiple_of(g * GROUP, GROUP), GROUP)], wm[g, :, 0:384],
                    preferred_element_type=f32)
                if first_one and at == 0:
                    proj[...] = term
                else:
                    proj[...] += term

        return emit

    def convolve():
        prod[0:8, :] = jnp.zeros((8, 128), f32)
        prod[8:, :] = proj[:, 128:256] * proj[:, 256:384]
        total = taps[0:1, :] * prod[6:6 + SEQ, :]
        total = total + taps[1:2, :] * prod[7:7 + SEQ, :]
        total = total + taps[2:3, :] * prod[8:8 + SEQ, :]
        conv[...] = (proj[:, 0:128] * total).astype(bf16)

    compute_after = ["load.t"] + mixer_loads
    for dist in ARRIVAL:
        compute_after = compute_after + ready["m", dist]
        compute(f"project{dist}", compute_after, project(dist == 0, [dist]), 0, 0.35)
        compute_after = [f"project{dist}"]
    compute("convolve", compute_after, convolve, 0, 0.7)

    nt = (((1,), (1,)), ((), ()))

    def product(phase, p, k, left, rights):
        for at, right in enumerate(rights):
            pp[phase, p, k, :, at * GROUP:(at + 1) * GROUP] = lax.dot_general(
                left[p * PART:(p + 1) * PART, :], right(), nt, preferred_element_type=f32).astype(bf16)

    def rows_of(dx):
        return pl.ds(pl.multiple_of(mod(x + dx, NX) * OWN, OWN), OWN)

    def core_rows(core):
        return pl.ds(pl.multiple_of(core * CORE_ROWS, CORE_ROWS), CORE_ROWS)

    def seq_rows(p, dx=0, core=None):
        core = c if core is None else core
        return pl.ds(pl.multiple_of(p * PART + core * CORE_ROWS + mod(x + dx, NX) * OWN, OWN), OWN)

    def sum_chunk(phase, p, k, groups, residual, prio):
        t = f"s{phase}{p}.{k}"
        d, e = ("+", "-") if k % 2 == 0 else ("-", "+")
        s = sign[d]
        send(f"{t}.pair", "c", [f"{t}.product"], lambda: pp.at[phase, p, k, core_rows(1 - c), :],
             lambda: dr.at[phase, p, k], lambda: dr.at[phase, p, k], CORE_ROWS * CHUNK * 2, prio)

        def add_pair():
            so[phase, p, k] = (
                pp[phase, p, k, core_rows(c), :].astype(f32) + dr[phase, p, k].astype(f32)).astype(bf16)

        compute(f"{t}.add", [f"{t}.product", f"{t}.pair"], add_pair, prio, 0.06)
        size = OWN * CHUNK * 2
        at = lambda dx: (lambda: so.at[phase, p, k, rows_of(dx), :])
        slot = lambda ref: (lambda: ref.at[phase, p, k])
        send(f"{t}.relay", "x" + d, [f"{t}.add"], at(2), slot(rl), slot(rl), size, prio)
        send(f"{t}.direct", "x" + e, [f"{t}.add"], at(-s), slot(fd), slot(fd), size, prio + 0.5)

        def add_relay():
            so[phase, p, k, rows_of(s), :] = (
                so[phase, p, k, rows_of(s), :].astype(f32) + rl[phase, p, k].astype(f32)).astype(bf16)

        compute(f"{t}.radd", [f"{t}.add", f"{t}.relay"], add_relay, prio, 0.03)
        send(f"{t}.final", "x" + d, [f"{t}.radd"], at(s), slot(fr), slot(fr), size, prio)

        def finish():
            total = so[phase, p, k, rows_of(0), :].astype(f32) + fr[phase, p, k].astype(f32)
            total = total + fd[phase, p, k].astype(f32)
            for at, group in enumerate(groups):
                columns = pl.ds(pl.multiple_of(group() * GROUP, GROUP), GROUP)
                v[p, :, columns] = (residual_scale * residual[seq_rows(p), columns].astype(f32)
                                    + total[:, at * GROUP:(at + 1) * GROUP])

        compute(f"{t}.finish", [f"{t}.add", f"{t}.final", f"{t}.direct"], finish, prio, 0.04)

    def norm(phase, p, gain, shift, dest, prio):
        def emit():
            values = v[p]
            mean = jnp.mean(values, -1, keepdims=True)
            centered = values - mean
            variance = jnp.mean(centered * centered, -1, keepdims=True)
            scaled = centered * lax.rsqrt(variance + norm_epsilon)
            dest[seq_rows(p), :] = (scaled * gain[...] + shift[...]).astype(bf16)

        compute(f"norm{phase}{p}", [f"s{phase}{p}.{k}.finish" for k in range(CHUNKS)], emit, prio, 0.25)

    HALF = WIDTH // 2

    def place(p, dx, h, other=False):
        def view(ref):
            rows = seq_rows(p, dx, 1 - c if other else c)
            return ref.at[rows, :] if h is None else ref.at[rows, pl.ds(h * HALF, HALF)]
        return view

    def gather(phase, p, ref, prio):
        def at(*where):
            return lambda: place(p, *where)(ref)

        t, size, landed = f"g{phase}{p}", OWN * HALF * 2, []
        start = [f"norm{phase}{p}"]
        for d, first_half in (("+", 0), ("-", 1)):
            for h in (first_half, 1 - first_half):
                send(f"{t}.A{d}{h}", "x" + d, start, at(0, h), at(0, h), at(-sign[d], h), size, prio)
                landed.append((f"{t}.A{d}{h}", (-sign[d], h)))
        send(f"{t}.P", "c", start, at(0, None), at(0, None), at(0, None, True), 2 * size, prio)
        landed.append((f"{t}.P", (0, None, True)))
        for d, h in (("+", 0), ("-", 1)):
            b = at(-sign[d], h)
            send(f"{t}.B{d}", "x" + d, [f"{t}.A{d}{h}"], b, b, at(2, h), size, prio)
            landed.append((f"{t}.B{d}", (2, h)))
        for name, dx, h in ((f"{t}.A+0", -1, 0), (f"{t}.A-1", 1, 1), (f"{t}.A+1", -1, 1),
                            (f"{t}.A-0", 1, 0), (f"{t}.B+", 2, 0), (f"{t}.B-", 2, 1)):
            send(f"{name}.P", "c", [name], at(dx, h), at(dx, h), at(dx, h, True), size, prio)
            landed.append((f"{name}.P", (dx, h, True)))
        return landed

    def hidden(p, n):
        columns = pl.ds(n * 256, 256)
        rows = pl.ds(p * PART, PART)
        up = jnp.dot(first[rows, :], wu[:, :, columns].reshape(WIDTH, 256), preferred_element_type=f32)
        hid[rows, columns] = jnp.square(jnp.maximum(up, 0.0)).astype(bf16)

    stores = []

    def store(name, deps, where):
        index = len(stores)
        copy = lambda: pltpu.make_async_copy(where(res), where(out_hbm), store_sems.at[index])
        stores.append(copy)
        ops.append(Op(name, deps, lambda: copy().start(), 5, dur=0.02))

    up_ready = ["load.u"] + [n for dist in ARRIVAL for n in ready["u", dist]]
    for p in range(PARTS):
        for k in range(CHUNKS):
            pair = (2 * k, 2 * k + 1)
            compute(f"s0{p}.{k}.product", ["convolve"],
                    functools.partial(product, 0, p, k, conv, [lambda g=g: wm[g, :, 384:512] for g in pair]),
                    0 + p, 0.25)
            sum_chunk(0, p, k, [lambda g=g: g for g in pair], tok, 0 + p)
        norm(0, p, mgain, mshift, first, 0 + p)
        landed = gather(0, p, first, 0 + p)
        for n in range(4):
            compute(f"hidden{p}{n}", [f"norm0{p}"] + [name for name, _ in landed] + up_ready,
                    functools.partial(hidden, p, n), 2 + p, 0.37)
        for k in range(CHUNKS):
            dists = ARRIVAL[2 * k:2 * k + 2]
            groups = [lambda dist=dist: mod(zl + dist, NZ) for dist in dists]
            arrived = [name for dist in dists for name in ready["d", dist]]
            compute(f"s1{p}.{k}.product", [f"hidden{p}{n}" for n in range(4)] + ["load.d"] + arrived,
                    functools.partial(product, 1, p, k, hid, [lambda g=g: wd[g()] for g in groups]),
                    2 + p, 0.5)
            sum_chunk(1, p, k, groups, first, 2 + p)
        norm(1, p, cgain, cshift, res, 2 + p)
        store(f"out{p}.own", [f"norm1{p}"], place(p, 0, None))
        for name, where in gather(1, p, res, 2 + p):
            store(f"out.{name}", [name], place(p, *where))

    order, done = plan(ops)
    if report is not None:
        report(order, done, len(sends), len(loads), len(stores))

    for start_load in loads:
        start_load()
    barrier = pltpu.get_barrier_semaphore()
    for link in peer:
        pl.semaphore_signal(barrier, inc=1, device_id=peer[link], device_id_type=pl.DeviceIdType.MESH)
    pl.semaphore_wait(barrier, len(peer))

    by_name = {op.name: op for op in ops}
    waited = set()

    def need(name):
        op = by_name[name]
        if op.wait is not None and name not in waited:
            waited.add(name)
            op.wait()

    for _, op in order:
        for name in op.deps:
            need(name)
        op.emit()
    for op in ops:
        need(op.name)
    for _, wait in sends:
        wait()
    for copy in stores:
        copy().wait()


N_SENDS, N_LOADS, N_STORES = 480, 7, 28


def local(tokens, gate_outer, gate_inner, conv_input, mixer_output, conv_taps, mixer_gain,
          mixer_shift, up_weight, down_weight, channel_gain, channel_shift):
    bf16, f32 = jnp.bfloat16, jnp.float32
    vmem, hbm = pl.BlockSpec(memory_space=pltpu.VMEM), pl.BlockSpec(memory_space=pl.ANY)
    return pl.pallas_call(
        layer_kernel,
        out_shape=jax.ShapeDtypeStruct((SEQ, WIDTH), bf16),
        in_specs=[hbm] * 7 + [vmem] * 5,
        out_specs=hbm,
        scratch_shapes=[
            pltpu.VMEM((SEQ, WIDTH), bf16),
            pltpu.VMEM((NZ, GROUP, 512), bf16),
            pltpu.VMEM((NZ, GROUP, 1024), bf16),
            pltpu.VMEM((NZ, GROUP, 1024), bf16),
            pltpu.VMEM((SEQ, 384), f32),
            pltpu.VMEM((SEQ + 8, 128), f32),
            pltpu.VMEM((SEQ, 128), bf16),
            pltpu.VMEM((2, PARTS, CHUNKS, PART, CHUNK), bf16),
            pltpu.VMEM((2, PARTS, CHUNKS, CORE_ROWS, CHUNK), bf16),
            pltpu.VMEM((2, PARTS, CHUNKS, CORE_ROWS, CHUNK), bf16),
            pltpu.VMEM((2, PARTS, CHUNKS, OWN, CHUNK), bf16),
            pltpu.VMEM((2, PARTS, CHUNKS, OWN, CHUNK), bf16),
            pltpu.VMEM((2, PARTS, CHUNKS, OWN, CHUNK), bf16),
            pltpu.VMEM((PARTS, OWN, WIDTH), f32),
            pltpu.VMEM((SEQ, WIDTH), bf16),
            pltpu.VMEM((SEQ, 1024), bf16),
            pltpu.VMEM((SEQ, WIDTH), bf16),
            pltpu.SemaphoreType.DMA((N_SENDS,)),
            pltpu.SemaphoreType.DMA((N_SENDS,)),
            pltpu.SemaphoreType.DMA((N_LOADS,)),
            pltpu.SemaphoreType.DMA((N_STORES,)),
        ],
        compiler_params=pltpu.CompilerParams(
            collective_id=0, has_side_effects=True, vmem_limit_bytes=60 * 2**20),
    )(tokens, gate_outer, gate_inner, conv_input, mixer_output, up_weight, down_weight, conv_taps,
      mixer_gain.reshape(1, -1), mixer_shift.reshape(1, -1), channel_gain.reshape(1, -1),
      channel_shift.reshape(1, -1))


def solution(mesh):
    weights = P("fs", "tp")
    in_specs = (
        P(("rep", "fs"), None), weights, weights, weights, weights, P(None, "tp"), P(), P(),
        weights, weights, P(), P(),
    )
    out_specs = P(("rep", "fs"), None)
    return jax.shard_map(local, mesh=mesh, in_specs=in_specs, out_specs=out_specs, check_vma=False)
```

```python
import functools

import jax
import jax.numpy as jnp
from jax import lax
from jax.experimental import pallas as pl
from jax.experimental.pallas import tpu as pltpu
from jax.sharding import PartitionSpec as P

residual_scale = 8.0**0.25
norm_epsilon = 1e-05

NZ, NY, NX = 8, 4, 4
SEQ, WIDTH = 512, 2048
ROWS = 64
GROUP = 256
PARTS = 2
PART = SEQ // PARTS
CORE_ROWS, OWN = PART // 2, PART // 8
CHUNKS, CHUNK = 4, 512
ARRIVAL = (0, 1, -1, 2, -2, 3, -3, 4)

LINK_RATE, LINK_LAT = 46.6e3, 1.9
PAIR_RATE, PAIR_LAT = 500e3, 1.1
BACKLOG = 1.0


PIECES = (
    ("m0", "y", 128, 1), ("m1", "y", 128, 1), ("m2", "z", 256, 1),
    ("u0", "y", 128, 4), ("u1", "y", 256, 4), ("u2", "z", 384, 4), ("u3", "z", 256, 4),
    ("d0", "y", 128, 5), ("d1", "y", 256, 5), ("d2", "z", 384, 5), ("d3", "z", 256, 5),
)
NOT_BEFORE = {4: 0.0, 5: 0.0}
PRIORITY = {}


class Op:
    def __init__(self, name, deps, emit, prio, dur=0.0, link=None, nbytes=0, wait=None, latency=0.0):
        self.name, self.deps, self.emit, self.prio = name, deps, emit, prio
        self.dur, self.link, self.nbytes, self.wait = dur, link, nbytes, wait
        self.latency, self.group = latency, None


def plan(ops):
    done, link_free, order, now = {}, {}, [], 0.0
    members = {}
    for op in ops:
        if op.group is not None:
            members.setdefault(op.group, []).append(op.name)
    group_of = {op.name: members[op.group] for op in ops if op.group is not None}
    for op in ops:
        op.deps = list(dict.fromkeys(m for d in op.deps for m in group_of.get(d, [d])))
    left = list(ops)
    while left:
        best = None
        for at, op in enumerate(left):
            if any(d not in done for d in op.deps):
                continue
            ready = max([done[d] for d in op.deps], default=NOT_BEFORE.get(op.prio, 0.0))
            ready = max(ready, NOT_BEFORE.get(op.prio, 0.0))
            if op.link is not None:
                ready = max(ready, link_free.get(op.link, 0.0) - (BACKLOG if op.prio >= 3 else 3 * BACKLOG))
            key = (max(ready, now), op.prio, at)
            if best is None or key < best[0]:
                best = (key, op)
        (start, _, _), op = best
        left.remove(op)
        now = start + (op.dur if op.link is None else 0.03)
        if op.link is None:
            done[op.name] = now + op.latency
        else:
            rate, lat = (PAIR_RATE, PAIR_LAT) if op.link == "c" else (LINK_RATE, LINK_LAT)
            begin = max(now, link_free.get(op.link, 0.0))
            link_free[op.link] = begin + op.nbytes / rate
            done[op.name] = link_free[op.link] + lat
        order.append((start, op))
    return order, done


def layer_kernel(
    tok_hbm, go_hbm, gi_hbm, ci_hbm, mo_hbm, up_hbm, dn_hbm, taps, mgain, mshift, cgain, cshift,
    res,
    tok, wm, wu, wd, proj, prod, conv, pp, so, dr, rl, fr, fd, v, first, hid,
    send_sems, recv_sems, load_sems,
    report=None,
):
    f32, bf16 = jnp.float32, jnp.bfloat16
    rep, fs, tp = lax.axis_index("rep"), lax.axis_index("fs"), lax.axis_index("tp")
    zl, y = lax.div(fs, NY), lax.rem(fs, NY)
    x, c = lax.div(tp, 2), lax.rem(tp, 2)
    z = rep * NZ + zl

    def mod(v, n):
        return lax.rem(v + 2 * n, n)

    def device(dz=0, dy=0, dx=0, dc=0):
        zz = mod(z + dz, 2 * NZ)
        return (
            lax.div(zz, NZ),
            lax.rem(zz, NZ) * NY + mod(y + dy, NY),
            mod(x + dx, NX) * 2 + lax.rem(c + dc, 2),
        )

    peer = {
        "z+": device(dz=1), "z-": device(dz=-1), "y+": device(dy=1), "y-": device(dy=-1),
        "x+": device(dx=1), "x-": device(dx=-1), "c": device(dc=1),
    }
    sign = {"+": 1, "-": -1}

    ops = []
    sends = {}

    send_groups, recv_groups = {}, {}

    def send(name, link, deps, src, dst, landed, nbytes, prio, sent, group=None):
        send_at = send_groups.setdefault(sent[0], len(send_groups))
        recv_at = recv_groups.setdefault(group[0] if group else name, len(recv_groups))

        def copy(s, d):
            return pltpu.make_async_remote_copy(
                src_ref=s, dst_ref=d, send_sem=send_sems.at[send_at], recv_sem=recv_sems.at[recv_at],
                device_id=peer[link], device_id_type=pl.DeviceIdType.MESH,
            )

        all_here = group[1] if group else landed
        sends.setdefault(sent[0], lambda: copy(sent[1](), sent[1]()).wait_send())
        op = Op(
            name, deps, lambda: copy(src(), dst()).start(), prio, link=link, nbytes=nbytes,
            wait=lambda: copy(all_here(), all_here()).wait_recv(),
        )
        op.group = group[0] if group else None
        ops.append(op)

    def compute(name, deps, emit, prio, dur):
        ops.append(Op(name, deps, emit, prio, dur=dur))

    loads = []

    def load(name, src, dst):
        index = len(loads)
        op = Op(name, [], lambda: None, 0, latency=0.5)
        op.wait = lambda: pltpu.make_async_copy(src(), dst(), load_sems.at[index]).wait()
        loads.append(lambda: pltpu.make_async_copy(src(), dst(), load_sems.at[index]).start())
        ops.append(op)

    def own(w, c0, n):
        return lambda: w.at[zl, pl.ds(pl.multiple_of(y * ROWS, ROWS), ROWS), pl.ds(c0, n)]

    load("load.m0", lambda: go_hbm, own(wm, 0, 128))
    load("load.m1", lambda: gi_hbm, own(wm, 128, 128))
    load("load.m2", lambda: ci_hbm, own(wm, 256, 128))
    load("load.m3", lambda: mo_hbm, own(wm, 384, 128))
    load("load.u", lambda: up_hbm, own(wu, 0, 1024))
    load("load.d", lambda: dn_hbm, own(wd, 0, 1024))
    load("load.t", lambda: tok_hbm, lambda: tok)

    def block(w, dz, dy, c0, n, half=None):
        rows, off = (ROWS, 0) if half is None else (ROWS // 2, half * ROWS // 2)

        def view():
            start = pl.multiple_of(mod(y + dy, NY) * ROWS + off, ROWS // 2)
            return w.at[mod(zl + dz, NZ), pl.ds(start, rows), pl.ds(c0, n)]

        return view

    def slab(w, dz, c0, n, half=None):
        rows, off = (GROUP, 0) if half is None else (GROUP // 2, half * GROUP // 2)
        return lambda: w.at[mod(zl + dz, NZ), pl.ds(off, rows), pl.ds(c0, n)]

    ready = {}

    def y_first(tag, w, c0, n, deps, prio):
        size = ROWS * n * 2
        part_of = lambda zs, rows: (lambda: w.at[zs, rows, pl.ds(c0, n)])
        sent_y = (f"{tag}.Y", part_of(0, pl.ds(0, 3 * ROWS)))
        sent_z = (f"{tag}.Z", part_of(pl.ds(0, 7), pl.ds(0, GROUP)))
        second = (f"{tag}.Y2", part_of(0, pl.ds(0, ROWS)))
        fourth = (f"{tag}.Z4", part_of(0, pl.ds(0, GROUP)))
        for d in "+-":
            s = sign[d]
            b = block(w, 0, 0, c0, n)
            send(f"{tag}.Y1{d}", "y" + d, deps, b, b, block(w, 0, -s, c0, n), size,
                 PRIORITY.get(f"{tag[0]}yY1", prio), sent_y)
        for d, half in (("+", 0), ("-", 1)):
            s = sign[d]
            b = block(w, 0, -s, c0, n, half)
            send(f"{tag}.Y2{d}", "y" + d, [f"{tag}.Y1{d}"], b, b, block(w, 0, -2 * s, c0, n, half), size // 2,
                 PRIORITY.get(f"{tag[0]}yY2", prio), sent_y, second)
        group = [f"{tag}.Y{h}{d}" for h in (1, 2) for d in "+-"]
        ready[tag[0], 0] = ready.get((tag[0], 0), []) + group
        for d, half in (("+", 0), ("-", 1)):
            s = sign[d]
            for h in (1, 2, 3, 4):
                part = half if h == 4 else None
                b = slab(w, -s * (h - 1), c0, n, part)
                before = deps + group if h == 1 else [f"{tag}.Z{h - 1}{d}"]
                send(f"{tag}.Z{h}{d}", "z" + d, before, b, b, slab(w, -s * h, c0, n, part),
                     NY * size // (1 if part is None else 2), PRIORITY.get(f"{tag[0]}yZ{h}", prio),
                     sent_z, fourth if h == 4 else None)
                dist = 4 if h == 4 else -s * h
                ready[tag[0], dist] = ready.get((tag[0], dist), []) + [f"{tag}.Z{h}{d}"]

    def z_first(tag, w, c0, n, deps, prio):
        size = ROWS * n * 2
        part_of = lambda zs, rows: (lambda: w.at[zs, rows, pl.ds(c0, n)])
        sent_z = part_of(0, pl.ds(0, 7 * ROWS // 2))
        sent_y = (f"{tag}.Y", part_of(pl.ds(0, 6), pl.ds(0, GROUP)))
        fourth = (f"{tag}.Z4", part_of(0, pl.ds(0, ROWS)))
        for d, half in (("+", 0), ("-", 1)):
            s = sign[d]
            for h in (1, 2, 3, 4):
                part = half if h == 4 else None
                b = block(w, -s * (h - 1), 0, c0, n, part)
                before = deps if h == 1 else [f"{tag}.Z{h - 1}{d}"]
                send(f"{tag}.Z{h}{d}", "z" + d, before, b, b, block(w, -s * h, 0, c0, n, part),
                     size // (1 if part is None else 2), PRIORITY.get(f"{tag[0]}zZ{h}", prio),
                     (f"{tag}.Z{d}", sent_z), fourth if h == 4 else None)
        for at, dist in enumerate(ARRIVAL):
            here = {0: deps, 4: [f"{tag}.Z4+", f"{tag}.Z4-"]}.get(
                dist, [f"{tag}.Z{abs(dist)}{'-' if dist > 0 else '+'}"])
            second = {
                "m": (f"{tag}.Y2.{at}", part_of(0, pl.ds(0, ROWS))),
                "u": (f"{tag}.Y2", part_of(pl.ds(0, 2), pl.ds(0, GROUP))),
                "d": (f"{tag}.Y2.{at // 2}", part_of(0, pl.ds(0, 2 * ROWS))),
            }[tag[0]]
            for d, half in (("+", 0), ("-", 1)):
                s = sign[d]
                b = block(w, dist, 0, c0, n)
                send(f"{tag}.Y1{d}{dist}", "y" + d, here, b, b, block(w, dist, -s, c0, n), size,
                     PRIORITY.get(f"{tag[0]}zY{abs(dist)}", prio), sent_y)
                b = block(w, dist, -s, c0, n, half)
                send(f"{tag}.Y2{d}{dist}", "y" + d, [f"{tag}.Y1{d}{dist}"], b, b,
                     block(w, dist, -2 * s, c0, n, half), size // 2,
                     PRIORITY.get(f"{tag[0]}zY{abs(dist)}", prio), sent_y, second)
            names = here + [f"{tag}.Y{h}{d}{dist}" for h in (1, 2) for d in "+-"]
            ready[tag[0], dist] = ready.get((tag[0], dist), []) + names

    seen = []
    mixer_loads = ["load.m0", "load.m1", "load.m2", "load.m3"]
    column, loads_of = 0, {"m": mixer_loads, "u": ["load.u"], "d": ["load.d"]}
    for tag, way, n, prio in PIECES:
        w = {"m": wm, "u": wu, "d": wd}[tag[0]]
        if tag[0] not in [t[0] for t in seen]:
            column = 0
        seen.append(tag)
        way = y_first if way == "y" else z_first
        way(tag, w, column, n, loads_of[tag[0]], prio)
        column += n

    def project(first_one, dists):
        def emit():
            for at, dist in enumerate(dists):
                g = mod(zl + dist, NZ)
                term = jnp.dot(
                    tok[:, pl.ds(pl.multiple_of(g * GROUP, GROUP), GROUP)], wm[g, :, 0:384],
                    preferred_element_type=f32)
                if first_one and at == 0:
                    proj[...] = term
                else:
                    proj[...] += term

        return emit

    def convolve():
        prod[0:8, :] = jnp.zeros((8, 128), f32)
        prod[8:, :] = proj[:, 128:256] * proj[:, 256:384]
        total = taps[0:1, :] * prod[6:6 + SEQ, :]
        total = total + taps[1:2, :] * prod[7:7 + SEQ, :]
        total = total + taps[2:3, :] * prod[8:8 + SEQ, :]
        conv[...] = (proj[:, 0:128] * total).astype(bf16)

    compute_after = ["load.t"] + mixer_loads
    for dist in ARRIVAL:
        compute_after = compute_after + ready["m", dist]
        compute(f"project{dist}", compute_after, project(dist == 0, [dist]), 0, 0.35)
        compute_after = [f"project{dist}"]
    compute("convolve", compute_after, convolve, 0, 0.7)

    nt = (((1,), (1,)), ((), ()))

    def product(phase, p, k, left, rights):
        for at, right in enumerate(rights):
            pp[phase, p, k, :, at * GROUP:(at + 1) * GROUP] = lax.dot_general(
                left[p * PART:(p + 1) * PART, :], right(), nt, preferred_element_type=f32).astype(bf16)

    def rows_of(dx):
        return pl.ds(pl.multiple_of(mod(x + dx, NX) * OWN, OWN), OWN)

    def core_rows(core):
        return pl.ds(pl.multiple_of(core * CORE_ROWS, CORE_ROWS), CORE_ROWS)

    def seq_rows(p, dx=0, core=None):
        core = c if core is None else core
        return pl.ds(pl.multiple_of(p * PART + core * CORE_ROWS + mod(x + dx, NX) * OWN, OWN), OWN)

    def sum_chunk(phase, p, k, groups, residual, prio):
        t = f"s{phase}{p}.{k}"
        d, e = ("+", "-") if k % 2 == 0 else ("-", "+")
        s = sign[d]
        send(f"{t}.pair", "c", [f"{t}.product"], lambda: pp.at[phase, p, k, core_rows(1 - c), :],
             lambda: dr.at[phase, p, k], lambda: dr.at[phase, p, k], CORE_ROWS * CHUNK * 2, prio,
             (f"s{phase}{p}.pair", lambda: dr.at[phase, p]))

        def add_pair():
            so[phase, p, k] = (
                pp[phase, p, k, core_rows(c), :].astype(f32) + dr[phase, p, k].astype(f32)).astype(bf16)

        compute(f"{t}.add", [f"{t}.product", f"{t}.pair"], add_pair, prio, 0.06)
        size = OWN * CHUNK * 2
        at = lambda dx: (lambda: so.at[phase, p, k, rows_of(dx), :])
        slot = lambda ref: (lambda: ref.at[phase, p, k])
        sent = (f"s{phase}{p}.x", lambda: so.at[phase, p, pl.ds(0, CHUNKS - 1)])
        last = (f"{t}.last", lambda: so.at[phase, p, k, pl.ds(0, 2 * OWN), :])
        send(f"{t}.relay", "x" + d, [f"{t}.add"], at(2), slot(rl), slot(rl), size, prio, sent)
        send(f"{t}.direct", "x" + e, [f"{t}.add"], at(-s), slot(fd), slot(fd), size, prio + 0.5,
             sent, last)

        def add_relay():
            so[phase, p, k, rows_of(s), :] = (
                so[phase, p, k, rows_of(s), :].astype(f32) + rl[phase, p, k].astype(f32)).astype(bf16)

        compute(f"{t}.radd", [f"{t}.add", f"{t}.relay"], add_relay, prio, 0.03)
        send(f"{t}.final", "x" + d, [f"{t}.radd"], at(s), slot(fr), slot(fr), size, prio, sent, last)

        def finish():
            total = so[phase, p, k, rows_of(0), :].astype(f32) + fr[phase, p, k].astype(f32)
            total = total + fd[phase, p, k].astype(f32)
            for at, group in enumerate(groups):
                columns = pl.ds(pl.multiple_of(group() * GROUP, GROUP), GROUP)
                v[p, :, columns] = (residual_scale * residual[seq_rows(p), columns].astype(f32)
                                    + total[:, at * GROUP:(at + 1) * GROUP])

        compute(f"{t}.finish", [f"{t}.add", f"{t}.final", f"{t}.direct"], finish, prio, 0.04)

    def norm(phase, p, gain, shift, dest, prio):
        def emit():
            values = v[p]
            mean = jnp.mean(values, -1, keepdims=True)
            centered = values - mean
            variance = jnp.mean(centered * centered, -1, keepdims=True)
            scaled = centered * lax.rsqrt(variance + norm_epsilon)
            dest[seq_rows(p), :] = (scaled * gain[...] + shift[...]).astype(bf16)

        compute(f"norm{phase}{p}", [f"s{phase}{p}.{k}.finish" for k in range(CHUNKS)], emit, prio, 0.25)

    HALF = WIDTH // 2

    def place(p, dx, h, other=False):
        def view(ref):
            rows = seq_rows(p, dx, 1 - c if other else c)
            return ref.at[rows, :] if h is None else ref.at[rows, pl.ds(h * HALF, HALF)]
        return view

    def gather(phase, p, ref, prio):
        def at(*where):
            return lambda: place(p, *where)(ref)

        t, size, landed = f"g{phase}{p}", OWN * HALF * 2, []
        start = [f"norm{phase}{p}"]
        first_rows = lambda rows: (lambda: ref.at[pl.ds(0, rows), :])
        sent_x, sent_c = (f"{t}.x", first_rows(3 * OWN)), (f"{t}.c", first_rows(4 * OWN))
        if phase == 0:
            pairs = [(f"{t}.P", first_rows(4 * OWN))] * 4
        else:
            pairs = [(f"{t}.P{i}", first_rows(rows)) for i, rows in enumerate((OWN, OWN, OWN, OWN))]
        for d, first_half in (("+", 0), ("-", 1)):
            for h in (first_half, 1 - first_half):
                send(f"{t}.A{d}{h}", "x" + d, start, at(0, h), at(0, h), at(-sign[d], h), size, prio, sent_x)
                landed.append((f"{t}.A{d}{h}", (-sign[d], h)))
        send(f"{t}.P", "c", start, at(0, None), at(0, None), at(0, None, True), 2 * size, prio, sent_c, pairs[0])
        landed.append((f"{t}.P", (0, None, True)))
        for d, h in (("+", 0), ("-", 1)):
            b = at(-sign[d], h)
            send(f"{t}.B{d}", "x" + d, [f"{t}.A{d}{h}"], b, b, at(2, h), size, prio, sent_x)
            landed.append((f"{t}.B{d}", (2, h)))
        for i, (name, dx, h) in enumerate((
                (f"{t}.A+0", -1, 0), (f"{t}.A-1", 1, 1), (f"{t}.A+1", -1, 1),
                (f"{t}.A-0", 1, 0), (f"{t}.B+", 2, 0), (f"{t}.B-", 2, 1))):
            send(f"{name}.P", "c", [name], at(dx, h), at(dx, h), at(dx, h, True), size, prio,
                 sent_c, pairs[1 + i // 2])
            landed.append((f"{name}.P", (dx, h, True)))
        return landed

    def hidden(p, n):
        rows = pl.ds(p * PART, PART)
        for at in (2 * n, 2 * n + 1):
            columns = pl.ds(at * 256, 256)
            up = jnp.dot(first[rows, :], wu[:, :, columns].reshape(WIDTH, 256), preferred_element_type=f32)
            hid[rows, columns] = jnp.square(jnp.maximum(up, 0.0)).astype(bf16)

    up_ready = ["load.u"] + [n for dist in ARRIVAL for n in ready["u", dist]]
    for p in range(PARTS):
        for k in range(CHUNKS):
            pair = (2 * k, 2 * k + 1)
            compute(f"s0{p}.{k}.product", ["convolve"],
                    functools.partial(product, 0, p, k, conv, [lambda g=g: wm[g, :, 384:512] for g in pair]),
                    0 + p, 0.25)
            sum_chunk(0, p, k, [lambda g=g: g for g in pair], tok, 0 + p)
        norm(0, p, mgain, mshift, first, 0 + p)
        landed = gather(0, p, first, 0 + p)
        for n in range(2):
            compute(f"hidden{p}{n}", [f"norm0{p}"] + [name for name, _ in landed] + up_ready,
                    functools.partial(hidden, p, n), 2 + p, 0.75)
        for k in range(CHUNKS):
            dists = ARRIVAL[2 * k:2 * k + 2]
            groups = [lambda dist=dist: mod(zl + dist, NZ) for dist in dists]
            arrived = [name for dist in dists for name in ready["d", dist]]
            compute(f"s1{p}.{k}.product", [f"hidden{p}{n}" for n in range(2)] + ["load.d"] + arrived,
                    functools.partial(product, 1, p, k, hid, [lambda g=g: wd[g()] for g in groups]),
                    2 + p, 0.5)
            sum_chunk(1, p, k, groups, first, 2 + p)
        norm(1, p, cgain, cshift, res, 2 + p)
        gather(1, p, res, 2 + p)

    order, done = plan(ops)
    if report is not None:
        report(order, done, len(send_groups), len(recv_groups), len(loads))
    assert (len(send_groups), len(recv_groups), len(loads)) == (N_SENDS, N_RECVS, N_LOADS), (
        len(send_groups), len(recv_groups), len(loads))

    for start_load in loads:
        start_load()
    barrier = pltpu.get_barrier_semaphore()
    for link in peer:
        pl.semaphore_signal(barrier, inc=1, device_id=peer[link], device_id_type=pl.DeviceIdType.MESH)
    pl.semaphore_wait(barrier, len(peer))

    by_name = {op.name: op for op in ops}
    waited = set()

    def need(name):
        op = by_name[name]
        key = op.group or name
        if op.wait is not None and key not in waited:
            waited.add(key)
            op.wait()

    for _, op in order:
        for name in op.deps:
            need(name)
        op.emit()
    for op in ops:
        need(op.name)
    for wait in sends.values():
        wait()


N_SENDS, N_RECVS, N_LOADS = 43, 275, 7


def local(tokens, gate_outer, gate_inner, conv_input, mixer_output, conv_taps, mixer_gain,
          mixer_shift, up_weight, down_weight, channel_gain, channel_shift):
    bf16, f32 = jnp.bfloat16, jnp.float32
    vmem, hbm = pl.BlockSpec(memory_space=pltpu.VMEM), pl.BlockSpec(memory_space=pl.ANY)
    return pl.pallas_call(
        layer_kernel,
        out_shape=pltpu.VMEM((SEQ, WIDTH), bf16),
        in_specs=[hbm] * 7 + [vmem] * 5,
        out_specs=vmem,
        scratch_shapes=[
            pltpu.VMEM((SEQ, WIDTH), bf16),
            pltpu.VMEM((NZ, GROUP, 512), bf16),
            pltpu.VMEM((NZ, GROUP, 1024), bf16),
            pltpu.VMEM((NZ, GROUP, 1024), bf16),
            pltpu.VMEM((SEQ, 384), f32),
            pltpu.VMEM((SEQ + 8, 128), f32),
            pltpu.VMEM((SEQ, 128), bf16),
            pltpu.VMEM((2, PARTS, CHUNKS, PART, CHUNK), bf16),
            pltpu.VMEM((2, PARTS, CHUNKS, CORE_ROWS, CHUNK), bf16),
            pltpu.VMEM((2, PARTS, CHUNKS, CORE_ROWS, CHUNK), bf16),
            pltpu.VMEM((2, PARTS, CHUNKS, OWN, CHUNK), bf16),
            pltpu.VMEM((2, PARTS, CHUNKS, OWN, CHUNK), bf16),
            pltpu.VMEM((2, PARTS, CHUNKS, OWN, CHUNK), bf16),
            pltpu.VMEM((PARTS, OWN, WIDTH), f32),
            pltpu.VMEM((SEQ, WIDTH), bf16),
            pltpu.VMEM((SEQ, 1024), bf16),
            pltpu.SemaphoreType.DMA((N_SENDS,)),
            pltpu.SemaphoreType.DMA((N_RECVS,)),
            pltpu.SemaphoreType.DMA((N_LOADS,)),
        ],
        compiler_params=pltpu.CompilerParams(
            collective_id=0, has_side_effects=True, vmem_limit_bytes=60 * 2**20),
    )(tokens, gate_outer, gate_inner, conv_input, mixer_output, up_weight, down_weight, conv_taps,
      mixer_gain.reshape(1, -1), mixer_shift.reshape(1, -1), channel_gain.reshape(1, -1),
      channel_shift.reshape(1, -1))


def solution(mesh):
    weights = P("fs", "tp")
    in_specs = (
        P(("rep", "fs"), None), weights, weights, weights, weights, P(None, "tp"), P(), P(),
        weights, weights, P(), P(),
    )
    out_specs = P(("rep", "fs"), None)
    return jax.shard_map(local, mesh=mesh, in_specs=in_specs, out_specs=out_specs, check_vma=False)
```

```python
import functools

import jax
import jax.numpy as jnp
from jax import lax
from jax.experimental import pallas as pl
from jax.experimental.pallas import tpu as pltpu
from jax.sharding import PartitionSpec as P

residual_scale = 8.0**0.25
norm_epsilon = 1e-05

NZ, NY, NX = 8, 4, 4
SEQ, WIDTH = 512, 2048
ROWS = 64
GROUP = 256
PARTS = 2
PART = SEQ // PARTS
CORE_ROWS, OWN = PART // 2, PART // 8
CHUNKS, CHUNK = 4, 512
NEAR = ("+", "-")
ARRIVAL = (0, 1, -1, 2, -2, 3, -3, 4)

LINK_RATE, LINK_LAT = 46.6e3, 1.9
PAIR_RATE, PAIR_LAT = 500e3, 1.1
BACKLOG = 1.08


PIECES = (
    ("m0", "y", 128, 1), ("m2", "z", 384, 1),
    ("u0", "y", 256, 4), ("u1", "y", 128, 4), ("u2", "z", 640, 4),
    ("d0", "y", 256, 5), ("d1", "y", 256, 5), ("d2", "z", 512, 5),
)
HOPS = {
    "m": {"y": (1.23, 2.17), "yz": (0.63, 0.88, 2.17, 0.68),
     "z": (1.89, 0.6, 1.2, 0.71), "zy": (0.96, 1.71, 1.24, 0.91, 2.1)},
    "u": {"y": (2.25, 1.09), "yz": (4.41, 4.71, 2.85, 4.22),
     "z": (5.36, 1.97, 2.56, 5.09), "zy": (3.67, 2.93, 2.85, 3.49, 2.72)},
    "d": {"y": (3.17, 2.62), "yz": (1.4, 5.34, 5.8, 2.75),
     "z": (1.15, 2.53, 1.97, 4.54), "zy": (2.22, 4.61, 1.89, 4.39, 5.9)},
}


class Op:
    def __init__(self, name, deps, emit, prio, dur=0.0, link=None, nbytes=0, wait=None, latency=0.0):
        self.name, self.deps, self.emit, self.prio = name, deps, emit, prio
        self.dur, self.link, self.nbytes, self.wait = dur, link, nbytes, wait
        self.latency, self.group = latency, None


def plan(ops):
    done, link_free, order, now = {}, {}, [], 0.0
    members = {}
    for op in ops:
        if op.group is not None:
            members.setdefault(op.group, []).append(op.name)
    group_of = {op.name: members[op.group] for op in ops if op.group is not None}
    for op in ops:
        op.deps = list(dict.fromkeys(m for d in op.deps for m in group_of.get(d, [d])))
    left = list(ops)
    while left:
        best = None
        for at, op in enumerate(left):
            if any(d not in done for d in op.deps):
                continue
            ready = max([done[d] for d in op.deps], default=0.0)
            if op.link is not None:
                ready = max(ready, link_free.get(op.link, 0.0) - (BACKLOG if op.prio >= 3 else 1.48 * BACKLOG))
            key = (max(ready, now), op.prio, at)
            if best is None or key < best[0]:
                best = (key, op)
        (start, _, _), op = best
        left.remove(op)
        now = start + (op.dur if op.link is None else 0.03)
        if op.link is None:
            done[op.name] = now + op.latency
        else:
            rate, lat = (PAIR_RATE, PAIR_LAT) if op.link == "c" else (LINK_RATE, LINK_LAT)
            begin = max(now, link_free.get(op.link, 0.0))
            link_free[op.link] = begin + op.nbytes / rate
            done[op.name] = link_free[op.link] + lat
        order.append((start, op))
    return order, done


def layer_kernel(
    tok_hbm, go_hbm, gi_hbm, ci_hbm, mo_hbm, up_hbm, dn_hbm, taps, mgain, mshift, cgain, cshift,
    res,
    tok, wm, wu, wd, proj, prod, conv, pp, so, dr, rl, fr, fd, v, first, hid,
    send_sems, recv_sems, load_sems,
    report=None,
):
    f32, bf16 = jnp.float32, jnp.bfloat16
    rep, fs, tp = lax.axis_index("rep"), lax.axis_index("fs"), lax.axis_index("tp")
    zl, y = lax.div(fs, NY), lax.rem(fs, NY)
    x, c = lax.div(tp, 2), lax.rem(tp, 2)
    z = rep * NZ + zl

    def mod(v, n):
        return lax.rem(v + 2 * n, n)

    def device(dz=0, dy=0, dx=0, dc=0):
        zz = mod(z + dz, 2 * NZ)
        return (
            lax.div(zz, NZ),
            lax.rem(zz, NZ) * NY + mod(y + dy, NY),
            mod(x + dx, NX) * 2 + lax.rem(c + dc, 2),
        )

    peer = {
        "z+": device(dz=1), "z-": device(dz=-1), "y+": device(dy=1), "y-": device(dy=-1),
        "x+": device(dx=1), "x-": device(dx=-1), "c": device(dc=1),
    }
    sign = {"+": 1, "-": -1}

    ops = []
    sends = {}

    send_groups, recv_groups = {}, {}

    def send(name, link, deps, src, dst, landed, nbytes, prio, sent, group=None):
        send_at = send_groups.setdefault(sent[0], len(send_groups))
        recv_at = recv_groups.setdefault(group[0] if group else name, len(recv_groups))

        def copy(s, d):
            return pltpu.make_async_remote_copy(
                src_ref=s, dst_ref=d, send_sem=send_sems.at[send_at], recv_sem=recv_sems.at[recv_at],
                device_id=peer[link], device_id_type=pl.DeviceIdType.MESH,
            )

        all_here = group[1] if group else landed
        sends.setdefault(sent[0], lambda: copy(sent[1](), sent[1]()).wait_send())
        op = Op(
            name, deps, lambda: copy(src(), dst()).start(), prio, link=link, nbytes=nbytes,
            wait=lambda: copy(all_here(), all_here()).wait_recv(),
        )
        op.group = group[0] if group else None
        ops.append(op)

    def compute(name, deps, emit, prio, dur):
        ops.append(Op(name, deps, emit, prio, dur=dur))

    loads = []

    def load(name, src, dst):
        index = len(loads)
        op = Op(name, [], lambda: None, 0, latency=0.5)
        op.wait = lambda: pltpu.make_async_copy(src(), dst(), load_sems.at[index]).wait()
        loads.append(lambda: pltpu.make_async_copy(src(), dst(), load_sems.at[index]).start())
        ops.append(op)

    def own(w, c0, n):
        return lambda: w.at[zl, pl.ds(pl.multiple_of(y * ROWS, ROWS), ROWS), pl.ds(c0, n)]

    load("load.m0", lambda: go_hbm, own(wm, 0, 128))
    load("load.m1", lambda: gi_hbm, own(wm, 128, 128))
    load("load.m2", lambda: ci_hbm, own(wm, 256, 128))
    load("load.m3", lambda: mo_hbm, own(wm, 384, 128))
    load("load.u", lambda: up_hbm, own(wu, 0, 1024))
    load("load.d", lambda: dn_hbm, own(wd, 0, 1024))
    load("load.t", lambda: tok_hbm, lambda: tok)

    def block(w, dz, dy, c0, n, half=None):
        rows, off = (ROWS, 0) if half is None else (ROWS // 2, half * ROWS // 2)

        def view():
            start = pl.multiple_of(mod(y + dy, NY) * ROWS + off, ROWS // 2)
            return w.at[mod(zl + dz, NZ), pl.ds(start, rows), pl.ds(c0, n)]

        return view

    def slab(w, dz, c0, n, half=None):
        rows, off = (GROUP, 0) if half is None else (GROUP // 2, half * GROUP // 2)
        return lambda: w.at[mod(zl + dz, NZ), pl.ds(off, rows), pl.ds(c0, n)]

    ready = {}

    def y_first(tag, w, c0, n, deps, prio):
        size = ROWS * n * 2
        part_of = lambda zs, rows: (lambda: w.at[zs, rows, pl.ds(c0, n)])
        sent_y = ((tag, "Y"), part_of(0, pl.ds(0, 3 * ROWS)))
        sent_z = ((tag, "Z"), part_of(pl.ds(0, 7), pl.ds(0, GROUP)))
        second = ((tag, "Y", 2), part_of(0, pl.ds(0, ROWS)))
        fourth = ((tag, "Z", 4), part_of(0, pl.ds(0, GROUP)))
        for d in "+-":
            s = sign[d]
            b = block(w, 0, 0, c0, n)
            send((tag, "Y", 1, d), "y" + d, deps, b, b, block(w, 0, -s, c0, n), size,
                 HOPS[tag[0]]["y"][0], sent_y)
        for d, half in (("+", 0), ("-", 1)):
            s = sign[d]
            b = block(w, 0, -s, c0, n, half)
            send((tag, "Y", 2, d), "y" + d, [(tag, "Y", 1, d)], b, b, block(w, 0, -2 * s, c0, n, half), size // 2,
                 HOPS[tag[0]]["y"][1], sent_y, second)
        group = [(tag, "Y", h, d) for h in (1, 2) for d in "+-"]
        ready[tag[0], 0] = ready.get((tag[0], 0), []) + group
        for d, half in (("+", 0), ("-", 1)):
            s = sign[d]
            for h in (1, 2, 3, 4):
                part = half if h == 4 else None
                b = slab(w, -s * (h - 1), c0, n, part)
                before = deps + group if h == 1 else [(tag, "Z", h - 1, d)]
                send((tag, "Z", h, d), "z" + d, before, b, b, slab(w, -s * h, c0, n, part),
                     NY * size // (1 if part is None else 2), HOPS[tag[0]]["yz"][h - 1],
                     sent_z, fourth if h == 4 else None)
                dist = 4 if h == 4 else -s * h
                ready[tag[0], dist] = ready.get((tag[0], dist), []) + [(tag, "Z", h, d)]

    def z_first(tag, w, c0, n, deps, prio):
        size = ROWS * n * 2
        part_of = lambda zs, rows: (lambda: w.at[zs, rows, pl.ds(c0, n)])
        sent_z = part_of(0, pl.ds(0, 7 * ROWS // 2))
        sent_y = ((tag, "Y"), part_of(pl.ds(0, 6), pl.ds(0, GROUP)))
        fourth = ((tag, "Z", 4), part_of(0, pl.ds(0, ROWS)))
        for d, half in (("+", 0), ("-", 1)):
            s = sign[d]
            for h in (1, 2, 3, 4):
                part = half if h == 4 else None
                b = block(w, -s * (h - 1), 0, c0, n, part)
                before = deps if h == 1 else [(tag, "Z", h - 1, d)]
                send((tag, "Z", h, d), "z" + d, before, b, b, block(w, -s * h, 0, c0, n, part),
                     size // (1 if part is None else 2), HOPS[tag[0]]["z"][h - 1],
                     ((tag, "Z", d), sent_z), fourth if h == 4 else None)
        for at, dist in enumerate(ARRIVAL):
            here = {0: deps, 4: [(tag, "Z", 4, "+"), (tag, "Z", 4, "-")]}.get(
                dist, [(tag, "Z", abs(dist), NEAR[dist > 0])])
            second = {
                "m": ((tag, "Y", 2, at), part_of(0, pl.ds(0, ROWS))),
                "u": ((tag, "Y", 2), part_of(pl.ds(0, 2), pl.ds(0, GROUP))),
                "d": ((tag, "Y", 2, at // 2), part_of(0, pl.ds(0, 2 * ROWS))),
            }[tag[0]]
            for d, half in (("+", 0), ("-", 1)):
                s = sign[d]
                b = block(w, dist, 0, c0, n)
                send((tag, "Y", 1, d, dist), "y" + d, here, b, b, block(w, dist, -s, c0, n), size,
                     HOPS[tag[0]]["zy"][abs(dist)], sent_y)
                b = block(w, dist, -s, c0, n, half)
                send((tag, "Y", 2, d, dist), "y" + d, [(tag, "Y", 1, d, dist)], b, b,
                     block(w, dist, -2 * s, c0, n, half), size // 2,
                     HOPS[tag[0]]["zy"][abs(dist)], sent_y, second)
            names = here + [(tag, "Y", h, d, dist) for h in (1, 2) for d in "+-"]
            ready[tag[0], dist] = ready.get((tag[0], dist), []) + names

    seen = []
    mixer_loads = ["load.m0", "load.m1", "load.m2", "load.m3"]
    column, loads_of = 0, {"m": mixer_loads, "u": ["load.u"], "d": ["load.d"]}
    for tag, way, n, prio in PIECES:
        w = {"m": wm, "u": wu, "d": wd}[tag[0]]
        if tag[0] not in [t[0] for t in seen]:
            column = 0
        seen.append(tag)
        way = y_first if way == "y" else z_first
        way(tag, w, column, n, loads_of[tag[0]], prio)
        column += n

    def project(first_one, dists):
        def emit():
            for at, dist in enumerate(dists):
                g = mod(zl + dist, NZ)
                term = jnp.dot(
                    tok[:, pl.ds(pl.multiple_of(g * GROUP, GROUP), GROUP)], wm[g, :, 0:384],
                    preferred_element_type=f32)
                if first_one and at == 0:
                    proj[...] = term
                else:
                    proj[...] += term

        return emit

    def convolve():
        prod[0:8, :] = jnp.zeros((8, 128), f32)
        prod[8:, :] = proj[:, 128:256] * proj[:, 256:384]
        total = taps[0:1, :] * prod[6:6 + SEQ, :]
        total = total + taps[1:2, :] * prod[7:7 + SEQ, :]
        total = total + taps[2:3, :] * prod[8:8 + SEQ, :]
        conv[...] = (proj[:, 0:128] * total).astype(bf16)

    compute_after = ["load.t"] + mixer_loads
    for dist in ARRIVAL:
        compute_after = compute_after + ready["m", dist]
        compute(("project", dist), compute_after, project(dist == 0, [dist]), 0, 0.35)
        compute_after = [("project", dist)]
    compute("convolve", compute_after, convolve, 0, 0.7)

    nt = (((1,), (1,)), ((), ()))

    def product(phase, p, k, left, rights):
        for at, right in enumerate(rights):
            pp[phase, p, k, :, at * GROUP:(at + 1) * GROUP] = lax.dot_general(
                left[p * PART:(p + 1) * PART, :], right(), nt, preferred_element_type=f32).astype(bf16)

    def rows_of(dx):
        return pl.ds(pl.multiple_of(mod(x + dx, NX) * OWN, OWN), OWN)

    def core_rows(core):
        return pl.ds(pl.multiple_of(core * CORE_ROWS, CORE_ROWS), CORE_ROWS)

    def seq_rows(p, dx=0, core=None):
        core = c if core is None else core
        return pl.ds(pl.multiple_of(p * PART + core * CORE_ROWS + mod(x + dx, NX) * OWN, OWN), OWN)

    def sum_chunk(phase, p, k, groups, residual, prio):
        t = ("s", phase, p, k)
        d, e = ("+", "-") if k % 2 == 0 else ("-", "+")
        s = sign[d]
        send((t, "pair"), "c", [(t, "product")], lambda: pp.at[phase, p, k, core_rows(1 - c), :],
             lambda: dr.at[phase, p, k], lambda: dr.at[phase, p, k], CORE_ROWS * CHUNK * 2, prio,
             (("s", phase, p, "pair"), lambda: dr.at[phase, p]))

        def add_pair():
            so[phase, p, k] = (
                pp[phase, p, k, core_rows(c), :].astype(f32) + dr[phase, p, k].astype(f32)).astype(bf16)

        compute((t, "add"), [(t, "product"), (t, "pair")], add_pair, prio, 0.06)
        size = OWN * CHUNK * 2
        at = lambda dx: (lambda: so.at[phase, p, k, rows_of(dx), :])
        slot = lambda ref: (lambda: ref.at[phase, p, k])
        sent = (("s", phase, p, "x"), lambda: so.at[phase, p, pl.ds(0, CHUNKS - 1)])
        last = ((t, "last"), lambda: so.at[phase, p, k, pl.ds(0, 2 * OWN), :])
        send((t, "relay"), "x" + d, [(t, "add")], at(2), slot(rl), slot(rl), size, prio, sent)
        send((t, "direct"), "x" + e, [(t, "add")], at(-s), slot(fd), slot(fd), size, prio + 0.5,
             sent, last)

        def add_relay():
            so[phase, p, k, rows_of(s), :] = (
                so[phase, p, k, rows_of(s), :].astype(f32) + rl[phase, p, k].astype(f32)).astype(bf16)

        compute((t, "radd"), [(t, "add"), (t, "relay")], add_relay, prio, 0.03)
        send((t, "final"), "x" + d, [(t, "radd")], at(s), slot(fr), slot(fr), size, prio, sent, last)

        def finish():
            total = so[phase, p, k, rows_of(0), :].astype(f32) + fr[phase, p, k].astype(f32)
            total = total + fd[phase, p, k].astype(f32)
            for at, group in enumerate(groups):
                columns = pl.ds(pl.multiple_of(group() * GROUP, GROUP), GROUP)
                v[p, :, columns] = (residual_scale * residual[seq_rows(p), columns].astype(f32)
                                    + total[:, at * GROUP:(at + 1) * GROUP])

        compute((t, "finish"), [(t, "add"), (t, "final"), (t, "direct")], finish, prio, 0.04)

    def norm(phase, p, gain, shift, dest, prio):
        def emit():
            values = v[p]
            mean = jnp.mean(values, -1, keepdims=True)
            centered = values - mean
            variance = jnp.mean(centered * centered, -1, keepdims=True)
            scaled = centered * lax.rsqrt(variance + norm_epsilon)
            dest[seq_rows(p), :] = (scaled * gain[...] + shift[...]).astype(bf16)

        compute(("norm", phase, p), [(("s", phase, p, k), "finish") for k in range(CHUNKS)], emit, prio, 0.25)

    HALF = WIDTH // 2

    def place(p, dx, h, other=False):
        def view(ref):
            rows = seq_rows(p, dx, 1 - c if other else c)
            return ref.at[rows, :] if h is None else ref.at[rows, pl.ds(h * HALF, HALF)]
        return view

    def gather(phase, p, ref, prio):
        def at(*where):
            return lambda: place(p, *where)(ref)

        t, size, landed = ("g", phase, p), OWN * HALF * 2, []
        start = [("norm", phase, p)]
        first_rows = lambda rows: (lambda: ref.at[pl.ds(0, rows), :])
        sent_x, sent_c = ((t, "x"), first_rows(3 * OWN)), ((t, "c"), first_rows(4 * OWN))
        if phase == 0:
            pairs = [((t, "P"), first_rows(4 * OWN))] * 4
        else:
            pairs = [((t, "P", i), first_rows(rows)) for i, rows in enumerate((OWN, OWN, OWN, OWN))]
        for d, first_half in (("+", 0), ("-", 1)):
            for h in (first_half, 1 - first_half):
                send((t, "A", d, h), "x" + d, start, at(0, h), at(0, h), at(-sign[d], h), size, prio, sent_x)
                landed.append(((t, "A", d, h), (-sign[d], h)))
        send((t, "P"), "c", start, at(0, None), at(0, None), at(0, None, True), 2 * size, prio, sent_c, pairs[0])
        landed.append(((t, "P"), (0, None, True)))
        for d, h in (("+", 0), ("-", 1)):
            b = at(-sign[d], h)
            send((t, "B", d), "x" + d, [(t, "A", d, h)], b, b, at(2, h), size, prio, sent_x)
            landed.append(((t, "B", d), (2, h)))
        for i, (name, dx, h) in enumerate((
                ((t, "A", "+", 0), -1, 0), ((t, "A", "-", 1), 1, 1), ((t, "A", "+", 1), -1, 1),
                ((t, "A", "-", 0), 1, 0), ((t, "B", "+"), 2, 0), ((t, "B", "-"), 2, 1))):
            send((name, "P"), "c", [name], at(dx, h), at(dx, h), at(dx, h, True), size, prio,
                 sent_c, pairs[1 + i // 2])
            landed.append(((name, "P"), (dx, h, True)))
        return landed

    def hidden(p, n):
        rows = pl.ds(p * PART, PART)
        for at in (2 * n, 2 * n + 1):
            columns = pl.ds(at * 256, 256)
            up = jnp.dot(first[rows, :], wu[:, :, columns].reshape(WIDTH, 256), preferred_element_type=f32)
            hid[rows, columns] = jnp.square(jnp.maximum(up, 0.0)).astype(bf16)

    up_ready = ["load.u"] + [n for dist in ARRIVAL for n in ready["u", dist]]
    for p in range(PARTS):
        for k in range(CHUNKS):
            pair = (2 * k, 2 * k + 1)
            compute((("s", 0, p, k), "product"), ["convolve"],
                    functools.partial(product, 0, p, k, conv, [lambda g=g: wm[g, :, 384:512] for g in pair]),
                    0 + p, 0.25)
            sum_chunk(0, p, k, [lambda g=g: g for g in pair], tok, 0 + p)
        norm(0, p, mgain, mshift, first, 0 + p)
        landed = gather(0, p, first, 0 + p)
        for n in range(2):
            compute(("hidden", p, n), [("norm", 0, p)] + [name for name, _ in landed] + up_ready,
                    functools.partial(hidden, p, n), 2 + p, 0.75)
        for k in range(CHUNKS):
            dists = ARRIVAL[2 * k:2 * k + 2]
            groups = [lambda dist=dist: mod(zl + dist, NZ) for dist in dists]
            arrived = [name for dist in dists for name in ready["d", dist]]
            compute((("s", 1, p, k), "product"), [("hidden", p, n) for n in range(2)] + ["load.d"] + arrived,
                    functools.partial(product, 1, p, k, hid, [lambda g=g: wd[g()] for g in groups]),
                    2 + p, 0.5)
            sum_chunk(1, p, k, groups, first, 2 + p)
        norm(1, p, cgain, cshift, res, 2 + p)
        gather(1, p, res, 2 + p)

    order, done = plan(ops)
    if report is not None:
        report(order, done, len(send_groups), len(recv_groups), len(loads))
    assert (len(send_groups), len(recv_groups), len(loads)) == (N_SENDS, N_RECVS, N_LOADS), (
        len(send_groups), len(recv_groups), len(loads))

    for start_load in loads:
        start_load()
    barrier = pltpu.get_barrier_semaphore()
    for link in peer:
        pl.semaphore_signal(barrier, inc=1, device_id=peer[link], device_id_type=pl.DeviceIdType.MESH)
    pl.semaphore_wait(barrier, len(peer))

    by_name = {op.name: op for op in ops}
    waited = set()

    def need(name):
        op = by_name[name]
        key = op.group or name
        if op.wait is not None and key not in waited:
            waited.add(key)
            op.wait()

    for _, op in order:
        for name in op.deps:
            need(name)
        op.emit()
    for op in ops:
        need(op.name)
    for wait in sends.values():
        wait()


N_SENDS, N_RECVS, N_LOADS = 35, 214, 7


def local(tokens, gate_outer, gate_inner, conv_input, mixer_output, conv_taps, mixer_gain,
          mixer_shift, up_weight, down_weight, channel_gain, channel_shift):
    bf16, f32 = jnp.bfloat16, jnp.float32
    vmem, hbm = pl.BlockSpec(memory_space=pltpu.VMEM), pl.BlockSpec(memory_space=pl.ANY)
    return pl.pallas_call(
        layer_kernel,
        out_shape=pltpu.VMEM((SEQ, WIDTH), bf16),
        in_specs=[hbm] * 7 + [vmem] * 5,
        out_specs=vmem,
        scratch_shapes=[
            pltpu.VMEM((SEQ, WIDTH), bf16),
            pltpu.VMEM((NZ, GROUP, 512), bf16),
            pltpu.VMEM((NZ, GROUP, 1024), bf16),
            pltpu.VMEM((NZ, GROUP, 1024), bf16),
            pltpu.VMEM((SEQ, 384), f32),
            pltpu.VMEM((SEQ + 8, 128), f32),
            pltpu.VMEM((SEQ, 128), bf16),
            pltpu.VMEM((2, PARTS, CHUNKS, PART, CHUNK), bf16),
            pltpu.VMEM((2, PARTS, CHUNKS, CORE_ROWS, CHUNK), bf16),
            pltpu.VMEM((2, PARTS, CHUNKS, CORE_ROWS, CHUNK), bf16),
            pltpu.VMEM((2, PARTS, CHUNKS, OWN, CHUNK), bf16),
            pltpu.VMEM((2, PARTS, CHUNKS, OWN, CHUNK), bf16),
            pltpu.VMEM((2, PARTS, CHUNKS, OWN, CHUNK), bf16),
            pltpu.VMEM((PARTS, OWN, WIDTH), f32),
            pltpu.VMEM((SEQ, WIDTH), bf16),
            pltpu.VMEM((SEQ, 1024), bf16),
            pltpu.SemaphoreType.DMA((N_SENDS,)),
            pltpu.SemaphoreType.DMA((N_RECVS,)),
            pltpu.SemaphoreType.DMA((N_LOADS,)),
        ],
        compiler_params=pltpu.CompilerParams(
            collective_id=0, has_side_effects=True, vmem_limit_bytes=60 * 2**20),
    )(tokens, gate_outer, gate_inner, conv_input, mixer_output, up_weight, down_weight, conv_taps,
      mixer_gain.reshape(1, -1), mixer_shift.reshape(1, -1), channel_gain.reshape(1, -1),
      channel_shift.reshape(1, -1))


def solution(mesh):
    weights = P("fs", "tp")
    in_specs = (
        P(("rep", "fs"), None), weights, weights, weights, weights, P(None, "tp"), P(), P(),
        weights, weights, P(), P(),
    )
    out_specs = P(("rep", "fs"), None)
    return jax.shard_map(local, mesh=mesh, in_specs=in_specs, out_specs=out_specs, check_vma=False)
```

```python
import functools

import jax
import jax.numpy as jnp
from jax import lax
from jax.experimental import pallas as pl
from jax.experimental.pallas import tpu as pltpu
from jax.sharding import PartitionSpec as P

residual_scale = 8.0**0.25
norm_epsilon = 1e-05

NZ, NY, NX = 8, 4, 4
SEQ, WIDTH = 512, 2048
ROWS = 64
GROUP = 256
PARTS = 2
PART = SEQ // PARTS
CORE_ROWS, OWN = PART // 2, PART // 8
CHUNKS, CHUNK = 4, 512
NEAR = ("+", "-")
ARRIVAL = (0, 1, -1, 2, -2, 3, -3, 4)
LATE = ((0, 1), (-1, 2), (-2, 3), (-3,), (4,))
DIRECT = (False, False, False, False, True)

LINK_RATE, LINK_LAT = 46.6e3, 1.9
PAIR_RATE, PAIR_LAT = 500e3, 1.1
BACKLOG = 1.08
PATHS = {"c": (PAIR_RATE, PAIR_LAT), "x2": (LINK_RATE, 2.6)}


PIECES = (
    ("m0", "y", 128, 1), ("m2", "z", 384, 1),
    ("u0", "y", 256, 4), ("u1", "y", 128, 4), ("u2", "z", 640, 4),
    ("d0", "y", 256, 5), ("d1", "y", 256, 5), ("d2", "z", 512, 5),
)
HOPS = {
    "m": {"y": (1.23, 2.17), "yz": (0.63, 0.88, 2.17, 0.68),
     "z": (1.89, 0.6, 1.2, 0.71), "zy": (0.96, 1.71, 1.24, 0.91, 2.1)},
    "u": {"y": (2.25, 1.09), "yz": (4.41, 4.71, 2.85, 4.22),
     "z": (5.36, 1.97, 2.56, 5.09), "zy": (3.67, 2.93, 2.85, 3.49, 2.72)},
    "d": {"y": (3.17, 2.62), "yz": (1.4, 5.34, 5.8, 2.75),
     "z": (1.15, 2.53, 1.97, 4.54), "zy": (2.22, 4.61, 1.89, 4.39, 5.9)},
}


class Op:
    def __init__(self, name, deps, emit, prio, dur=0.0, link=None, nbytes=0, wait=None, latency=0.0):
        self.name, self.deps, self.emit, self.prio = name, deps, emit, prio
        self.dur, self.link, self.nbytes, self.wait = dur, link, nbytes, wait
        self.latency, self.group = latency, None


def plan(ops):
    done, link_free, order, now = {}, {}, [], 0.0
    members = {}
    for op in ops:
        if op.group is not None:
            members.setdefault(op.group, []).append(op.name)
    group_of = {op.name: members[op.group] for op in ops if op.group is not None}
    for op in ops:
        op.deps = list(dict.fromkeys(m for d in op.deps for m in group_of.get(d, [d])))
    left = list(ops)
    while left:
        best = None
        for at, op in enumerate(left):
            if any(d not in done for d in op.deps):
                continue
            ready = max([done[d] for d in op.deps], default=0.0)
            if op.link is not None:
                ready = max(ready, link_free.get(op.link, 0.0) - (BACKLOG if op.prio >= 3 else 1.48 * BACKLOG))
            key = (max(ready, now), op.prio, at)
            if best is None or key < best[0]:
                best = (key, op)
        (start, _, _), op = best
        left.remove(op)
        now = start + (op.dur if op.link is None else 0.03)
        if op.link is None:
            done[op.name] = now + op.latency
        else:
            rate, lat = PATHS.get(op.link, (LINK_RATE, LINK_LAT))
            begin = max(now, link_free.get(op.link, 0.0))
            link_free[op.link] = begin + op.nbytes / rate
            done[op.name] = link_free[op.link] + lat
        order.append((start, op))
    return order, done


def layer_kernel(
    tok_hbm, go_hbm, gi_hbm, ci_hbm, mo_hbm, up_hbm, dn_hbm, taps, mgain, mshift, cgain, cshift,
    res,
    tok, wm, wu, wd, proj, prod, conv, pp, so, dr, rl, fr, fd, v, first, hid,
    pp1, dr1, so1, in1, cs1, val, stats, send_sems, recv_sems, load_sems,
    report=None,
):
    f32, bf16 = jnp.float32, jnp.bfloat16
    rep, fs, tp = lax.axis_index("rep"), lax.axis_index("fs"), lax.axis_index("tp")
    zl, y = lax.div(fs, NY), lax.rem(fs, NY)
    x, c = lax.div(tp, 2), lax.rem(tp, 2)
    z = rep * NZ + zl

    def mod(v, n):
        return lax.rem(v + 2 * n, n)

    def device(dz=0, dy=0, dx=0, dc=0):
        zz = mod(z + dz, 2 * NZ)
        return (
            lax.div(zz, NZ),
            lax.rem(zz, NZ) * NY + mod(y + dy, NY),
            mod(x + dx, NX) * 2 + lax.rem(c + dc, 2),
        )

    peer = {
        "z+": device(dz=1), "z-": device(dz=-1), "y+": device(dy=1), "y-": device(dy=-1),
        "x+": device(dx=1), "x-": device(dx=-1), "x2": device(dx=2), "c": device(dc=1),
    }
    sign = {"+": 1, "-": -1}

    ops = []
    sends = {}

    send_groups, recv_groups = {}, {}

    def send(name, link, deps, src, dst, landed, nbytes, prio, sent, group=None):
        send_at = send_groups.setdefault(sent[0], len(send_groups))
        recv_at = recv_groups.setdefault(group[0] if group else name, len(recv_groups))

        def copy(s, d):
            return pltpu.make_async_remote_copy(
                src_ref=s, dst_ref=d, send_sem=send_sems.at[send_at], recv_sem=recv_sems.at[recv_at],
                device_id=peer[link], device_id_type=pl.DeviceIdType.MESH,
            )

        all_here = group[1] if group else landed
        sends.setdefault(sent[0], lambda: copy(sent[1](), sent[1]()).wait_send())
        op = Op(
            name, deps, lambda: copy(src(), dst()).start(), prio, link=link, nbytes=nbytes,
            wait=lambda: copy(all_here(), all_here()).wait_recv(),
        )
        op.group = group[0] if group else None
        ops.append(op)

    def compute(name, deps, emit, prio, dur):
        ops.append(Op(name, deps, emit, prio, dur=dur))

    loads = []

    def load(name, src, dst):
        index = len(loads)
        op = Op(name, [], lambda: None, 0, latency=0.5)
        op.wait = lambda: pltpu.make_async_copy(src(), dst(), load_sems.at[index]).wait()
        loads.append(lambda: pltpu.make_async_copy(src(), dst(), load_sems.at[index]).start())
        ops.append(op)

    def own(w, c0, n):
        return lambda: w.at[zl, pl.ds(pl.multiple_of(y * ROWS, ROWS), ROWS), pl.ds(c0, n)]

    load("load.m0", lambda: go_hbm, own(wm, 0, 128))
    load("load.m1", lambda: gi_hbm, own(wm, 128, 128))
    load("load.m2", lambda: ci_hbm, own(wm, 256, 128))
    load("load.m3", lambda: mo_hbm, own(wm, 384, 128))
    load("load.u", lambda: up_hbm, own(wu, 0, 1024))
    load("load.d", lambda: dn_hbm, own(wd, 0, 1024))
    load("load.t", lambda: tok_hbm, lambda: tok)

    def block(w, dz, dy, c0, n, half=None):
        rows, off = (ROWS, 0) if half is None else (ROWS // 2, half * ROWS // 2)

        def view():
            start = pl.multiple_of(mod(y + dy, NY) * ROWS + off, ROWS // 2)
            return w.at[mod(zl + dz, NZ), pl.ds(start, rows), pl.ds(c0, n)]

        return view

    def slab(w, dz, c0, n, half=None):
        rows, off = (GROUP, 0) if half is None else (GROUP // 2, half * GROUP // 2)
        return lambda: w.at[mod(zl + dz, NZ), pl.ds(off, rows), pl.ds(c0, n)]

    ready = {}

    def y_first(tag, w, c0, n, deps, prio):
        size = ROWS * n * 2
        part_of = lambda zs, rows: (lambda: w.at[zs, rows, pl.ds(c0, n)])
        sent_y = ((tag, "Y"), part_of(0, pl.ds(0, 3 * ROWS)))
        sent_z = ((tag, "Z"), part_of(pl.ds(0, 7), pl.ds(0, GROUP)))
        second = ((tag, "Y", 2), part_of(0, pl.ds(0, ROWS)))
        fourth = ((tag, "Z", 4), part_of(0, pl.ds(0, GROUP)))
        for d in "+-":
            s = sign[d]
            b = block(w, 0, 0, c0, n)
            send((tag, "Y", 1, d), "y" + d, deps, b, b, block(w, 0, -s, c0, n), size,
                 HOPS[tag[0]]["y"][0], sent_y)
        for d, half in (("+", 0), ("-", 1)):
            s = sign[d]
            b = block(w, 0, -s, c0, n, half)
            send((tag, "Y", 2, d), "y" + d, [(tag, "Y", 1, d)], b, b, block(w, 0, -2 * s, c0, n, half), size // 2,
                 HOPS[tag[0]]["y"][1], sent_y, second)
        group = [(tag, "Y", h, d) for h in (1, 2) for d in "+-"]
        ready[tag[0], 0] = ready.get((tag[0], 0), []) + group
        for d, half in (("+", 0), ("-", 1)):
            s = sign[d]
            for h in (1, 2, 3, 4):
                part = half if h == 4 else None
                b = slab(w, -s * (h - 1), c0, n, part)
                before = deps + group if h == 1 else [(tag, "Z", h - 1, d)]
                send((tag, "Z", h, d), "z" + d, before, b, b, slab(w, -s * h, c0, n, part),
                     NY * size // (1 if part is None else 2), HOPS[tag[0]]["yz"][h - 1],
                     sent_z, fourth if h == 4 else None)
                dist = 4 if h == 4 else -s * h
                ready[tag[0], dist] = ready.get((tag[0], dist), []) + [(tag, "Z", h, d)]

    def z_first(tag, w, c0, n, deps, prio):
        size = ROWS * n * 2
        part_of = lambda zs, rows: (lambda: w.at[zs, rows, pl.ds(c0, n)])
        sent_z = part_of(0, pl.ds(0, 7 * ROWS // 2))
        sent_y = ((tag, "Y"), part_of(pl.ds(0, 6), pl.ds(0, GROUP)))
        fourth = ((tag, "Z", 4), part_of(0, pl.ds(0, ROWS)))
        for d, half in (("+", 0), ("-", 1)):
            s = sign[d]
            for h in (1, 2, 3, 4):
                part = half if h == 4 else None
                b = block(w, -s * (h - 1), 0, c0, n, part)
                before = deps if h == 1 else [(tag, "Z", h - 1, d)]
                send((tag, "Z", h, d), "z" + d, before, b, b, block(w, -s * h, 0, c0, n, part),
                     size // (1 if part is None else 2), HOPS[tag[0]]["z"][h - 1],
                     ((tag, "Z", d), sent_z), fourth if h == 4 else None)
        late = {dist: j for j, dists in enumerate(LATE) for dist in dists}
        for at, dist in enumerate(ARRIVAL):
            here = {0: deps, 4: [(tag, "Z", 4, "+"), (tag, "Z", 4, "-")]}.get(
                dist, [(tag, "Z", abs(dist), NEAR[dist > 0])])
            second = {
                "m": ((tag, "Y", 2, at), part_of(0, pl.ds(0, ROWS))),
                "u": ((tag, "Y", 2), part_of(pl.ds(0, 2), pl.ds(0, GROUP))),
                "d": ((tag, "Y", 2, late[dist]), part_of(0, pl.ds(0, ROWS * len(LATE[late[dist]])))),
            }[tag[0]]
            for d, half in (("+", 0), ("-", 1)):
                s = sign[d]
                b = block(w, dist, 0, c0, n)
                send((tag, "Y", 1, d, dist), "y" + d, here, b, b, block(w, dist, -s, c0, n), size,
                     HOPS[tag[0]]["zy"][abs(dist)], sent_y)
                b = block(w, dist, -s, c0, n, half)
                send((tag, "Y", 2, d, dist), "y" + d, [(tag, "Y", 1, d, dist)], b, b,
                     block(w, dist, -2 * s, c0, n, half), size // 2,
                     HOPS[tag[0]]["zy"][abs(dist)], sent_y, second)
            names = here + [(tag, "Y", h, d, dist) for h in (1, 2) for d in "+-"]
            ready[tag[0], dist] = ready.get((tag[0], dist), []) + names

    seen = []
    mixer_loads = ["load.m0", "load.m1", "load.m2", "load.m3"]
    column, loads_of = 0, {"m": mixer_loads, "u": ["load.u"], "d": ["load.d"]}
    for tag, way, n, prio in PIECES:
        w = {"m": wm, "u": wu, "d": wd}[tag[0]]
        if tag[0] not in [t[0] for t in seen]:
            column = 0
        seen.append(tag)
        way = y_first if way == "y" else z_first
        way(tag, w, column, n, loads_of[tag[0]], prio)
        column += n

    def project(first_one, dists):
        def emit():
            for at, dist in enumerate(dists):
                g = mod(zl + dist, NZ)
                term = jnp.dot(
                    tok[:, pl.ds(pl.multiple_of(g * GROUP, GROUP), GROUP)], wm[g, :, 0:384],
                    preferred_element_type=f32)
                if first_one and at == 0:
                    proj[...] = term
                else:
                    proj[...] += term

        return emit

    def convolve():
        prod[0:8, :] = jnp.zeros((8, 128), f32)
        prod[8:, :] = proj[:, 128:256] * proj[:, 256:384]
        total = taps[0:1, :] * prod[6:6 + SEQ, :]
        total = total + taps[1:2, :] * prod[7:7 + SEQ, :]
        total = total + taps[2:3, :] * prod[8:8 + SEQ, :]
        conv[...] = (proj[:, 0:128] * total).astype(bf16)

    compute_after = ["load.t"] + mixer_loads
    for dist in ARRIVAL:
        compute_after = compute_after + ready["m", dist]
        compute(("project", dist), compute_after, project(dist == 0, [dist]), 0, 0.35)
        compute_after = [("project", dist)]
    compute("convolve", compute_after, convolve, 0, 0.7)

    nt = (((1,), (1,)), ((), ()))

    def product(phase, p, k, left, rights):
        for at, right in enumerate(rights):
            pp[phase, p, k, :, at * GROUP:(at + 1) * GROUP] = lax.dot_general(
                left[p * PART:(p + 1) * PART, :], right(), nt, preferred_element_type=f32).astype(bf16)

    def rows_of(dx):
        return pl.ds(pl.multiple_of(mod(x + dx, NX) * OWN, OWN), OWN)

    def core_rows(core):
        return pl.ds(pl.multiple_of(core * CORE_ROWS, CORE_ROWS), CORE_ROWS)

    def seq_rows(p, dx=0, core=None):
        core = c if core is None else core
        return pl.ds(pl.multiple_of(p * PART + core * CORE_ROWS + mod(x + dx, NX) * OWN, OWN), OWN)

    def sum_chunk(phase, p, k, groups, residual, prio):
        t = ("s", phase, p, k)
        d, e = ("+", "-") if k % 2 == 0 else ("-", "+")
        s = sign[d]
        send((t, "pair"), "c", [(t, "product")], lambda: pp.at[phase, p, k, core_rows(1 - c), :],
             lambda: dr.at[phase, p, k], lambda: dr.at[phase, p, k], CORE_ROWS * CHUNK * 2, prio,
             (("s", phase, p, "pair"), lambda: dr.at[phase, p]))

        def add_pair():
            so[phase, p, k] = (
                pp[phase, p, k, core_rows(c), :].astype(f32) + dr[phase, p, k].astype(f32)).astype(bf16)

        compute((t, "add"), [(t, "product"), (t, "pair")], add_pair, prio, 0.06)
        size = OWN * CHUNK * 2
        at = lambda dx: (lambda: so.at[phase, p, k, rows_of(dx), :])
        slot = lambda ref: (lambda: ref.at[phase, p, k])
        sent = (("s", phase, p, "x"), lambda: so.at[phase, p, pl.ds(0, CHUNKS - 1)])
        last = ((t, "last"), lambda: so.at[phase, p, k, pl.ds(0, 2 * OWN), :])
        send((t, "relay"), "x" + d, [(t, "add")], at(2), slot(rl), slot(rl), size, prio, sent)
        send((t, "direct"), "x" + e, [(t, "add")], at(-s), slot(fd), slot(fd), size, prio + 0.5,
             sent, last)

        def add_relay():
            so[phase, p, k, rows_of(s), :] = (
                so[phase, p, k, rows_of(s), :].astype(f32) + rl[phase, p, k].astype(f32)).astype(bf16)

        compute((t, "radd"), [(t, "add"), (t, "relay")], add_relay, prio, 0.03)
        send((t, "final"), "x" + d, [(t, "radd")], at(s), slot(fr), slot(fr), size, prio, sent, last)

        def finish():
            total = so[phase, p, k, rows_of(0), :].astype(f32) + fr[phase, p, k].astype(f32)
            total = total + fd[phase, p, k].astype(f32)
            for at, group in enumerate(groups):
                columns = pl.ds(pl.multiple_of(group() * GROUP, GROUP), GROUP)
                v[p, :, columns] = (residual_scale * residual[seq_rows(p), columns].astype(f32)
                                    + total[:, at * GROUP:(at + 1) * GROUP])

        compute((t, "finish"), [(t, "add"), (t, "final"), (t, "direct")], finish, prio, 0.04)

    def norm(phase, p, gain, shift, dest, prio):
        def emit():
            values = v[p]
            mean = jnp.mean(values, -1, keepdims=True)
            centered = values - mean
            variance = jnp.mean(centered * centered, -1, keepdims=True)
            scaled = centered * lax.rsqrt(variance + norm_epsilon)
            dest[seq_rows(p), :] = (scaled * gain[...] + shift[...]).astype(bf16)

        compute(("norm", phase, p), [(("s", phase, p, k), "finish") for k in range(CHUNKS)], emit, prio, 0.25)

    HALF = WIDTH // 2

    def place(p, dx, h, other=False):
        def view(ref):
            rows = seq_rows(p, dx, 1 - c if other else c)
            return ref.at[rows, :] if h is None else ref.at[rows, pl.ds(h * HALF, HALF)]
        return view

    def gather(phase, p, ref, prio):
        def at(*where):
            return lambda: place(p, *where)(ref)

        t, size, landed = ("g", phase, p), OWN * HALF * 2, []
        start = [("norm", phase, p)]
        first_rows = lambda rows: (lambda: ref.at[pl.ds(0, rows), :])
        sent_x, sent_c = ((t, "x"), first_rows(3 * OWN)), ((t, "c"), first_rows(4 * OWN))
        if phase == 0:
            pairs = [((t, "P"), first_rows(4 * OWN))] * 4
        else:
            pairs = [((t, "P", i), first_rows(rows)) for i, rows in enumerate((OWN, OWN, OWN, OWN))]
        for d, first_half in (("+", 0), ("-", 1)):
            for h in (first_half, 1 - first_half):
                send((t, "A", d, h), "x" + d, start, at(0, h), at(0, h), at(-sign[d], h), size, prio, sent_x)
                landed.append(((t, "A", d, h), (-sign[d], h)))
        send((t, "P"), "c", start, at(0, None), at(0, None), at(0, None, True), 2 * size, prio, sent_c, pairs[0])
        landed.append(((t, "P"), (0, None, True)))
        for d, h in (("+", 0), ("-", 1)):
            b = at(-sign[d], h)
            send((t, "B", d), "x" + d, [(t, "A", d, h)], b, b, at(2, h), size, prio, sent_x)
            landed.append(((t, "B", d), (2, h)))
        for i, (name, dx, h) in enumerate((
                ((t, "A", "+", 0), -1, 0), ((t, "A", "-", 1), 1, 1), ((t, "A", "+", 1), -1, 1),
                ((t, "A", "-", 0), 1, 0), ((t, "B", "+"), 2, 0), ((t, "B", "-"), 2, 1))):
            send((name, "P"), "c", [name], at(dx, h), at(dx, h), at(dx, h, True), size, prio,
                 sent_c, pairs[1 + i // 2])
            landed.append(((name, "P"), (dx, h, True)))
        return landed

    def hidden(p, n):
        rows = pl.ds(p * PART, PART)
        for at in (2 * n, 2 * n + 1):
            columns = pl.ds(at * 256, 256)
            up = jnp.dot(first[rows, :], wu[:, :, columns].reshape(WIDTH, 256), preferred_element_type=f32)
            hid[rows, columns] = jnp.square(jnp.maximum(up, 0.0)).astype(bf16)

    up_ready = ["load.u"] + [n for dist in ARRIVAL for n in ready["u", dist]]
    for p in range(PARTS):
        for k in range(CHUNKS):
            pair = (2 * k, 2 * k + 1)
            compute((("s", 0, p, k), "product"), ["convolve"],
                    functools.partial(product, 0, p, k, conv, [lambda g=g: wm[g, :, 384:512] for g in pair]),
                    0 + p, 0.25)
            sum_chunk(0, p, k, [lambda g=g: g for g in pair], tok, 0 + p)
        norm(0, p, mgain, mshift, first, 0 + p)
        landed = gather(0, p, first, 0 + p)
        for n in range(2):
            compute(("hidden", p, n), [("norm", 0, p)] + [name for name, _ in landed] + up_ready,
                    functools.partial(hidden, p, n), 2 + p, 0.75)

    own_block, half_of = ROWS, SEQ // 2

    def late_rows(dx=0, core=None, rows=own_block, off=0):
        core = c if core is None else core
        start = core * half_of + mod(x + dx, NX) * own_block + off
        return pl.ds(pl.multiple_of(start, own_block // 2), rows)

    def late_half(core):
        return pl.ds(pl.multiple_of(core * half_of, half_of), half_of)

    def in_half(dx):
        return pl.ds(pl.multiple_of(mod(x + dx, NX) * own_block, own_block), own_block)

    def late_chunk(j, dists, direct, prio):
        t, width = ("late", j), GROUP * len(dists)
        wide = pl.ds(0, width)
        groups = [mod(zl + dist, NZ) for dist in dists]
        columns = [pl.ds(pl.multiple_of(g * GROUP, GROUP), GROUP) for g in groups]
        arrived = [name for dist in dists for name in ready["d", dist]]

        def multiply():
            for at, g in enumerate(groups):
                for r in range(2):
                    rows = pl.ds(r * half_of, half_of)
                    pp1[j, rows, at * GROUP:(at + 1) * GROUP] = lax.dot_general(
                        hid[rows, :], wd[g], nt, preferred_element_type=f32).astype(bf16)

        compute((t, "product"), [("hidden", p, n) for p in range(PARTS) for n in range(2)] + ["load.d"] + arrived,
                multiply, prio, 0.5 * len(dists))
        sent_x = ((t, "x"), lambda: cs1.at[j, pl.ds(0, 6 * own_block), wide])
        sent_c = ((t, "c"), lambda: cs1.at[j, :, wide])
        size = own_block * width * 2
        send((t, "pair"), "c", [(t, "product")], lambda: pp1.at[j, late_half(1 - c), wide],
             lambda: dr1.at[j, :, wide], lambda: dr1.at[j, :, wide], NX * size, prio, sent_c)

        def add_pair():
            so1[j, :, wide] = (
                pp1[j, late_half(c), wide].astype(f32) + dr1[j, :, wide].astype(f32)).astype(bf16)

        compute((t, "add"), [(t, "pair")], add_pair, prio, 0.1)
        at = lambda dx: (lambda: so1.at[j, in_half(dx), wide])
        slot = lambda i: (lambda: in1.at[j, i, :, wide])
        d, e = ("+", "-") if j % 2 == 0 else ("-", "+")
        s = sign[d]
        if direct:
            last = ((t, "last"), lambda: so1.at[j, pl.ds(0, 3 * own_block), wide])
            send((t, "far"), "x2", [(t, "add")], at(2), slot(0), slot(0), size, prio, sent_x, last)
            send((t, "plus"), "x+", [(t, "add")], at(1), slot(1), slot(1), size, prio, sent_x, last)
            send((t, "minus"), "x-", [(t, "add")], at(-1), slot(2), slot(2), size, prio, sent_x, last)
            terms, from_others = (0, 1, 2), [(t, "far"), (t, "plus"), (t, "minus")]
        else:
            last = ((t, "last"), lambda: so1.at[j, pl.ds(0, 2 * own_block), wide])
            send((t, "relay"), "x" + d, [(t, "add")], at(2), slot(0), slot(0), size, prio, sent_x)
            send((t, "direct"), "x" + e, [(t, "add")], at(-s), slot(2), slot(2), size, prio + 0.5, sent_x, last)

            def add_relay():
                so1[j, in_half(s), wide] = (
                    so1[j, in_half(s), wide].astype(f32) + in1[j, 0, :, wide].astype(f32)).astype(bf16)

            compute((t, "radd"), [(t, "relay")], add_relay, prio, 0.05)
            send((t, "final"), "x" + d, [(t, "radd")], at(s), slot(1), slot(1), size, prio, sent_x, last)
            terms, from_others = (1, 2), [(t, "final"), (t, "direct")]

        def finish():
            total = so1[j, in_half(0), wide].astype(f32)
            for i in terms:
                total = total + in1[j, i, :, wide].astype(f32)
            cs1[j, late_rows(), wide] = total.astype(bf16)

        compute((t, "finish"), from_others, finish, prio, 0.06)

        def there(*where, **more):
            return lambda: cs1.at[j, late_rows(*where, **more), wide]

        begin = [(t, "finish")]
        paired = ((t, "P"), lambda: cs1.at[j, pl.ds(0, half_of), wide])
        other = 1 - c
        send((t, "A", "+"), "x+", begin, there(0), there(0), there(-1), size, prio, sent_x)
        send((t, "A", "-"), "x-", begin, there(0), there(0), there(1), size, prio, sent_x)
        if direct:
            send((t, "A", "x2"), "x2", begin, there(0), there(0), there(2), size, prio, sent_x)
            far = [(t, "A", "x2")]
        else:
            both = ((t, "B"), there(2))
            for d, off in (("+", 0), ("-", own_block // 2)):
                piece = dict(rows=own_block // 2, off=off)
                b = there(-sign[d], **piece)
                send((t, "B", d), "x" + d, [(t, "A", d)], b, b, there(2, **piece), size // 2, prio, sent_x, both)
            far = [(t, "B", "+"), (t, "B", "-")]
        for dx, after in ((0, begin), (-1, [(t, "A", "+")]), (1, [(t, "A", "-")]), (2, far)):
            send((t, "P", dx), "c", after, there(dx), there(dx), there(dx, other), size, prio, sent_c, paired)

        def count():
            def step(i, _):
                rows = pl.ds(pl.multiple_of(i * 64, 64), 64)
                for at, cols in enumerate(columns):
                    value = (residual_scale * first[rows, cols].astype(f32)
                             + cs1[j, rows, at * GROUP:(at + 1) * GROUP].astype(f32))
                    val[rows, cols] = value
                    if j == 0 and at == 0:
                        stats[0, rows, :] = jnp.mean(value, -1, keepdims=True)
                    value = value - stats[0, rows, :]
                    one = jnp.sum(value, -1, keepdims=True)
                    two = jnp.sum(value * value, -1, keepdims=True)
                    if j == 0 and at == 0:
                        stats[1, rows, :], stats[2, rows, :] = one, two
                    else:
                        stats[1, rows, :] += one
                        stats[2, rows, :] += two
                return 0

            lax.fori_loop(0, SEQ // 64, step, 0)

        compute((t, "count"), begin + far + [(t, "P", dx) for dx in (0, -1, 1, 2)]
                + ([("late", j - 1, "count")] if j else []), count, prio, 0.3 * len(dists))
        ops[-1].name = ("late", j, "count")

    for j, dists in enumerate(LATE):
        late_chunk(j, dists, DIRECT[j], 2 + 0.1 * j)

    def finish_norm():
        def step(i, _):
            rows = pl.ds(pl.multiple_of(i * 64, 64), 64)
            off = stats[1, rows, :] * (1.0 / WIDTH)
            variance = jnp.maximum(stats[2, rows, :] * (1.0 / WIDTH) - off * off, 0.0)
            scale = lax.rsqrt(variance + norm_epsilon)
            centered = val[rows, :] - (stats[0, rows, :] + off)
            res[rows, :] = (centered * scale * cgain[...] + cshift[...]).astype(bf16)
            return 0

        lax.fori_loop(0, SEQ // 64, step, 0)

    compute("finish_norm", [("late", j, "count") for j in range(len(LATE))], finish_norm, 0, 1.2)

    order, done = plan(ops)
    if report is not None:
        report(order, done, len(send_groups), len(recv_groups), len(loads))
    assert (len(send_groups), len(recv_groups), len(loads)) == (N_SENDS, N_RECVS, N_LOADS), (
        len(send_groups), len(recv_groups), len(loads))

    for start_load in loads:
        start_load()
    barrier = pltpu.get_barrier_semaphore()
    for link in peer:
        pl.semaphore_signal(barrier, inc=1, device_id=peer[link], device_id_type=pl.DeviceIdType.MESH)
    pl.semaphore_wait(barrier, len(peer))

    by_name = {op.name: op for op in ops}
    waited = set()

    def need(name):
        op = by_name[name]
        key = op.group or name
        if op.wait is not None and key not in waited:
            waited.add(key)
            op.wait()

    for _, op in order:
        for name in op.deps:
            need(name)
        op.emit()
    for op in ops:
        need(op.name)
    for wait in sends.values():
        wait()


N_SENDS, N_RECVS, N_LOADS = 37, 205, 7


def local(tokens, gate_outer, gate_inner, conv_input, mixer_output, conv_taps, mixer_gain,
          mixer_shift, up_weight, down_weight, channel_gain, channel_shift):
    bf16, f32 = jnp.bfloat16, jnp.float32
    vmem, hbm = pl.BlockSpec(memory_space=pltpu.VMEM), pl.BlockSpec(memory_space=pl.ANY)
    return pl.pallas_call(
        layer_kernel,
        out_shape=pltpu.VMEM((SEQ, WIDTH), bf16),
        in_specs=[hbm] * 7 + [vmem] * 5,
        out_specs=vmem,
        scratch_shapes=[
            pltpu.VMEM((SEQ, WIDTH), bf16),
            pltpu.VMEM((NZ, GROUP, 512), bf16),
            pltpu.VMEM((NZ, GROUP, 1024), bf16),
            pltpu.VMEM((NZ, GROUP, 1024), bf16),
            pltpu.VMEM((SEQ, 384), f32),
            pltpu.VMEM((SEQ + 8, 128), f32),
            pltpu.VMEM((SEQ, 128), bf16),
            pltpu.VMEM((1, PARTS, CHUNKS, PART, CHUNK), bf16),
            pltpu.VMEM((1, PARTS, CHUNKS, CORE_ROWS, CHUNK), bf16),
            pltpu.VMEM((1, PARTS, CHUNKS, CORE_ROWS, CHUNK), bf16),
            pltpu.VMEM((1, PARTS, CHUNKS, OWN, CHUNK), bf16),
            pltpu.VMEM((1, PARTS, CHUNKS, OWN, CHUNK), bf16),
            pltpu.VMEM((1, PARTS, CHUNKS, OWN, CHUNK), bf16),
            pltpu.VMEM((PARTS, OWN, WIDTH), f32),
            pltpu.VMEM((SEQ, WIDTH), bf16),
            pltpu.VMEM((SEQ, 1024), bf16),
            pltpu.VMEM((len(LATE), SEQ, CHUNK), bf16),
            pltpu.VMEM((len(LATE), SEQ // 2, CHUNK), bf16),
            pltpu.VMEM((len(LATE), SEQ // 2, CHUNK), bf16),
            pltpu.VMEM((len(LATE), 3, ROWS, CHUNK), bf16),
            pltpu.VMEM((len(LATE), SEQ, CHUNK), bf16),
            pltpu.VMEM((SEQ, WIDTH), f32),
            pltpu.VMEM((3, SEQ, 1), f32),
            pltpu.SemaphoreType.DMA((N_SENDS,)),
            pltpu.SemaphoreType.DMA((N_RECVS,)),
            pltpu.SemaphoreType.DMA((N_LOADS,)),
        ],
        compiler_params=pltpu.CompilerParams(
            collective_id=0, has_side_effects=True, vmem_limit_bytes=56 * 2**20),
    )(tokens, gate_outer, gate_inner, conv_input, mixer_output, up_weight, down_weight, conv_taps,
      mixer_gain.reshape(1, -1), mixer_shift.reshape(1, -1), channel_gain.reshape(1, -1),
      channel_shift.reshape(1, -1))


def solution(mesh):
    weights = P("fs", "tp")
    in_specs = (
        P(("rep", "fs"), None), weights, weights, weights, weights, P(None, "tp"), P(), P(),
        weights, weights, P(), P(),
    )
    out_specs = P(("rep", "fs"), None)
    return jax.shard_map(local, mesh=mesh, in_specs=in_specs, out_specs=out_specs, check_vma=False)
```

```python
import functools

import jax
import jax.numpy as jnp
from jax import lax
from jax.experimental import pallas as pl
from jax.experimental.pallas import tpu as pltpu
from jax.sharding import PartitionSpec as P

residual_scale = 8.0**0.25
norm_epsilon = 1e-05

NZ, NY, NX = 8, 4, 4
SEQ, WIDTH = 512, 2048
ROWS = 64
GROUP = 256
PARTS = 2
PART = SEQ // PARTS
CORE_ROWS, OWN = PART // 2, PART // 8
CHUNKS, CHUNK = 4, 512
NEAR = ("+", "-")
ARRIVAL = (0, 1, -1, 2, -2, 3, -3, 4)
LATE = ((0, 1), (-1, 2), (-2, 3), (-3,), (4,))
DIRECT = (False, False, False, True, True)

LINK_RATE, LINK_LAT = 46.6e3, 1.9
PAIR_RATE, PAIR_LAT = 500e3, 1.1
BACKLOG = 2.39
PATHS = {"c": (PAIR_RATE, PAIR_LAT), "x2": (LINK_RATE, 2.6)}


PIECES = (
    ("m0", "y", 128, 1),
    ("m2", "z", 384, 1),
    ("u0", "y", 128, 4),
    ("u1", "y", 256, 4),
    ("u2", "z", 384, 4),
    ("u3", "z", 256, 4),
    ("d0", "y", 256, 5),
    ("d1", "y", 256, 5),
    ("d2", "z", 512, 5),
)
HOPS = {
    "m": {"y": (2.13, 0.62), "yz": (5.5, 0.56, 5.79, 3.68),
          "z": (1.2, 3.12, 3.32, 4.69), "zy": (4.31, 4.14, 4.44, 5.8, 5.47)},
    "u": {"y": (4.44, 2.55), "yz": (6, 3.2, 6, 1.93),
          "z": (0.3, 5.81, 6, 3.59), "zy": (0.72, 0.66, 0.77, 6, 1.06)},
    "d": {"y": (4.84, 3.77), "yz": (2.16, 3.17, 1.76, 5.74),
          "z": (0.3, 3.82, 4.28, 6), "zy": (3.88, 1.07, 5.66, 2.05, 2.8)},
}
EARLIEST = {"uz": 7.5, "dy": 8.8, "dz": 15.2}


class Op:
    def __init__(self, name, deps, emit, prio, dur=0.0, link=None, nbytes=0, wait=None, latency=0.0):
        self.name, self.deps, self.emit, self.prio = name, deps, emit, prio
        self.dur, self.link, self.nbytes, self.wait = dur, link, nbytes, wait
        self.latency, self.group, self.earliest = latency, None, 0.0


def plan(ops):
    done, link_free, order, now = {}, {}, [], 0.0
    members = {}
    for op in ops:
        if op.group is not None:
            members.setdefault(op.group, []).append(op.name)
    group_of = {op.name: members[op.group] for op in ops if op.group is not None}
    for op in ops:
        op.deps = list(dict.fromkeys(m for d in op.deps for m in group_of.get(d, [d])))
    left = list(ops)
    while left:
        best = None
        for at, op in enumerate(left):
            if any(d not in done for d in op.deps):
                continue
            ready = max([done[d] for d in op.deps] + [op.earliest])
            if op.link is not None:
                ready = max(ready, link_free.get(op.link, 0.0) - (BACKLOG if op.prio >= 3 else 0.65 * BACKLOG))
            key = (max(ready, now), op.prio, at)
            if best is None or key < best[0]:
                best = (key, op)
        (start, _, _), op = best
        left.remove(op)
        now = start + (op.dur if op.link is None else 0.03)
        if op.link is None:
            done[op.name] = now + op.latency
        else:
            rate, lat = PATHS.get(op.link, (LINK_RATE, LINK_LAT))
            begin = max(now, link_free.get(op.link, 0.0))
            link_free[op.link] = begin + op.nbytes / rate
            done[op.name] = link_free[op.link] + lat
        order.append((start, op))
    return order, done


def layer_kernel(
    tok_hbm, go_hbm, gi_hbm, ci_hbm, mo_hbm, up_hbm, dn_hbm, taps, mgain, mshift, cgain, cshift,
    res,
    tok, wm, wu, wd, proj, prod, conv, pp, so, dr, rl, fr, fd, v, first, hid,
    pp1, dr1, so1, in1, cs1, val, stats, send_sems, recv_sems, load_sems,
    report=None,
):
    f32, bf16 = jnp.float32, jnp.bfloat16
    rep, fs, tp = lax.axis_index("rep"), lax.axis_index("fs"), lax.axis_index("tp")
    zl, y = lax.div(fs, NY), lax.rem(fs, NY)
    x, c = lax.div(tp, 2), lax.rem(tp, 2)
    z = rep * NZ + zl

    def mod(v, n):
        return lax.rem(v + 2 * n, n)

    def device(dz=0, dy=0, dx=0, dc=0):
        zz = mod(z + dz, 2 * NZ)
        return (
            lax.div(zz, NZ),
            lax.rem(zz, NZ) * NY + mod(y + dy, NY),
            mod(x + dx, NX) * 2 + lax.rem(c + dc, 2),
        )

    peer = {
        "z+": device(dz=1), "z-": device(dz=-1), "y+": device(dy=1), "y-": device(dy=-1),
        "x+": device(dx=1), "x-": device(dx=-1), "x2": device(dx=2), "c": device(dc=1),
    }
    sign = {"+": 1, "-": -1}

    ops = []
    sends = {}

    send_groups, recv_groups = {}, {}

    def send(name, link, deps, src, dst, landed, nbytes, prio, sent, group=None):
        send_at = send_groups.setdefault(sent[0], len(send_groups))
        recv_at = recv_groups.setdefault(group[0] if group else name, len(recv_groups))

        def copy(s, d):
            return pltpu.make_async_remote_copy(
                src_ref=s, dst_ref=d, send_sem=send_sems.at[send_at], recv_sem=recv_sems.at[recv_at],
                device_id=peer[link], device_id_type=pl.DeviceIdType.MESH,
            )

        all_here = group[1] if group else landed
        sends.setdefault(sent[0], lambda: copy(sent[1](), sent[1]()).wait_send())
        op = Op(
            name, deps, lambda: copy(src(), dst()).start(), prio, link=link, nbytes=nbytes,
            wait=lambda: copy(all_here(), all_here()).wait_recv(),
        )
        op.group = group[0] if group else None
        ops.append(op)

    def compute(name, deps, emit, prio, dur):
        ops.append(Op(name, deps, emit, prio, dur=dur))

    loads = []

    def load(name, src, dst):
        index = len(loads)
        op = Op(name, [], lambda: None, 0, latency=0.5)
        op.wait = lambda: pltpu.make_async_copy(src(), dst(), load_sems.at[index]).wait()
        loads.append(lambda: pltpu.make_async_copy(src(), dst(), load_sems.at[index]).start())
        ops.append(op)

    def own(w, c0, n):
        return lambda: w.at[zl, pl.ds(pl.multiple_of(y * ROWS, ROWS), ROWS), pl.ds(c0, n)]

    load("load.m0", lambda: go_hbm, own(wm, 0, 128))
    load("load.m1", lambda: gi_hbm, own(wm, 128, 128))
    load("load.m2", lambda: ci_hbm, own(wm, 256, 128))
    load("load.m3", lambda: mo_hbm, own(wm, 384, 128))
    load("load.u", lambda: up_hbm, own(wu, 0, 1024))
    load("load.d", lambda: dn_hbm, own(wd, 0, 1024))
    load("load.t", lambda: tok_hbm, lambda: tok)

    def block(w, dz, dy, c0, n, half=None):
        rows, off = (ROWS, 0) if half is None else (ROWS // 2, half * ROWS // 2)

        def view():
            start = pl.multiple_of(mod(y + dy, NY) * ROWS + off, ROWS // 2)
            return w.at[mod(zl + dz, NZ), pl.ds(start, rows), pl.ds(c0, n)]

        return view

    def slab(w, dz, c0, n, half=None):
        rows, off = (GROUP, 0) if half is None else (GROUP // 2, half * GROUP // 2)
        return lambda: w.at[mod(zl + dz, NZ), pl.ds(off, rows), pl.ds(c0, n)]

    ready = {}

    def y_first(tag, w, c0, n, deps, prio):
        size = ROWS * n * 2
        part_of = lambda zs, rows: (lambda: w.at[zs, rows, pl.ds(c0, n)])
        sent_y = ((tag, "Y"), part_of(0, pl.ds(0, 3 * ROWS)))
        sent_z = ((tag, "Z"), part_of(pl.ds(0, 7), pl.ds(0, GROUP)))
        second = ((tag, "Y", 2), part_of(0, pl.ds(0, ROWS)))
        fourth = ((tag, "Z", 4), part_of(0, pl.ds(0, GROUP)))
        for d in "+-":
            s = sign[d]
            b = block(w, 0, 0, c0, n)
            send((tag, "Y", 1, d), "y" + d, deps, b, b, block(w, 0, -s, c0, n), size,
                 HOPS[tag[0]]["y"][0], sent_y)
        for d, half in (("+", 0), ("-", 1)):
            s = sign[d]
            b = block(w, 0, -s, c0, n, half)
            send((tag, "Y", 2, d), "y" + d, [(tag, "Y", 1, d)], b, b, block(w, 0, -2 * s, c0, n, half), size // 2,
                 HOPS[tag[0]]["y"][1], sent_y, second)
        group = [(tag, "Y", h, d) for h in (1, 2) for d in "+-"]
        ready[tag[0], 0] = ready.get((tag[0], 0), []) + group
        for d, half in (("+", 0), ("-", 1)):
            s = sign[d]
            for h in (1, 2, 3, 4):
                part = half if h == 4 else None
                b = slab(w, -s * (h - 1), c0, n, part)
                before = deps + group if h == 1 else [(tag, "Z", h - 1, d)]
                send((tag, "Z", h, d), "z" + d, before, b, b, slab(w, -s * h, c0, n, part),
                     NY * size // (1 if part is None else 2), HOPS[tag[0]]["yz"][h - 1],
                     sent_z, fourth if h == 4 else None)
                dist = 4 if h == 4 else -s * h
                ready[tag[0], dist] = ready.get((tag[0], dist), []) + [(tag, "Z", h, d)]

    def z_first(tag, w, c0, n, deps, prio):
        size = ROWS * n * 2
        part_of = lambda zs, rows: (lambda: w.at[zs, rows, pl.ds(c0, n)])
        sent_z = part_of(0, pl.ds(0, 7 * ROWS // 2))
        sent_y = ((tag, "Y"), part_of(pl.ds(0, 6), pl.ds(0, GROUP)))
        fourth = ((tag, "Z", 4), part_of(0, pl.ds(0, ROWS)))
        for d, half in (("+", 0), ("-", 1)):
            s = sign[d]
            for h in (1, 2, 3, 4):
                part = half if h == 4 else None
                b = block(w, -s * (h - 1), 0, c0, n, part)
                before = deps if h == 1 else [(tag, "Z", h - 1, d)]
                send((tag, "Z", h, d), "z" + d, before, b, b, block(w, -s * h, 0, c0, n, part),
                     size // (1 if part is None else 2), HOPS[tag[0]]["z"][h - 1],
                     ((tag, "Z", d), sent_z), fourth if h == 4 else None)
        late = {dist: j for j, dists in enumerate(LATE) for dist in dists}
        for at, dist in enumerate(ARRIVAL):
            here = {0: deps, 4: [(tag, "Z", 4, "+"), (tag, "Z", 4, "-")]}.get(
                dist, [(tag, "Z", abs(dist), NEAR[dist > 0])])
            second = {
                "m": ((tag, "Y", 2, at), part_of(0, pl.ds(0, ROWS))),
                "u": ((tag, "Y", 2), part_of(pl.ds(0, 2), pl.ds(0, GROUP))),
                "d": ((tag, "Y", 2, late[dist]), part_of(0, pl.ds(0, ROWS * len(LATE[late[dist]])))),
            }[tag[0]]
            for d, half in (("+", 0), ("-", 1)):
                s = sign[d]
                b = block(w, dist, 0, c0, n)
                send((tag, "Y", 1, d, dist), "y" + d, here, b, b, block(w, dist, -s, c0, n), size,
                     HOPS[tag[0]]["zy"][abs(dist)], sent_y)
                b = block(w, dist, -s, c0, n, half)
                send((tag, "Y", 2, d, dist), "y" + d, [(tag, "Y", 1, d, dist)], b, b,
                     block(w, dist, -2 * s, c0, n, half), size // 2,
                     HOPS[tag[0]]["zy"][abs(dist)], sent_y, second)
            names = here + [(tag, "Y", h, d, dist) for h in (1, 2) for d in "+-"]
            ready[tag[0], dist] = ready.get((tag[0], dist), []) + names

    seen = []
    mixer_loads = ["load.m0", "load.m1", "load.m2", "load.m3"]
    column, loads_of = 0, {"m": mixer_loads, "u": ["load.u"], "d": ["load.d"]}
    for tag, way, n, prio in PIECES:
        w = {"m": wm, "u": wu, "d": wd}[tag[0]]
        if tag[0] not in [t[0] for t in seen]:
            column = 0
        seen.append(tag)
        way = y_first if way == "y" else z_first
        way(tag, w, column, n, loads_of[tag[0]], prio)
        column += n

    def project(first_one, dists):
        def emit():
            for at, dist in enumerate(dists):
                g = mod(zl + dist, NZ)
                term = jnp.dot(
                    tok[:, pl.ds(pl.multiple_of(g * GROUP, GROUP), GROUP)], wm[g, :, 0:384],
                    preferred_element_type=f32)
                if first_one and at == 0:
                    proj[...] = term
                else:
                    proj[...] += term

        return emit

    def convolve():
        prod[0:8, :] = jnp.zeros((8, 128), f32)
        prod[8:, :] = proj[:, 128:256] * proj[:, 256:384]
        total = taps[0:1, :] * prod[6:6 + SEQ, :]
        total = total + taps[1:2, :] * prod[7:7 + SEQ, :]
        total = total + taps[2:3, :] * prod[8:8 + SEQ, :]
        conv[...] = (proj[:, 0:128] * total).astype(bf16)

    compute_after = ["load.t"] + mixer_loads
    for dist in ARRIVAL:
        compute_after = compute_after + ready["m", dist]
        compute(("project", dist), compute_after, project(dist == 0, [dist]), 0, 0.35)
        compute_after = [("project", dist)]
    compute("convolve", compute_after, convolve, 0, 0.7)

    nt = (((1,), (1,)), ((), ()))

    def product(phase, p, k, left, rights):
        for at, right in enumerate(rights):
            pp[phase, p, k, :, at * GROUP:(at + 1) * GROUP] = lax.dot_general(
                left[p * PART:(p + 1) * PART, :], right(), nt, preferred_element_type=f32).astype(bf16)

    def rows_of(dx):
        return pl.ds(pl.multiple_of(mod(x + dx, NX) * OWN, OWN), OWN)

    def core_rows(core):
        return pl.ds(pl.multiple_of(core * CORE_ROWS, CORE_ROWS), CORE_ROWS)

    def seq_rows(p, dx=0, core=None):
        core = c if core is None else core
        return pl.ds(pl.multiple_of(p * PART + core * CORE_ROWS + mod(x + dx, NX) * OWN, OWN), OWN)

    def sum_chunk(phase, p, k, groups, residual, prio):
        t = ("s", phase, p, k)
        d, e = ("+", "-") if k % 2 == 0 else ("-", "+")
        s = sign[d]
        send((t, "pair"), "c", [(t, "product")], lambda: pp.at[phase, p, k, core_rows(1 - c), :],
             lambda: dr.at[phase, p, k], lambda: dr.at[phase, p, k], CORE_ROWS * CHUNK * 2, prio,
             (("s", phase, p, "pair"), lambda: dr.at[phase, p]))

        def add_pair():
            so[phase, p, k] = (
                pp[phase, p, k, core_rows(c), :].astype(f32) + dr[phase, p, k].astype(f32)).astype(bf16)

        compute((t, "add"), [(t, "product"), (t, "pair")], add_pair, prio, 0.06)
        size = OWN * CHUNK * 2
        at = lambda dx: (lambda: so.at[phase, p, k, rows_of(dx), :])
        slot = lambda ref: (lambda: ref.at[phase, p, k])
        sent = (("s", phase, p, "x"), lambda: so.at[phase, p, pl.ds(0, CHUNKS - 1)])
        last = ((t, "last"), lambda: so.at[phase, p, k, pl.ds(0, 2 * OWN), :])
        send((t, "relay"), "x" + d, [(t, "add")], at(2), slot(rl), slot(rl), size, prio, sent)
        send((t, "direct"), "x" + e, [(t, "add")], at(-s), slot(fd), slot(fd), size, prio + 0.5,
             sent, last)

        def add_relay():
            so[phase, p, k, rows_of(s), :] = (
                so[phase, p, k, rows_of(s), :].astype(f32) + rl[phase, p, k].astype(f32)).astype(bf16)

        compute((t, "radd"), [(t, "add"), (t, "relay")], add_relay, prio, 0.03)
        send((t, "final"), "x" + d, [(t, "radd")], at(s), slot(fr), slot(fr), size, prio, sent, last)

        def finish():
            total = so[phase, p, k, rows_of(0), :].astype(f32) + fr[phase, p, k].astype(f32)
            total = total + fd[phase, p, k].astype(f32)
            for at, group in enumerate(groups):
                columns = pl.ds(pl.multiple_of(group() * GROUP, GROUP), GROUP)
                v[p, :, columns] = (residual_scale * residual[seq_rows(p), columns].astype(f32)
                                    + total[:, at * GROUP:(at + 1) * GROUP])

        compute((t, "finish"), [(t, "add"), (t, "final"), (t, "direct")], finish, prio, 0.04)

    def norm(phase, p, gain, shift, dest, prio):
        def emit():
            values = v[p]
            mean = jnp.mean(values, -1, keepdims=True)
            centered = values - mean
            variance = jnp.mean(centered * centered, -1, keepdims=True)
            scaled = centered * lax.rsqrt(variance + norm_epsilon)
            dest[seq_rows(p), :] = (scaled * gain[...] + shift[...]).astype(bf16)

        compute(("norm", phase, p), [(("s", phase, p, k), "finish") for k in range(CHUNKS)], emit, prio, 0.25)

    HALF = WIDTH // 2

    def place(p, dx, h, other=False):
        def view(ref):
            rows = seq_rows(p, dx, 1 - c if other else c)
            return ref.at[rows, :] if h is None else ref.at[rows, pl.ds(h * HALF, HALF)]
        return view

    def gather(phase, p, ref, prio):
        def at(*where):
            return lambda: place(p, *where)(ref)

        t, size, landed = ("g", phase, p), OWN * HALF * 2, []
        start = [("norm", phase, p)]
        first_rows = lambda rows: (lambda: ref.at[pl.ds(0, rows), :])
        sent_x, sent_c = ((t, "x"), first_rows(3 * OWN)), ((t, "c"), first_rows(4 * OWN))
        if phase == 0:
            pairs = [((t, "P"), first_rows(4 * OWN))] * 4
        else:
            pairs = [((t, "P", i), first_rows(rows)) for i, rows in enumerate((OWN, OWN, OWN, OWN))]
        for d, first_half in (("+", 0), ("-", 1)):
            for h in (first_half, 1 - first_half):
                send((t, "A", d, h), "x" + d, start, at(0, h), at(0, h), at(-sign[d], h), size, prio, sent_x)
                landed.append(((t, "A", d, h), (-sign[d], h)))
        send((t, "P"), "c", start, at(0, None), at(0, None), at(0, None, True), 2 * size, prio, sent_c, pairs[0])
        landed.append(((t, "P"), (0, None, True)))
        for d, h in (("+", 0), ("-", 1)):
            b = at(-sign[d], h)
            send((t, "B", d), "x" + d, [(t, "A", d, h)], b, b, at(2, h), size, prio, sent_x)
            landed.append(((t, "B", d), (2, h)))
        for i, (name, dx, h) in enumerate((
                ((t, "A", "+", 0), -1, 0), ((t, "A", "-", 1), 1, 1), ((t, "A", "+", 1), -1, 1),
                ((t, "A", "-", 0), 1, 0), ((t, "B", "+"), 2, 0), ((t, "B", "-"), 2, 1))):
            send((name, "P"), "c", [name], at(dx, h), at(dx, h), at(dx, h, True), size, prio,
                 sent_c, pairs[1 + i // 2])
            landed.append(((name, "P"), (dx, h, True)))
        return landed

    def hidden(p, n):
        rows = pl.ds(p * PART, PART)
        for at in (2 * n, 2 * n + 1):
            columns = pl.ds(at * 256, 256)
            up = jnp.dot(first[rows, :], wu[:, :, columns].reshape(WIDTH, 256), preferred_element_type=f32)
            hid[rows, columns] = jnp.square(jnp.maximum(up, 0.0)).astype(bf16)

    up_ready = ["load.u"] + [n for dist in ARRIVAL for n in ready["u", dist]]
    for p in range(PARTS):
        for k in range(CHUNKS):
            pair = (2 * k, 2 * k + 1)
            compute((("s", 0, p, k), "product"), ["convolve"],
                    functools.partial(product, 0, p, k, conv, [lambda g=g: wm[g, :, 384:512] for g in pair]),
                    0 + p, 0.25)
            sum_chunk(0, p, k, [lambda g=g: g for g in pair], tok, 0 + p)
        norm(0, p, mgain, mshift, first, 0 + p)
        landed = gather(0, p, first, 0 + p)
        for n in range(2):
            compute(("hidden", p, n), [("norm", 0, p)] + [name for name, _ in landed] + up_ready,
                    functools.partial(hidden, p, n), 2 + p, 0.75)

    own_block, half_of = OWN, CORE_ROWS

    def late_rows(dx=0, core=None, rows=own_block, off=0):
        core = c if core is None else core
        start = core * half_of + mod(x + dx, NX) * own_block + off
        return pl.ds(pl.multiple_of(start, own_block // 2), rows)

    def late_half(core):
        return pl.ds(pl.multiple_of(core * half_of, half_of), half_of)

    def in_half(dx):
        return pl.ds(pl.multiple_of(mod(x + dx, NX) * own_block, own_block), own_block)

    def late_chunk(p, j, dists, direct, prio):
        t, width = ("late", p, j), GROUP * len(dists)
        wide = pl.ds(0, width)
        groups = [mod(zl + dist, NZ) for dist in dists]
        columns = [pl.ds(pl.multiple_of(g * GROUP, GROUP), GROUP) for g in groups]
        arrived = [name for dist in dists for name in ready["d", dist]]

        def multiply():
            for at, g in enumerate(groups):
                for r in range(1, -1, -1) if len(groups) == 1 else (None,):
                    size, start = (PART, 0) if r is None else (half_of, r * half_of)
                    pp1[p, j, pl.ds(start, size), at * GROUP:(at + 1) * GROUP] = lax.dot_general(
                        hid[pl.ds(p * PART + start, size), :], wd[g], nt, preferred_element_type=f32).astype(bf16)

        compute((t, "product"), [("hidden", p, n) for n in range(2)] + ["load.d"] + arrived,
                multiply, prio, 0.25 * len(dists))
        sent_x = ((t, "x"), lambda: cs1.at[p, j, pl.ds(0, 6 * own_block), wide])
        sent_c = ((t, "c"), lambda: cs1.at[p, j, :, wide])
        size = own_block * width * 2
        send((t, "pair"), "c", [(t, "product")], lambda: pp1.at[p, j, late_half(1 - c), wide],
             lambda: dr1.at[p, j, :, wide], lambda: dr1.at[p, j, :, wide], NX * size, prio, sent_c)

        def add_pair():
            so1[p, j, :, wide] = (
                pp1[p, j, late_half(c), wide].astype(f32) + dr1[p, j, :, wide].astype(f32)).astype(bf16)

        compute((t, "add"), [(t, "pair")], add_pair, prio, 0.1)
        at = lambda dx: (lambda: so1.at[p, j, in_half(dx), wide])
        slot = lambda i: (lambda: in1.at[p, j, i, :, wide])
        d, e = ("+", "-") if j % 2 == 0 else ("-", "+")
        s = sign[d]
        if direct:
            last = ((t, "last"), lambda: so1.at[p, j, pl.ds(0, 3 * own_block), wide])
            send((t, "far"), "x2", [(t, "add")], at(2), slot(0), slot(0), size, prio, sent_x, last)
            send((t, "plus"), "x+", [(t, "add")], at(1), slot(1), slot(1), size, prio, sent_x, last)
            send((t, "minus"), "x-", [(t, "add")], at(-1), slot(2), slot(2), size, prio, sent_x, last)
            terms, from_others = (0, 1, 2), [(t, "far"), (t, "plus"), (t, "minus")]
        else:
            last = ((t, "last"), lambda: so1.at[p, j, pl.ds(0, 2 * own_block), wide])
            send((t, "relay"), "x" + d, [(t, "add")], at(2), slot(0), slot(0), size, prio, sent_x)
            send((t, "direct"), "x" + e, [(t, "add")], at(-s), slot(2), slot(2), size, prio + 0.5, sent_x, last)

            def add_relay():
                so1[p, j, in_half(s), wide] = (
                    so1[p, j, in_half(s), wide].astype(f32) + in1[p, j, 0, :, wide].astype(f32)).astype(bf16)

            compute((t, "radd"), [(t, "relay")], add_relay, prio, 0.05)
            send((t, "final"), "x" + d, [(t, "radd")], at(s), slot(1), slot(1), size, prio, sent_x, last)
            terms, from_others = (1, 2), [(t, "final"), (t, "direct")]

        def finish():
            total = so1[p, j, in_half(0), wide].astype(f32)
            for i in terms:
                total = total + in1[p, j, i, :, wide].astype(f32)
            cs1[p, j, late_rows(), wide] = total.astype(bf16)

        compute((t, "finish"), from_others, finish, prio, 0.06)

        def there(*where, **more):
            return lambda: cs1.at[p, j, late_rows(*where, **more), wide]

        begin = [(t, "finish")]
        paired = ((t, "P"), lambda: cs1.at[p, j, pl.ds(0, half_of), wide])
        other = 1 - c
        send((t, "A", "+"), "x+", begin, there(0), there(0), there(-1), size, prio, sent_x)
        send((t, "A", "-"), "x-", begin, there(0), there(0), there(1), size, prio, sent_x)
        if direct:
            send((t, "A", "x2"), "x2", begin, there(0), there(0), there(2), size, prio, sent_x)
            far = [(t, "A", "x2")]
        else:
            both = ((t, "B"), there(2))
            for d, off in (("+", 0), ("-", own_block // 2)):
                piece = dict(rows=own_block // 2, off=off)
                b = there(-sign[d], **piece)
                send((t, "B", d), "x" + d, [(t, "A", d)], b, b, there(2, **piece), size // 2, prio, sent_x, both)
            far = [(t, "B", "+"), (t, "B", "-")]
        for dx, after in ((0, begin), (-1, [(t, "A", "+")]), (1, [(t, "A", "-")]), (2, far)):
            send((t, "P", dx), "c", after, there(dx), there(dx), there(dx, other), size, prio, sent_c, paired)

        def count():
            def step(i, _):
                here = pl.ds(pl.multiple_of(i * 64, 64), 64)
                rows = pl.ds(pl.multiple_of(p * PART + i * 64, 64), 64)
                shift, one, two = stats[0, rows, :], stats[1, rows, :], stats[2, rows, :]
                for at, cols in enumerate(columns):
                    value = (residual_scale * first[rows, cols].astype(f32)
                             + cs1[p, j, here, at * GROUP:(at + 1) * GROUP].astype(f32))
                    val[rows, cols] = value
                    for lanes in range(0, GROUP, 128):
                        part = value[:, lanes:lanes + 128] - shift
                        one, two = one + part, two + part * part
                stats[1, rows, :], stats[2, rows, :] = one, two
                return 0

            lax.fori_loop(0, PART // 64, step, 0)

        compute((t, "count"), begin + far + [("stats", p)] + [(t, "P", dx) for dx in (0, -1, 1, 2)],
                count, prio + 1, 0.15 * len(dists))

    def begin_stats(p):
        def emit():
            rows = pl.ds(p * PART, PART)
            shift = residual_scale * first[rows, 0:128].astype(f32)[:, 0:1]
            stats[0, rows, :] = jnp.broadcast_to(shift, (PART, 128))
            stats[1, rows, :] = jnp.zeros((PART, 128), f32)
            stats[2, rows, :] = jnp.zeros((PART, 128), f32)

        compute(("stats", p), [("hidden", p, 1)], emit, 6, 0.1)

    for p in range(PARTS):
        begin_stats(p)
        for j, dists in enumerate(LATE):
            late_chunk(p, j, dists, DIRECT[j], 2 + 0.5 * p + 0.05 * j)

    def finish_norm(p):
        def step(i, _):
            rows = pl.ds(pl.multiple_of(p * PART + i * 64, 64), 64)
            off = jnp.sum(stats[1, rows, :], -1, keepdims=True) * (1.0 / WIDTH)
            square = jnp.sum(stats[2, rows, :], -1, keepdims=True) * (1.0 / WIDTH)
            scale = lax.rsqrt(jnp.maximum(square - off * off, 0.0) + norm_epsilon)
            centered = val[rows, :] - (stats[0, rows, 0:1] + off)
            res[rows, :] = (centered * scale * cgain[...] + cshift[...]).astype(bf16)
            return 0

        lax.fori_loop(0, PART // 64, step, 0)

    for p in range(PARTS):
        compute(("finish_norm", p), [(("late", p, j), "count") for j in range(len(LATE))],
                functools.partial(finish_norm, p), 6, 0.65)

    for tag, way, _, _ in PIECES:
        for op in ops:
            if isinstance(op.name, tuple) and op.name[0] == tag:
                op.earliest = EARLIEST.get(tag[0] + way, 0.0)
    order, done = plan(ops)
    if report is not None:
        report(order, done, len(send_groups), len(recv_groups), len(loads))
    assert (len(send_groups), len(recv_groups), len(loads)) == (N_SENDS, N_RECVS, N_LOADS), (
        len(send_groups), len(recv_groups), len(loads))

    for start_load in loads:
        start_load()
    barrier = pltpu.get_barrier_semaphore()
    for link in peer:
        pl.semaphore_signal(barrier, inc=1, device_id=peer[link], device_id_type=pl.DeviceIdType.MESH)
    pl.semaphore_wait(barrier, len(peer))

    by_name = {op.name: op for op in ops}
    waited = set()

    def need(name):
        op = by_name[name]
        key = op.group or name
        if op.wait is not None and key not in waited:
            waited.add(key)
            op.wait()

    for _, op in order:
        for name in op.deps:
            need(name)
        op.emit()
    for op in ops:
        need(op.name)
    for wait in sends.values():
        wait()


N_SENDS, N_RECVS, N_LOADS = 50, 261, 7


def local(tokens, gate_outer, gate_inner, conv_input, mixer_output, conv_taps, mixer_gain,
          mixer_shift, up_weight, down_weight, channel_gain, channel_shift):
    bf16, f32 = jnp.bfloat16, jnp.float32
    vmem, hbm = pl.BlockSpec(memory_space=pltpu.VMEM), pl.BlockSpec(memory_space=pl.ANY)
    return pl.pallas_call(
        layer_kernel,
        out_shape=pltpu.VMEM((SEQ, WIDTH), bf16),
        in_specs=[hbm] * 7 + [vmem] * 5,
        out_specs=vmem,
        scratch_shapes=[
            pltpu.VMEM((SEQ, WIDTH), bf16),
            pltpu.VMEM((NZ, GROUP, 512), bf16),
            pltpu.VMEM((NZ, GROUP, 1024), bf16),
            pltpu.VMEM((NZ, GROUP, 1024), bf16),
            pltpu.VMEM((SEQ, 384), f32),
            pltpu.VMEM((SEQ + 8, 128), f32),
            pltpu.VMEM((SEQ, 128), bf16),
            pltpu.VMEM((1, PARTS, CHUNKS, PART, CHUNK), bf16),
            pltpu.VMEM((1, PARTS, CHUNKS, CORE_ROWS, CHUNK), bf16),
            pltpu.VMEM((1, PARTS, CHUNKS, CORE_ROWS, CHUNK), bf16),
            pltpu.VMEM((1, PARTS, CHUNKS, OWN, CHUNK), bf16),
            pltpu.VMEM((1, PARTS, CHUNKS, OWN, CHUNK), bf16),
            pltpu.VMEM((1, PARTS, CHUNKS, OWN, CHUNK), bf16),
            pltpu.VMEM((PARTS, OWN, WIDTH), f32),
            pltpu.VMEM((SEQ, WIDTH), bf16),
            pltpu.VMEM((SEQ, 1024), bf16),
            pltpu.VMEM((PARTS, len(LATE), PART, CHUNK), bf16),
            pltpu.VMEM((PARTS, len(LATE), CORE_ROWS, CHUNK), bf16),
            pltpu.VMEM((PARTS, len(LATE), CORE_ROWS, CHUNK), bf16),
            pltpu.VMEM((PARTS, len(LATE), 3, OWN, CHUNK), bf16),
            pltpu.VMEM((PARTS, len(LATE), PART, CHUNK), bf16),
            pltpu.VMEM((SEQ, WIDTH), f32),
            pltpu.VMEM((3, SEQ, 128), f32),
            pltpu.SemaphoreType.DMA((N_SENDS,)),
            pltpu.SemaphoreType.DMA((N_RECVS,)),
            pltpu.SemaphoreType.DMA((N_LOADS,)),
        ],
        compiler_params=pltpu.CompilerParams(
            collective_id=0, has_side_effects=True, vmem_limit_bytes=56 * 2**20),
    )(tokens, gate_outer, gate_inner, conv_input, mixer_output, up_weight, down_weight, conv_taps,
      mixer_gain.reshape(1, -1), mixer_shift.reshape(1, -1), channel_gain.reshape(1, -1),
      channel_shift.reshape(1, -1))


def solution(mesh):
    weights = P("fs", "tp")
    in_specs = (
        P(("rep", "fs"), None), weights, weights, weights, weights, P(None, "tp"), P(), P(),
        weights, weights, P(), P(),
    )
    out_specs = P(("rep", "fs"), None)
    return jax.shard_map(local, mesh=mesh, in_specs=in_specs, out_specs=out_specs, check_vma=False)
```

```python
import functools

import jax
import jax.numpy as jnp
from jax import lax
from jax.experimental import pallas as pl
from jax.experimental.pallas import tpu as pltpu
from jax.sharding import PartitionSpec as P

residual_scale = 8.0**0.25
norm_epsilon = 1e-05

NZ, NY, NX = 8, 4, 4
SEQ, WIDTH = 512, 2048
ROWS = 64
GROUP = 256
PARTS = 2
PART = SEQ // PARTS
CORE_ROWS, OWN = PART // 2, PART // 8
CHUNKS, CHUNK = 4, 512
NEAR = ("+", "-")
ARRIVAL = (0, 1, -1, 2, -2, 3, -3, 4)
LATE = ((0, 1), (-1, 2), (-2, 3), (-3,), (4,))
DIRECT = (False, False, False, False, True)

LINK_RATE, LINK_LAT = 45.0e3, 2.1
PAIR_RATE, PAIR_LAT = 400e3, 1.6
BACKLOG = 2.19
PATHS = {"c": (PAIR_RATE, PAIR_LAT), "x+": (LINK_RATE, 2.6), "x-": (LINK_RATE, 2.6)}


PIECES = (
    ("m0", "y", 128, 1),
    ("m2", "z", 384, 1),
    ("u0", "y", 128, 4),
    ("u1", "y", 256, 4),
    ("u2", "z", 384, 4),
    ("u3", "z", 256, 4),
    ("d0", "y", 256, 5),
    ("d1", "y", 256, 5),
    ("d2", "z", 512, 5),
)
HOPS = {
    "m": {"y": (5.61, 4.34), "yz": (5.34, 6, 0.53, 6),
          "z": (4.44, 4.62, 0.82, 4.99), "zy": (5.9, 4.34, 4.14, 4.25, 4.06)},
    "u": {"y": (2.22, 1.12), "yz": (3.71, 6, 1.21, 5.27),
          "z": (0.3, 3.75, 0.94, 1.15), "zy": (6, 0.54, 3.36, 1.2, 3.15)},
    "d": {"y": (5.58, 3.55), "yz": (0.71, 1.27, 1.04, 6),
          "z": (0.3, 0.72, 2.95, 5.59), "zy": (4.92, 2.2, 2.34, 2.56, 1.36)},
}
EARLIEST = {"uy": 6.0, "uz": 11.0, "dy": 16.3, "dz": 19.5}


class Op:
    def __init__(self, name, deps, emit, prio, dur=0.0, link=None, nbytes=0, wait=None, latency=0.0):
        self.name, self.deps, self.emit, self.prio = name, deps, emit, prio
        self.dur, self.link, self.nbytes, self.wait = dur, link, nbytes, wait
        self.latency, self.group, self.earliest = latency, None, 0.0


def plan(ops):
    done, link_free, order, now = {}, {}, [], 0.0
    members = {}
    for op in ops:
        if op.group is not None:
            members.setdefault(op.group, []).append(op.name)
    group_of = {op.name: members[op.group] for op in ops if op.group is not None}
    for op in ops:
        op.deps = list(dict.fromkeys(m for d in op.deps for m in group_of.get(d, [d])))
    left = list(ops)
    while left:
        best = None
        for at, op in enumerate(left):
            if any(d not in done for d in op.deps):
                continue
            ready = max([done[d] for d in op.deps] + [op.earliest])
            if op.link is not None:
                ready = max(ready, link_free.get(op.link, 0.0) - (BACKLOG if op.prio >= 3 else 0.73 * BACKLOG))
            key = (max(ready, now), op.prio, at)
            if best is None or key < best[0]:
                best = (key, op)
        (start, _, _), op = best
        left.remove(op)
        now = start + (op.dur if op.link is None else 0.03)
        if op.link is None:
            done[op.name] = now + op.latency
        else:
            rate, lat = PATHS.get(op.link, (LINK_RATE, LINK_LAT))
            begin = max(now, link_free.get(op.link, 0.0))
            link_free[op.link] = begin + op.nbytes / rate
            done[op.name] = link_free[op.link] + lat
        order.append((start, op))
    return order, done


def layer_kernel(
    tok_hbm, go_hbm, gi_hbm, ci_hbm, mo_hbm, up_hbm, dn_hbm, taps, mgain, mshift, cgain, cshift,
    res,
    tok, wm, wu, wd, proj, prod, conv, pp, so, dr, rl, fr, fd, v, first, hid,
    pp1, dr1, so1, in1, cs1, val, stats, send_sems, recv_sems, load_sems,
    report=None,
):
    f32, bf16 = jnp.float32, jnp.bfloat16
    rep, fs, tp = lax.axis_index("rep"), lax.axis_index("fs"), lax.axis_index("tp")
    zl, y = lax.div(fs, NY), lax.rem(fs, NY)
    x, c = lax.div(tp, 2), lax.rem(tp, 2)
    z = rep * NZ + zl

    def mod(v, n):
        return lax.rem(v + 2 * n, n)

    def device(dz=0, dy=0, dx=0, dc=0):
        zz = mod(z + dz, 2 * NZ)
        return (
            lax.div(zz, NZ),
            lax.rem(zz, NZ) * NY + mod(y + dy, NY),
            mod(x + dx, NX) * 2 + lax.rem(c + dc, 2),
        )

    peer = {
        "z+": device(dz=1), "z-": device(dz=-1), "y+": device(dy=1), "y-": device(dy=-1),
        "x+": device(dx=1), "x-": device(dx=-1), "x2": device(dx=2), "c": device(dc=1),
    }
    sign = {"+": 1, "-": -1}

    ops = []
    sends = {}

    send_groups, recv_groups = {}, {}

    def send(name, link, deps, src, dst, landed, nbytes, prio, sent, group=None):
        send_at = send_groups.setdefault(sent[0], len(send_groups))
        recv_at = recv_groups.setdefault(group[0] if group else name, len(recv_groups))

        def copy(s, d):
            return pltpu.make_async_remote_copy(
                src_ref=s, dst_ref=d, send_sem=send_sems.at[send_at], recv_sem=recv_sems.at[recv_at],
                device_id=peer[link], device_id_type=pl.DeviceIdType.MESH,
            )

        all_here = group[1] if group else landed
        sends.setdefault(sent[0], lambda: copy(sent[1](), sent[1]()).wait_send())
        op = Op(
            name, deps, lambda: copy(src(), dst()).start(), prio,
            link="x+" if link == "x2" else link, nbytes=2 * nbytes if link == "x2" else nbytes,
            wait=lambda: copy(all_here(), all_here()).wait_recv(),
        )
        op.group = group[0] if group else None
        ops.append(op)

    def compute(name, deps, emit, prio, dur):
        ops.append(Op(name, deps, emit, prio, dur=dur))

    loads = []

    def load(name, src, dst):
        index = len(loads)
        op = Op(name, [], lambda: None, 0, latency=0.5)
        op.wait = lambda: pltpu.make_async_copy(src(), dst(), load_sems.at[index]).wait()
        loads.append(lambda: pltpu.make_async_copy(src(), dst(), load_sems.at[index]).start())
        ops.append(op)

    def own(w, c0, n):
        return lambda: w.at[zl, pl.ds(pl.multiple_of(y * ROWS, ROWS), ROWS), pl.ds(c0, n)]

    load("load.m0", lambda: go_hbm, own(wm, 0, 128))
    load("load.m1", lambda: gi_hbm, own(wm, 128, 128))
    load("load.m2", lambda: ci_hbm, own(wm, 256, 128))
    load("load.m3", lambda: mo_hbm, own(wm, 384, 128))
    load("load.u", lambda: up_hbm, own(wu, 0, 1024))
    load("load.d", lambda: dn_hbm, own(wd, 0, 1024))
    load("load.t", lambda: tok_hbm, lambda: tok)

    def block(w, dz, dy, c0, n, half=None):
        rows, off = (ROWS, 0) if half is None else (ROWS // 2, half * ROWS // 2)

        def view():
            start = pl.multiple_of(mod(y + dy, NY) * ROWS + off, ROWS // 2)
            return w.at[mod(zl + dz, NZ), pl.ds(start, rows), pl.ds(c0, n)]

        return view

    def slab(w, dz, c0, n, half=None):
        rows, off = (GROUP, 0) if half is None else (GROUP // 2, half * GROUP // 2)
        return lambda: w.at[mod(zl + dz, NZ), pl.ds(off, rows), pl.ds(c0, n)]

    ready = {}

    def y_first(tag, w, c0, n, deps, prio):
        size = ROWS * n * 2
        part_of = lambda zs, rows: (lambda: w.at[zs, rows, pl.ds(c0, n)])
        sent_y = ((tag, "Y"), part_of(0, pl.ds(0, 3 * ROWS)))
        sent_z = ((tag, "Z"), part_of(pl.ds(0, 7), pl.ds(0, GROUP)))
        second = ((tag, "Y", 2), part_of(0, pl.ds(0, ROWS)))
        fourth = ((tag, "Z", 4), part_of(0, pl.ds(0, GROUP)))
        for d in "+-":
            s = sign[d]
            b = block(w, 0, 0, c0, n)
            send((tag, "Y", 1, d), "y" + d, deps, b, b, block(w, 0, -s, c0, n), size,
                 HOPS[tag[0]]["y"][0], sent_y)
        for d, half in (("+", 0), ("-", 1)):
            s = sign[d]
            b = block(w, 0, -s, c0, n, half)
            send((tag, "Y", 2, d), "y" + d, [(tag, "Y", 1, d)], b, b, block(w, 0, -2 * s, c0, n, half), size // 2,
                 HOPS[tag[0]]["y"][1], sent_y, second)
        group = [(tag, "Y", h, d) for h in (1, 2) for d in "+-"]
        ready[tag[0], 0] = ready.get((tag[0], 0), []) + group
        for d, half in (("+", 0), ("-", 1)):
            s = sign[d]
            for h in (1, 2, 3, 4):
                part = half if h == 4 else None
                b = slab(w, -s * (h - 1), c0, n, part)
                before = deps + group if h == 1 else [(tag, "Z", h - 1, d)]
                send((tag, "Z", h, d), "z" + d, before, b, b, slab(w, -s * h, c0, n, part),
                     NY * size // (1 if part is None else 2), HOPS[tag[0]]["yz"][h - 1],
                     sent_z, fourth if h == 4 else None)
                dist = 4 if h == 4 else -s * h
                ready[tag[0], dist] = ready.get((tag[0], dist), []) + [(tag, "Z", h, d)]

    def z_first(tag, w, c0, n, deps, prio):
        size = ROWS * n * 2
        part_of = lambda zs, rows: (lambda: w.at[zs, rows, pl.ds(c0, n)])
        sent_z = part_of(0, pl.ds(0, 7 * ROWS // 2))
        sent_y = ((tag, "Y"), part_of(pl.ds(0, 6), pl.ds(0, GROUP)))
        fourth = ((tag, "Z", 4), part_of(0, pl.ds(0, ROWS)))
        for d, half in (("+", 0), ("-", 1)):
            s = sign[d]
            for h in (1, 2, 3, 4):
                part = half if h == 4 else None
                b = block(w, -s * (h - 1), 0, c0, n, part)
                before = deps if h == 1 else [(tag, "Z", h - 1, d)]
                send((tag, "Z", h, d), "z" + d, before, b, b, block(w, -s * h, 0, c0, n, part),
                     size // (1 if part is None else 2), HOPS[tag[0]]["z"][h - 1],
                     ((tag, "Z", d), sent_z), fourth if h == 4 else None)
        late = {dist: j for j, dists in enumerate(LATE) for dist in dists}
        for at, dist in enumerate(ARRIVAL):
            here = {0: deps, 4: [(tag, "Z", 4, "+"), (tag, "Z", 4, "-")]}.get(
                dist, [(tag, "Z", abs(dist), NEAR[dist > 0])])
            second = {
                "m": ((tag, "Y", 2, at), part_of(0, pl.ds(0, ROWS))),
                "u": ((tag, "Y", 2), part_of(pl.ds(0, 2), pl.ds(0, GROUP))),
                "d": ((tag, "Y", 2, late[dist]), part_of(0, pl.ds(0, ROWS * len(LATE[late[dist]])))),
            }[tag[0]]
            for d, half in (("+", 0), ("-", 1)):
                s = sign[d]
                b = block(w, dist, 0, c0, n)
                send((tag, "Y", 1, d, dist), "y" + d, here, b, b, block(w, dist, -s, c0, n), size,
                     HOPS[tag[0]]["zy"][abs(dist)], sent_y)
                b = block(w, dist, -s, c0, n, half)
                send((tag, "Y", 2, d, dist), "y" + d, [(tag, "Y", 1, d, dist)], b, b,
                     block(w, dist, -2 * s, c0, n, half), size // 2,
                     HOPS[tag[0]]["zy"][abs(dist)], sent_y, second)
            names = here + [(tag, "Y", h, d, dist) for h in (1, 2) for d in "+-"]
            ready[tag[0], dist] = ready.get((tag[0], dist), []) + names

    seen = []
    mixer_loads = ["load.m0", "load.m1", "load.m2", "load.m3"]
    column, loads_of = 0, {"m": mixer_loads, "u": ["load.u"], "d": ["load.d"]}
    for tag, way, n, prio in PIECES:
        w = {"m": wm, "u": wu, "d": wd}[tag[0]]
        if tag[0] not in [t[0] for t in seen]:
            column = 0
        seen.append(tag)
        way = y_first if way == "y" else z_first
        way(tag, w, column, n, loads_of[tag[0]], prio)
        column += n

    def project(first_one, dists):
        def emit():
            for at, dist in enumerate(dists):
                g = mod(zl + dist, NZ)
                term = jnp.dot(
                    tok[:, pl.ds(pl.multiple_of(g * GROUP, GROUP), GROUP)], wm[g, :, 0:384],
                    preferred_element_type=f32)
                if first_one and at == 0:
                    proj[...] = term
                else:
                    proj[...] += term

        return emit

    def convolve():
        prod[0:8, :] = jnp.zeros((8, 128), f32)
        prod[8:, :] = proj[:, 128:256] * proj[:, 256:384]
        total = taps[0:1, :] * prod[6:6 + SEQ, :]
        total = total + taps[1:2, :] * prod[7:7 + SEQ, :]
        total = total + taps[2:3, :] * prod[8:8 + SEQ, :]
        conv[...] = (proj[:, 0:128] * total).astype(bf16)

    compute_after = ["load.t"] + mixer_loads
    for dist in ARRIVAL:
        compute_after = compute_after + ready["m", dist]
        compute(("project", dist), compute_after, project(dist == 0, [dist]), 0, 0.35)
        compute_after = [("project", dist)]
    compute("convolve", compute_after, convolve, 0, 0.7)

    nt = (((1,), (1,)), ((), ()))

    def product(phase, p, k, left, rights):
        for at, right in enumerate(rights):
            pp[phase, p, k, :, at * GROUP:(at + 1) * GROUP] = lax.dot_general(
                left[p * PART:(p + 1) * PART, :], right(), nt, preferred_element_type=f32).astype(bf16)

    def rows_of(dx):
        return pl.ds(pl.multiple_of(mod(x + dx, NX) * OWN, OWN), OWN)

    def core_rows(core):
        return pl.ds(pl.multiple_of(core * CORE_ROWS, CORE_ROWS), CORE_ROWS)

    def seq_rows(p, dx=0, core=None):
        core = c if core is None else core
        return pl.ds(pl.multiple_of(p * PART + core * CORE_ROWS + mod(x + dx, NX) * OWN, OWN), OWN)

    def sum_chunk(phase, p, k, groups, residual, prio):
        t = ("s", phase, p, k)
        d, e = ("+", "-") if k % 2 == 0 else ("-", "+")
        s = sign[d]
        send((t, "pair"), "c", [(t, "product")], lambda: pp.at[phase, p, k, core_rows(1 - c), :],
             lambda: dr.at[phase, p, k], lambda: dr.at[phase, p, k], CORE_ROWS * CHUNK * 2, prio,
             (("s", phase, p, "pair"), lambda: dr.at[phase, p]))

        def add_pair():
            so[phase, p, k] = (
                pp[phase, p, k, core_rows(c), :].astype(f32) + dr[phase, p, k].astype(f32)).astype(bf16)

        compute((t, "add"), [(t, "product"), (t, "pair")], add_pair, prio, 0.06)
        size = OWN * CHUNK * 2
        at = lambda dx: (lambda: so.at[phase, p, k, rows_of(dx), :])
        slot = lambda ref: (lambda: ref.at[phase, p, k])
        sent = (("s", phase, p, "x"), lambda: so.at[phase, p, pl.ds(0, CHUNKS - 1)])
        last = ((t, "last"), lambda: so.at[phase, p, k, pl.ds(0, 2 * OWN), :])
        send((t, "relay"), "x" + d, [(t, "add")], at(2), slot(rl), slot(rl), size, prio, sent)
        send((t, "direct"), "x" + e, [(t, "add")], at(-s), slot(fd), slot(fd), size, prio + 0.5,
             sent, last)

        def add_relay():
            so[phase, p, k, rows_of(s), :] = (
                so[phase, p, k, rows_of(s), :].astype(f32) + rl[phase, p, k].astype(f32)).astype(bf16)

        compute((t, "radd"), [(t, "add"), (t, "relay")], add_relay, prio, 0.03)
        send((t, "final"), "x" + d, [(t, "radd")], at(s), slot(fr), slot(fr), size, prio, sent, last)

        def finish():
            total = so[phase, p, k, rows_of(0), :].astype(f32) + fr[phase, p, k].astype(f32)
            total = total + fd[phase, p, k].astype(f32)
            for at, group in enumerate(groups):
                columns = pl.ds(pl.multiple_of(group() * GROUP, GROUP), GROUP)
                v[p, :, columns] = (residual_scale * residual[seq_rows(p), columns].astype(f32)
                                    + total[:, at * GROUP:(at + 1) * GROUP])

        compute((t, "finish"), [(t, "add"), (t, "final"), (t, "direct")], finish, prio, 0.04)

    def norm(phase, p, gain, shift, dest, prio):
        def emit():
            values = v[p]
            mean = jnp.mean(values, -1, keepdims=True)
            centered = values - mean
            variance = jnp.mean(centered * centered, -1, keepdims=True)
            scaled = centered * lax.rsqrt(variance + norm_epsilon)
            dest[seq_rows(p), :] = (scaled * gain[...] + shift[...]).astype(bf16)

        compute(("norm", phase, p), [(("s", phase, p, k), "finish") for k in range(CHUNKS)], emit, prio, 0.25)

    HALF = WIDTH // 2

    def place(p, dx, h, other=False):
        def view(ref):
            rows = seq_rows(p, dx, 1 - c if other else c)
            return ref.at[rows, :] if h is None else ref.at[rows, pl.ds(h * HALF, HALF)]
        return view

    def gather(phase, p, ref, prio):
        def at(*where):
            return lambda: place(p, *where)(ref)

        t, size, landed = ("g", phase, p), OWN * HALF * 2, []
        start = [("norm", phase, p)]
        first_rows = lambda rows: (lambda: ref.at[pl.ds(0, rows), :])
        sent_x, sent_c = ((t, "x"), first_rows(3 * OWN)), ((t, "c"), first_rows(4 * OWN))
        if phase == 0:
            pairs = [((t, "P"), first_rows(4 * OWN))] * 4
        else:
            pairs = [((t, "P", i), first_rows(rows)) for i, rows in enumerate((OWN, OWN, OWN, OWN))]
        for d, first_half in (("+", 0), ("-", 1)):
            for h in (first_half, 1 - first_half):
                send((t, "A", d, h), "x" + d, start, at(0, h), at(0, h), at(-sign[d], h), size, prio, sent_x)
                landed.append(((t, "A", d, h), (-sign[d], h)))
        send((t, "P"), "c", start, at(0, None), at(0, None), at(0, None, True), 2 * size, prio, sent_c, pairs[0])
        landed.append(((t, "P"), (0, None, True)))
        for d, h in (("+", 0), ("-", 1)):
            b = at(-sign[d], h)
            send((t, "B", d), "x" + d, [(t, "A", d, h)], b, b, at(2, h), size, prio, sent_x)
            landed.append(((t, "B", d), (2, h)))
        for i, (name, dx, h) in enumerate((
                ((t, "A", "+", 0), -1, 0), ((t, "A", "-", 1), 1, 1), ((t, "A", "+", 1), -1, 1),
                ((t, "A", "-", 0), 1, 0), ((t, "B", "+"), 2, 0), ((t, "B", "-"), 2, 1))):
            send((name, "P"), "c", [name], at(dx, h), at(dx, h), at(dx, h, True), size, prio,
                 sent_c, pairs[1 + i // 2])
            landed.append(((name, "P"), (dx, h, True)))
        return landed

    def hidden(p, n):
        rows = pl.ds(p * PART, PART)
        for at in (2 * n, 2 * n + 1):
            columns = pl.ds(at * 256, 256)
            up = jnp.dot(first[rows, :], wu[:, :, columns].reshape(WIDTH, 256), preferred_element_type=f32)
            hid[rows, columns] = jnp.square(jnp.maximum(up, 0.0)).astype(bf16)

    up_ready = ["load.u"] + [n for dist in ARRIVAL for n in ready["u", dist]]
    for p in range(PARTS):
        for k in range(CHUNKS):
            pair = (2 * k, 2 * k + 1)
            compute((("s", 0, p, k), "product"), ["convolve"],
                    functools.partial(product, 0, p, k, conv, [lambda g=g: wm[g, :, 384:512] for g in pair]),
                    0 + p, 0.25)
            sum_chunk(0, p, k, [lambda g=g: g for g in pair], tok, 0 + p)
        norm(0, p, mgain, mshift, first, 0 + p)
        landed = gather(0, p, first, 0 + p)
        for n in range(2):
            compute(("hidden", p, n), [("norm", 0, p)] + [name for name, _ in landed] + up_ready,
                    functools.partial(hidden, p, n), 2 + p, 0.75)

    own_block, half_of = OWN, CORE_ROWS

    def late_rows(dx=0, core=None, rows=own_block, off=0):
        core = c if core is None else core
        start = core * half_of + mod(x + dx, NX) * own_block + off
        return pl.ds(pl.multiple_of(start, own_block // 2), rows)

    def late_half(core):
        return pl.ds(pl.multiple_of(core * half_of, half_of), half_of)

    def in_half(dx):
        return pl.ds(pl.multiple_of(mod(x + dx, NX) * own_block, own_block), own_block)

    def late_chunk(p, j, dists, direct, prio):
        t, width = ("late", p, j), GROUP * len(dists)
        wide = pl.ds(0, width)
        groups = [mod(zl + dist, NZ) for dist in dists]
        columns = [pl.ds(pl.multiple_of(g * GROUP, GROUP), GROUP) for g in groups]
        arrived = [name for dist in dists for name in ready["d", dist]]

        def multiply():
            for at, g in enumerate(groups):
                for r in range(1, -1, -1) if len(groups) == 1 else (None,):
                    size, start = (PART, 0) if r is None else (half_of, r * half_of)
                    pp1[p, j, pl.ds(start, size), at * GROUP:(at + 1) * GROUP] = lax.dot_general(
                        hid[pl.ds(p * PART + start, size), :], wd[g], nt, preferred_element_type=f32).astype(bf16)

        compute((t, "product"), [("hidden", p, n) for n in range(2)] + ["load.d"] + arrived,
                multiply, prio, 0.25 * len(dists))
        sent_x = ((t, "x"), lambda: cs1.at[p, j, pl.ds(0, 6 * own_block), wide])
        sent_c = ((t, "c"), lambda: cs1.at[p, j, :, wide])
        size = own_block * width * 2
        send((t, "pair"), "c", [(t, "product")], lambda: pp1.at[p, j, late_half(1 - c), wide],
             lambda: dr1.at[p, j, :, wide], lambda: dr1.at[p, j, :, wide], NX * size, prio, sent_c)

        def add_pair():
            so1[p, j, :, wide] = (
                pp1[p, j, late_half(c), wide].astype(f32) + dr1[p, j, :, wide].astype(f32)).astype(bf16)

        compute((t, "add"), [(t, "pair")], add_pair, prio, 0.1)
        at = lambda dx: (lambda: so1.at[p, j, in_half(dx), wide])
        slot = lambda i: (lambda: in1.at[p, j, i, :, wide])
        d, e = ("+", "-") if j % 2 == 0 else ("-", "+")
        s = sign[d]
        if direct:
            last = ((t, "last"), lambda: so1.at[p, j, pl.ds(0, 3 * own_block), wide])
            send((t, "far"), "x2", [(t, "add")], at(2), slot(0), slot(0), size, prio, sent_x, last)
            send((t, "plus"), "x+", [(t, "add")], at(1), slot(1), slot(1), size, prio, sent_x, last)
            send((t, "minus"), "x-", [(t, "add")], at(-1), slot(2), slot(2), size, prio, sent_x, last)
            terms, from_others = (0, 1, 2), [(t, "far"), (t, "plus"), (t, "minus")]
        else:
            last = ((t, "last"), lambda: so1.at[p, j, pl.ds(0, 2 * own_block), wide])
            send((t, "relay"), "x" + d, [(t, "add")], at(2), slot(0), slot(0), size, prio, sent_x)
            send((t, "direct"), "x" + e, [(t, "add")], at(-s), slot(2), slot(2), size, prio + 0.5, sent_x, last)

            def add_relay():
                so1[p, j, in_half(s), wide] = (
                    so1[p, j, in_half(s), wide].astype(f32) + in1[p, j, 0, :, wide].astype(f32)).astype(bf16)

            compute((t, "radd"), [(t, "relay")], add_relay, prio, 0.05)
            send((t, "final"), "x" + d, [(t, "radd")], at(s), slot(1), slot(1), size, prio, sent_x, last)
            terms, from_others = (1, 2), [(t, "final"), (t, "direct")]

        def finish():
            total = so1[p, j, in_half(0), wide].astype(f32)
            for i in terms:
                total = total + in1[p, j, i, :, wide].astype(f32)
            cs1[p, j, late_rows(), wide] = total.astype(bf16)

        compute((t, "finish"), from_others, finish, prio, 0.06)

        def there(*where, **more):
            return lambda: cs1.at[p, j, late_rows(*where, **more), wide]

        begin = [(t, "finish")]
        paired = ((t, "P"), lambda: cs1.at[p, j, pl.ds(0, half_of), wide])
        other = 1 - c
        send((t, "A", "+"), "x+", begin, there(0), there(0), there(-1), size, prio, sent_x)
        send((t, "A", "-"), "x-", begin, there(0), there(0), there(1), size, prio, sent_x)
        if direct:
            send((t, "A", "x2"), "x2", begin, there(0), there(0), there(2), size, prio, sent_x)
            far = [(t, "A", "x2")]
        else:
            both = ((t, "B"), there(2))
            for d, off in (("+", 0), ("-", own_block // 2)):
                piece = dict(rows=own_block // 2, off=off)
                b = there(-sign[d], **piece)
                send((t, "B", d), "x" + d, [(t, "A", d)], b, b, there(2, **piece), size // 2, prio, sent_x, both)
            far = [(t, "B", "+"), (t, "B", "-")]
        for dx, after in ((0, begin), (-1, [(t, "A", "+")]), (1, [(t, "A", "-")]), (2, far)):
            send((t, "P", dx), "c", after, there(dx), there(dx), there(dx, other), size, prio, sent_c, paired)

        def count():
            def step(i, _):
                here = pl.ds(pl.multiple_of(i * 64, 64), 64)
                rows = pl.ds(pl.multiple_of(p * PART + i * 64, 64), 64)
                shift, one, two = stats[0, rows, :], stats[1, rows, :], stats[2, rows, :]
                for at, cols in enumerate(columns):
                    value = (residual_scale * first[rows, cols].astype(f32)
                             + cs1[p, j, here, at * GROUP:(at + 1) * GROUP].astype(f32))
                    val[rows, cols] = value
                    for lanes in range(0, GROUP, 128):
                        part = value[:, lanes:lanes + 128] - shift
                        one, two = one + part, two + part * part
                stats[1, rows, :], stats[2, rows, :] = one, two
                return 0

            lax.fori_loop(0, PART // 64, step, 0)

        compute((t, "count"), begin + far + [("stats", p)] + [(t, "P", dx) for dx in (0, -1, 1, 2)],
                count, prio + 1, 0.15 * len(dists))

    def begin_stats(p):
        def emit():
            rows = pl.ds(p * PART, PART)
            shift = residual_scale * first[rows, 0:128].astype(f32)[:, 0:1]
            stats[0, rows, :] = jnp.broadcast_to(shift, (PART, 128))
            stats[1, rows, :] = jnp.zeros((PART, 128), f32)
            stats[2, rows, :] = jnp.zeros((PART, 128), f32)

        compute(("stats", p), [("hidden", p, 1)], emit, 6, 0.1)

    for p in range(PARTS):
        begin_stats(p)
        for j, dists in enumerate(LATE):
            late_chunk(p, j, dists, DIRECT[j], 2 + 0.5 * p + 0.05 * j)

    def finish_norm(p):
        def step(i, _):
            rows = pl.ds(pl.multiple_of(p * PART + i * 64, 64), 64)
            off = jnp.sum(stats[1, rows, :], -1, keepdims=True) * (1.0 / WIDTH)
            square = jnp.sum(stats[2, rows, :], -1, keepdims=True) * (1.0 / WIDTH)
            scale = lax.rsqrt(jnp.maximum(square - off * off, 0.0) + norm_epsilon)
            centered = val[rows, :] - (stats[0, rows, 0:1] + off)
            res[rows, :] = (centered * scale * cgain[...] + cshift[...]).astype(bf16)
            return 0

        lax.fori_loop(0, PART // 64, step, 0)

    for p in range(PARTS):
        compute(("finish_norm", p), [(("late", p, j), "count") for j in range(len(LATE))],
                functools.partial(finish_norm, p), 6, 1.05)

    for tag, way, _, _ in PIECES:
        for op in ops:
            if isinstance(op.name, tuple) and op.name[0] == tag:
                op.earliest = EARLIEST.get(tag[0] + way, 0.0)
    order, done = plan(ops)
    if report is not None:
        report(order, done, len(send_groups), len(recv_groups), len(loads))
    assert (len(send_groups), len(recv_groups), len(loads)) == (N_SENDS, N_RECVS, N_LOADS), (
        len(send_groups), len(recv_groups), len(loads))

    for start_load in loads:
        start_load()
    barrier = pltpu.get_barrier_semaphore()
    for link in peer:
        pl.semaphore_signal(barrier, inc=1, device_id=peer[link], device_id_type=pl.DeviceIdType.MESH)
    pl.semaphore_wait(barrier, len(peer))

    by_name = {op.name: op for op in ops}
    waited = set()

    def need(name):
        op = by_name[name]
        key = op.group or name
        if op.wait is not None and key not in waited:
            waited.add(key)
            op.wait()

    for _, op in order:
        for name in op.deps:
            need(name)
        op.emit()
    for op in ops:
        need(op.name)
    for wait in sends.values():
        wait()


N_SENDS, N_RECVS, N_LOADS = 50, 263, 7


def local(tokens, gate_outer, gate_inner, conv_input, mixer_output, conv_taps, mixer_gain,
          mixer_shift, up_weight, down_weight, channel_gain, channel_shift):
    bf16, f32 = jnp.bfloat16, jnp.float32
    vmem, hbm = pl.BlockSpec(memory_space=pltpu.VMEM), pl.BlockSpec(memory_space=pl.ANY)
    return pl.pallas_call(
        layer_kernel,
        out_shape=pltpu.VMEM((SEQ, WIDTH), bf16),
        in_specs=[hbm] * 7 + [vmem] * 5,
        out_specs=vmem,
        scratch_shapes=[
            pltpu.VMEM((SEQ, WIDTH), bf16),
            pltpu.VMEM((NZ, GROUP, 512), bf16),
            pltpu.VMEM((NZ, GROUP, 1024), bf16),
            pltpu.VMEM((NZ, GROUP, 1024), bf16),
            pltpu.VMEM((SEQ, 384), f32),
            pltpu.VMEM((SEQ + 8, 128), f32),
            pltpu.VMEM((SEQ, 128), bf16),
            pltpu.VMEM((1, PARTS, CHUNKS, PART, CHUNK), bf16),
            pltpu.VMEM((1, PARTS, CHUNKS, CORE_ROWS, CHUNK), bf16),
            pltpu.VMEM((1, PARTS, CHUNKS, CORE_ROWS, CHUNK), bf16),
            pltpu.VMEM((1, PARTS, CHUNKS, OWN, CHUNK), bf16),
            pltpu.VMEM((1, PARTS, CHUNKS, OWN, CHUNK), bf16),
            pltpu.VMEM((1, PARTS, CHUNKS, OWN, CHUNK), bf16),
            pltpu.VMEM((PARTS, OWN, WIDTH), f32),
            pltpu.VMEM((SEQ, WIDTH), bf16),
            pltpu.VMEM((SEQ, 1024), bf16),
            pltpu.VMEM((PARTS, len(LATE), PART, CHUNK), bf16),
            pltpu.VMEM((PARTS, len(LATE), CORE_ROWS, CHUNK), bf16),
            pltpu.VMEM((PARTS, len(LATE), CORE_ROWS, CHUNK), bf16),
            pltpu.VMEM((PARTS, len(LATE), 3, OWN, CHUNK), bf16),
            pltpu.VMEM((PARTS, len(LATE), PART, CHUNK), bf16),
            pltpu.VMEM((SEQ, WIDTH), f32),
            pltpu.VMEM((3, SEQ, 128), f32),
            pltpu.SemaphoreType.DMA((N_SENDS,)),
            pltpu.SemaphoreType.DMA((N_RECVS,)),
            pltpu.SemaphoreType.DMA((N_LOADS,)),
        ],
        compiler_params=pltpu.CompilerParams(
            collective_id=0, has_side_effects=True, vmem_limit_bytes=56 * 2**20),
    )(tokens, gate_outer, gate_inner, conv_input, mixer_output, up_weight, down_weight, conv_taps,
      mixer_gain.reshape(1, -1), mixer_shift.reshape(1, -1), channel_gain.reshape(1, -1),
      channel_shift.reshape(1, -1))


def solution(mesh):
    weights = P("fs", "tp")
    in_specs = (
        P(("rep", "fs"), None), weights, weights, weights, weights, P(None, "tp"), P(), P(),
        weights, weights, P(), P(),
    )
    out_specs = P(("rep", "fs"), None)
    return jax.shard_map(local, mesh=mesh, in_specs=in_specs, out_specs=out_specs, check_vma=False)
```

```python
import functools

import jax
import jax.numpy as jnp
from jax import lax
from jax.experimental import pallas as pl
from jax.experimental.pallas import tpu as pltpu
from jax.sharding import PartitionSpec as P

residual_scale = 8.0**0.25
norm_epsilon = 1e-05

NZ, NY, NX = 8, 4, 4
SEQ, WIDTH = 512, 2048
ROWS = 64
GROUP = 256
PARTS = 2
PART = SEQ // PARTS
CORE_ROWS, OWN = PART // 2, PART // 8
CHUNKS, CHUNK = 4, 512
NEAR = ("+", "-")
ARRIVAL = (0, 1, -1, 2, -2, 3, -3, 4)
LATE = ((0, 1), (-1, 2), (-2, 3), (-3, 4))
DIRECT = (False, False, False, False)

LINK_RATE, LINK_LAT = 45.0e3, 2.1
PAIR_RATE, PAIR_LAT = 400e3, 1.6
BACKLOG = 1.9
PATHS = {"c": (PAIR_RATE, PAIR_LAT), "x+": (LINK_RATE, 2.6), "x-": (LINK_RATE, 2.6)}


PIECES = (
    ("m0", "y", 128, 1),
    ("m2", "z", 384, 1),
    ("u0", "y", 128, 4),
    ("u1", "y", 256, 4),
    ("u2", "z", 384, 4),
    ("u3", "z", 256, 4),
    ("d0", "y", 256, 5),
    ("d1", "y", 256, 5),
    ("d2", "z", 512, 5),
)
HOPS = {
    "m": {"y": (0.76, 3.57), "yz": (5.4, 4.91, 3.59, 6),
          "z": (0.75, 4.7, 5.55, 2.49), "zy": (6, 4.33, 6, 3.75, 3.57)},
    "u": {"y": (3.62, 4.53), "yz": (3.69, 1.44, 4.5, 2.13),
          "z": (1.42, 1.1, 0.76, 3.22), "zy": (0.3, 0.99, 3.35, 3.91, 1.5)},
    "d": {"y": (5.22, 3.72), "yz": (6, 1.71, 5.65, 1.31),
          "z": (1.86, 2.09, 0.83, 2.25), "zy": (2.19, 0.3, 1.5, 2.04, 2.99)},
}
EARLIEST = {"uy": 3.8, "uz": 11.0, "dy": 15.3, "dz": 0.1}


class Op:
    def __init__(self, name, deps, emit, prio, dur=0.0, link=None, nbytes=0, wait=None, latency=0.0):
        self.name, self.deps, self.emit, self.prio = name, deps, emit, prio
        self.dur, self.link, self.nbytes, self.wait = dur, link, nbytes, wait
        self.latency, self.group, self.earliest = latency, None, 0.0


def plan(ops):
    done, link_free, order, now = {}, {}, [], 0.0
    members = {}
    for op in ops:
        if op.group is not None:
            members.setdefault(op.group, []).append(op.name)
    group_of = {op.name: members[op.group] for op in ops if op.group is not None}
    for op in ops:
        op.deps = list(dict.fromkeys(m for d in op.deps for m in group_of.get(d, [d])))
    left = list(ops)
    while left:
        best = None
        for at, op in enumerate(left):
            if any(d not in done for d in op.deps):
                continue
            ready = max([done[d] for d in op.deps] + [op.earliest])
            if op.link is not None:
                ready = max(ready, link_free.get(op.link, 0.0) - (BACKLOG if op.prio >= 3 else 0.94 * BACKLOG))
            key = (max(ready, now), op.prio, at)
            if best is None or key < best[0]:
                best = (key, op)
        (start, _, _), op = best
        left.remove(op)
        now = start + (op.dur if op.link is None else 0.03)
        if op.link is None:
            done[op.name] = now + op.latency
        else:
            rate, lat = PATHS.get(op.link, (LINK_RATE, LINK_LAT))
            begin = max(now, link_free.get(op.link, 0.0))
            link_free[op.link] = begin + op.nbytes / rate
            done[op.name] = link_free[op.link] + lat
        order.append((start, op))
    return order, done


def layer_kernel(
    tok_hbm, go_hbm, gi_hbm, ci_hbm, mo_hbm, up_hbm, dn_hbm, taps, mgain, mshift, cgain, cshift,
    res,
    tok, wm, wu, wd, proj, prod, conv, pp, so, dr, rl, fr, fd, v, first, hid,
    pp1, dr1, so1, in1, cs1, val, stats, send_sems, recv_sems, load_sems,
    report=None,
):
    f32, bf16 = jnp.float32, jnp.bfloat16
    rep, fs, tp = lax.axis_index("rep"), lax.axis_index("fs"), lax.axis_index("tp")
    zl, y = lax.div(fs, NY), lax.rem(fs, NY)
    x, c = lax.div(tp, 2), lax.rem(tp, 2)
    z = rep * NZ + zl

    def mod(v, n):
        return lax.rem(v + 2 * n, n)

    def device(dz=0, dy=0, dx=0, dc=0):
        zz = mod(z + dz, 2 * NZ)
        return (
            lax.div(zz, NZ),
            lax.rem(zz, NZ) * NY + mod(y + dy, NY),
            mod(x + dx, NX) * 2 + lax.rem(c + dc, 2),
        )

    peer = {
        "z+": device(dz=1), "z-": device(dz=-1), "y+": device(dy=1), "y-": device(dy=-1),
        "x+": device(dx=1), "x-": device(dx=-1), "x2": device(dx=2), "c": device(dc=1),
    }
    sign = {"+": 1, "-": -1}

    ops = []
    sends = {}

    send_groups, recv_groups = {}, {}

    def send(name, link, deps, src, dst, landed, nbytes, prio, sent, group=None):
        send_at = send_groups.setdefault(sent[0], len(send_groups))
        recv_at = recv_groups.setdefault(group[0] if group else name, len(recv_groups))

        def copy(s, d):
            return pltpu.make_async_remote_copy(
                src_ref=s, dst_ref=d, send_sem=send_sems.at[send_at], recv_sem=recv_sems.at[recv_at],
                device_id=peer[link], device_id_type=pl.DeviceIdType.MESH,
            )

        all_here = group[1] if group else landed
        sends.setdefault(sent[0], lambda: copy(sent[1](), sent[1]()).wait_send())
        op = Op(
            name, deps, lambda: copy(src(), dst()).start(), prio,
            link="x+" if link == "x2" else link, nbytes=2 * nbytes if link == "x2" else nbytes,
            wait=lambda: copy(all_here(), all_here()).wait_recv(),
        )
        op.group = group[0] if group else None
        ops.append(op)

    def compute(name, deps, emit, prio, dur):
        ops.append(Op(name, deps, emit, prio, dur=dur))

    loads = []

    def load(name, src, dst):
        index = len(loads)
        op = Op(name, [], lambda: None, 0, latency=0.5)
        op.wait = lambda: pltpu.make_async_copy(src(), dst(), load_sems.at[index]).wait()
        loads.append(lambda: pltpu.make_async_copy(src(), dst(), load_sems.at[index]).start())
        ops.append(op)

    def own(w, c0, n):
        return lambda: w.at[zl, pl.ds(pl.multiple_of(y * ROWS, ROWS), ROWS), pl.ds(c0, n)]

    load("load.m0", lambda: go_hbm, own(wm, 0, 128))
    load("load.m1", lambda: gi_hbm, own(wm, 128, 128))
    load("load.m2", lambda: ci_hbm, own(wm, 256, 128))
    load("load.m3", lambda: mo_hbm, own(wm, 384, 128))
    load("load.u", lambda: up_hbm, own(wu, 0, 1024))
    load("load.d", lambda: dn_hbm, own(wd, 0, 1024))
    load("load.t", lambda: tok_hbm, lambda: tok)

    def block(w, dz, dy, c0, n, half=None):
        rows, off = (ROWS, 0) if half is None else (ROWS // 2, half * ROWS // 2)

        def view():
            start = pl.multiple_of(mod(y + dy, NY) * ROWS + off, ROWS // 2)
            return w.at[mod(zl + dz, NZ), pl.ds(start, rows), pl.ds(c0, n)]

        return view

    def slab(w, dz, c0, n, half=None):
        rows, off = (GROUP, 0) if half is None else (GROUP // 2, half * GROUP // 2)
        return lambda: w.at[mod(zl + dz, NZ), pl.ds(off, rows), pl.ds(c0, n)]

    ready = {}

    def y_first(tag, w, c0, n, deps, prio):
        size = ROWS * n * 2
        part_of = lambda zs, rows: (lambda: w.at[zs, rows, pl.ds(c0, n)])
        sent_y = ((tag, "Y"), part_of(0, pl.ds(0, 3 * ROWS)))
        sent_z = ((tag, "Z"), part_of(pl.ds(0, 7), pl.ds(0, GROUP)))
        second = ((tag, "Y", 2), part_of(0, pl.ds(0, ROWS)))
        fourth = ((tag, "Z", 4), part_of(0, pl.ds(0, GROUP)))
        for d in "+-":
            s = sign[d]
            b = block(w, 0, 0, c0, n)
            send((tag, "Y", 1, d), "y" + d, deps, b, b, block(w, 0, -s, c0, n), size,
                 HOPS[tag[0]]["y"][0], sent_y)
        for d, half in (("+", 0), ("-", 1)):
            s = sign[d]
            b = block(w, 0, -s, c0, n, half)
            send((tag, "Y", 2, d), "y" + d, [(tag, "Y", 1, d)], b, b, block(w, 0, -2 * s, c0, n, half), size // 2,
                 HOPS[tag[0]]["y"][1], sent_y, second)
        group = [(tag, "Y", h, d) for h in (1, 2) for d in "+-"]
        ready[tag[0], 0] = ready.get((tag[0], 0), []) + group
        for d, half in (("+", 0), ("-", 1)):
            s = sign[d]
            for h in (1, 2, 3, 4):
                part = half if h == 4 else None
                b = slab(w, -s * (h - 1), c0, n, part)
                before = deps + group if h == 1 else [(tag, "Z", h - 1, d)]
                send((tag, "Z", h, d), "z" + d, before, b, b, slab(w, -s * h, c0, n, part),
                     NY * size // (1 if part is None else 2), HOPS[tag[0]]["yz"][h - 1],
                     sent_z, fourth if h == 4 else None)
                dist = 4 if h == 4 else -s * h
                ready[tag[0], dist] = ready.get((tag[0], dist), []) + [(tag, "Z", h, d)]

    def z_first(tag, w, c0, n, deps, prio):
        size = ROWS * n * 2
        part_of = lambda zs, rows: (lambda: w.at[zs, rows, pl.ds(c0, n)])
        sent_z = part_of(0, pl.ds(0, 7 * ROWS // 2))
        sent_y = ((tag, "Y"), part_of(pl.ds(0, 6), pl.ds(0, GROUP)))
        fourth = ((tag, "Z", 4), part_of(0, pl.ds(0, ROWS)))
        for d, half in (("+", 0), ("-", 1)):
            s = sign[d]
            for h in (1, 2, 3, 4):
                part = half if h == 4 else None
                b = block(w, -s * (h - 1), 0, c0, n, part)
                before = deps if h == 1 else [(tag, "Z", h - 1, d)]
                send((tag, "Z", h, d), "z" + d, before, b, b, block(w, -s * h, 0, c0, n, part),
                     size // (1 if part is None else 2), HOPS[tag[0]]["z"][h - 1],
                     ((tag, "Z", d), sent_z), fourth if h == 4 else None)
        late = {dist: j for j, dists in enumerate(LATE) for dist in dists}
        for at, dist in enumerate(ARRIVAL):
            here = {0: deps, 4: [(tag, "Z", 4, "+"), (tag, "Z", 4, "-")]}.get(
                dist, [(tag, "Z", abs(dist), NEAR[dist > 0])])
            second = {
                "m": ((tag, "Y", 2, at), part_of(0, pl.ds(0, ROWS))),
                "u": ((tag, "Y", 2), part_of(pl.ds(0, 2), pl.ds(0, GROUP))),
                "d": ((tag, "Y", 2, late[dist]), part_of(0, pl.ds(0, ROWS * len(LATE[late[dist]])))),
            }[tag[0]]
            for d, half in (("+", 0), ("-", 1)):
                s = sign[d]
                b = block(w, dist, 0, c0, n)
                send((tag, "Y", 1, d, dist), "y" + d, here, b, b, block(w, dist, -s, c0, n), size,
                     HOPS[tag[0]]["zy"][abs(dist)], sent_y)
                b = block(w, dist, -s, c0, n, half)
                send((tag, "Y", 2, d, dist), "y" + d, [(tag, "Y", 1, d, dist)], b, b,
                     block(w, dist, -2 * s, c0, n, half), size // 2,
                     HOPS[tag[0]]["zy"][abs(dist)], sent_y, second)
            names = here + [(tag, "Y", h, d, dist) for h in (1, 2) for d in "+-"]
            ready[tag[0], dist] = ready.get((tag[0], dist), []) + names

    seen = []
    mixer_loads = ["load.m0", "load.m1", "load.m2", "load.m3"]
    column, loads_of = 0, {"m": mixer_loads, "u": ["load.u"], "d": ["load.d"]}
    for tag, way, n, prio in PIECES:
        w = {"m": wm, "u": wu, "d": wd}[tag[0]]
        if tag[0] not in [t[0] for t in seen]:
            column = 0
        seen.append(tag)
        way = y_first if way == "y" else z_first
        way(tag, w, column, n, loads_of[tag[0]], prio)
        column += n

    def project(first_one, dists):
        def emit():
            for at, dist in enumerate(dists):
                g = mod(zl + dist, NZ)
                term = jnp.dot(
                    tok[:, pl.ds(pl.multiple_of(g * GROUP, GROUP), GROUP)], wm[g, :, 0:384],
                    preferred_element_type=f32)
                if first_one and at == 0:
                    proj[...] = term
                else:
                    proj[...] += term

        return emit

    def convolve():
        prod[0:8, :] = jnp.zeros((8, 128), f32)
        prod[8:, :] = proj[:, 128:256] * proj[:, 256:384]
        total = taps[0:1, :] * prod[6:6 + SEQ, :]
        total = total + taps[1:2, :] * prod[7:7 + SEQ, :]
        total = total + taps[2:3, :] * prod[8:8 + SEQ, :]
        conv[...] = (proj[:, 0:128] * total).astype(bf16)

    compute_after = ["load.t"] + mixer_loads
    for dist in ARRIVAL:
        compute_after = compute_after + ready["m", dist]
        compute(("project", dist), compute_after, project(dist == 0, [dist]), 0, 0.35)
        compute_after = [("project", dist)]
    compute("convolve", compute_after, convolve, 0, 0.7)

    nt = (((1,), (1,)), ((), ()))

    def product(phase, p, k, left, rights):
        for at, right in enumerate(rights):
            pp[phase, p, k, :, at * GROUP:(at + 1) * GROUP] = lax.dot_general(
                left[p * PART:(p + 1) * PART, :], right(), nt, preferred_element_type=f32).astype(bf16)

    def rows_of(dx):
        return pl.ds(pl.multiple_of(mod(x + dx, NX) * OWN, OWN), OWN)

    def core_rows(core):
        return pl.ds(pl.multiple_of(core * CORE_ROWS, CORE_ROWS), CORE_ROWS)

    def seq_rows(p, dx=0, core=None):
        core = c if core is None else core
        return pl.ds(pl.multiple_of(p * PART + core * CORE_ROWS + mod(x + dx, NX) * OWN, OWN), OWN)

    def sum_chunk(phase, p, k, groups, residual, prio):
        t = ("s", phase, p, k)
        d, e = ("+", "-") if k % 2 == 0 else ("-", "+")
        s = sign[d]
        send((t, "pair"), "c", [(t, "product")], lambda: pp.at[phase, p, k, core_rows(1 - c), :],
             lambda: dr.at[phase, p, k], lambda: dr.at[phase, p, k], CORE_ROWS * CHUNK * 2, prio,
             (("s", phase, p, "pair"), lambda: dr.at[phase, p]))

        def add_pair():
            so[phase, p, k] = (
                pp[phase, p, k, core_rows(c), :].astype(f32) + dr[phase, p, k].astype(f32)).astype(bf16)

        compute((t, "add"), [(t, "product"), (t, "pair")], add_pair, prio, 0.06)
        size = OWN * CHUNK * 2
        at = lambda dx: (lambda: so.at[phase, p, k, rows_of(dx), :])
        slot = lambda ref: (lambda: ref.at[phase, p, k])
        sent = (("s", phase, p, "x"), lambda: so.at[phase, p, pl.ds(0, CHUNKS - 1)])
        last = ((t, "last"), lambda: so.at[phase, p, k, pl.ds(0, 2 * OWN), :])
        send((t, "relay"), "x" + d, [(t, "add")], at(2), slot(rl), slot(rl), size, prio, sent)
        send((t, "direct"), "x" + e, [(t, "add")], at(-s), slot(fd), slot(fd), size, prio + 0.5,
             sent, last)

        def add_relay():
            so[phase, p, k, rows_of(s), :] = (
                so[phase, p, k, rows_of(s), :].astype(f32) + rl[phase, p, k].astype(f32)).astype(bf16)

        compute((t, "radd"), [(t, "add"), (t, "relay")], add_relay, prio, 0.03)
        send((t, "final"), "x" + d, [(t, "radd")], at(s), slot(fr), slot(fr), size, prio, sent, last)

        def finish():
            total = so[phase, p, k, rows_of(0), :].astype(f32) + fr[phase, p, k].astype(f32)
            total = total + fd[phase, p, k].astype(f32)
            for at, group in enumerate(groups):
                columns = pl.ds(pl.multiple_of(group() * GROUP, GROUP), GROUP)
                v[p, :, columns] = (residual_scale * residual[seq_rows(p), columns].astype(f32)
                                    + total[:, at * GROUP:(at + 1) * GROUP])

        compute((t, "finish"), [(t, "add"), (t, "final"), (t, "direct")], finish, prio, 0.04)

    def norm(phase, p, gain, shift, dest, prio):
        def emit():
            values = v[p]
            mean = jnp.mean(values, -1, keepdims=True)
            centered = values - mean
            variance = jnp.mean(centered * centered, -1, keepdims=True)
            scaled = centered * lax.rsqrt(variance + norm_epsilon)
            dest[seq_rows(p), :] = (scaled * gain[...] + shift[...]).astype(bf16)

        compute(("norm", phase, p), [(("s", phase, p, k), "finish") for k in range(CHUNKS)], emit, prio, 0.25)

    HALF = WIDTH // 2

    def place(p, dx, h, other=False):
        def view(ref):
            rows = seq_rows(p, dx, 1 - c if other else c)
            return ref.at[rows, :] if h is None else ref.at[rows, pl.ds(h * HALF, HALF)]
        return view

    def gather(phase, p, ref, prio):
        def at(*where):
            return lambda: place(p, *where)(ref)

        t, size, landed = ("g", phase, p), OWN * HALF * 2, []
        start = [("norm", phase, p)]
        first_rows = lambda rows: (lambda: ref.at[pl.ds(0, rows), :])
        sent_x, sent_c = ((t, "x"), first_rows(3 * OWN)), ((t, "c"), first_rows(4 * OWN))
        if phase == 0:
            pairs = [((t, "P"), first_rows(4 * OWN))] * 4
        else:
            pairs = [((t, "P", i), first_rows(rows)) for i, rows in enumerate((OWN, OWN, OWN, OWN))]
        for d, first_half in (("+", 0), ("-", 1)):
            for h in (first_half, 1 - first_half):
                send((t, "A", d, h), "x" + d, start, at(0, h), at(0, h), at(-sign[d], h), size, prio, sent_x)
                landed.append(((t, "A", d, h), (-sign[d], h)))
        send((t, "P"), "c", start, at(0, None), at(0, None), at(0, None, True), 2 * size, prio, sent_c, pairs[0])
        landed.append(((t, "P"), (0, None, True)))
        for d, h in (("+", 0), ("-", 1)):
            b = at(-sign[d], h)
            send((t, "B", d), "x" + d, [(t, "A", d, h)], b, b, at(2, h), size, prio, sent_x)
            landed.append(((t, "B", d), (2, h)))
        for i, (name, dx, h) in enumerate((
                ((t, "A", "+", 0), -1, 0), ((t, "A", "-", 1), 1, 1), ((t, "A", "+", 1), -1, 1),
                ((t, "A", "-", 0), 1, 0), ((t, "B", "+"), 2, 0), ((t, "B", "-"), 2, 1))):
            send((name, "P"), "c", [name], at(dx, h), at(dx, h), at(dx, h, True), size, prio,
                 sent_c, pairs[1 + i // 2])
            landed.append(((name, "P"), (dx, h, True)))
        return landed

    def hidden(p, n):
        rows = pl.ds(p * PART, PART)
        for at in (2 * n, 2 * n + 1):
            columns = pl.ds(at * 256, 256)
            up = jnp.dot(first[rows, :], wu[:, :, columns].reshape(WIDTH, 256), preferred_element_type=f32)
            hid[rows, columns] = jnp.square(jnp.maximum(up, 0.0)).astype(bf16)

    up_ready = ["load.u"] + [n for dist in ARRIVAL for n in ready["u", dist]]
    for p in range(PARTS):
        for k in range(CHUNKS):
            pair = (2 * k, 2 * k + 1)
            compute((("s", 0, p, k), "product"), ["convolve"],
                    functools.partial(product, 0, p, k, conv, [lambda g=g: wm[g, :, 384:512] for g in pair]),
                    0 + p, 0.25)
            sum_chunk(0, p, k, [lambda g=g: g for g in pair], tok, 0 + p)
        norm(0, p, mgain, mshift, first, 0 + p)
        landed = gather(0, p, first, 0 + p)
        for n in range(2):
            compute(("hidden", p, n), [("norm", 0, p)] + [name for name, _ in landed] + up_ready,
                    functools.partial(hidden, p, n), 2 + p, 0.75)

    own_block, half_of = OWN, CORE_ROWS

    def late_rows(dx=0, core=None, rows=own_block, off=0):
        core = c if core is None else core
        start = core * half_of + mod(x + dx, NX) * own_block + off
        return pl.ds(pl.multiple_of(start, own_block // 2), rows)

    def late_half(core):
        return pl.ds(pl.multiple_of(core * half_of, half_of), half_of)

    def in_half(dx):
        return pl.ds(pl.multiple_of(mod(x + dx, NX) * own_block, own_block), own_block)

    def late_chunk(p, j, dists, direct, prio):
        t, width = ("late", p, j), GROUP * len(dists)
        wide = pl.ds(0, width)
        groups = [mod(zl + dist, NZ) for dist in dists]
        columns = [pl.ds(pl.multiple_of(g * GROUP, GROUP), GROUP) for g in groups]
        arrived = [name for dist in dists for name in ready["d", dist]]

        def multiply():
            for at, g in enumerate(groups):
                for r in range(1, -1, -1) if len(groups) == 1 else (None,):
                    size, start = (PART, 0) if r is None else (half_of, r * half_of)
                    pp1[p, j, pl.ds(start, size), at * GROUP:(at + 1) * GROUP] = lax.dot_general(
                        hid[pl.ds(p * PART + start, size), :], wd[g], nt, preferred_element_type=f32).astype(bf16)

        compute((t, "product"), [("hidden", p, n) for n in range(2)] + ["load.d"] + arrived,
                multiply, prio, 0.25 * len(dists))
        sent_x = ((t, "x"), lambda: cs1.at[p, j, pl.ds(0, 6 * own_block), wide])
        sent_c = ((t, "c"), lambda: cs1.at[p, j, :, wide])
        size = own_block * width * 2
        send((t, "pair"), "c", [(t, "product")], lambda: pp1.at[p, j, late_half(1 - c), wide],
             lambda: dr1.at[p, j, :, wide], lambda: dr1.at[p, j, :, wide], NX * size, prio, sent_c)

        def add_pair():
            so1[p, j, :, wide] = (
                pp1[p, j, late_half(c), wide].astype(f32) + dr1[p, j, :, wide].astype(f32)).astype(bf16)

        compute((t, "add"), [(t, "pair")], add_pair, prio, 0.1)
        at = lambda dx: (lambda: so1.at[p, j, in_half(dx), wide])
        slot = lambda i: (lambda: in1.at[p, j, i, :, wide])
        d, e = ("+", "-") if j % 2 == 0 else ("-", "+")
        s = sign[d]
        if direct:
            last = ((t, "last"), lambda: so1.at[p, j, pl.ds(0, 3 * own_block), wide])
            send((t, "far"), "x2", [(t, "add")], at(2), slot(0), slot(0), size, prio, sent_x, last)
            send((t, "plus"), "x+", [(t, "add")], at(1), slot(1), slot(1), size, prio, sent_x, last)
            send((t, "minus"), "x-", [(t, "add")], at(-1), slot(2), slot(2), size, prio, sent_x, last)
            terms, from_others = (0, 1, 2), [(t, "far"), (t, "plus"), (t, "minus")]
        else:
            last = ((t, "last"), lambda: so1.at[p, j, pl.ds(0, 2 * own_block), wide])
            send((t, "relay"), "x" + d, [(t, "add")], at(2), slot(0), slot(0), size, prio, sent_x)
            send((t, "direct"), "x" + e, [(t, "add")], at(-s), slot(2), slot(2), size, prio + 0.5, sent_x, last)

            def add_relay():
                so1[p, j, in_half(s), wide] = (
                    so1[p, j, in_half(s), wide].astype(f32) + in1[p, j, 0, :, wide].astype(f32)).astype(bf16)

            compute((t, "radd"), [(t, "relay")], add_relay, prio, 0.05)
            send((t, "final"), "x" + d, [(t, "radd")], at(s), slot(1), slot(1), size, prio, sent_x, last)
            terms, from_others = (1, 2), [(t, "final"), (t, "direct")]

        def finish():
            total = so1[p, j, in_half(0), wide].astype(f32)
            for i in terms:
                total = total + in1[p, j, i, :, wide].astype(f32)
            cs1[p, j, late_rows(), wide] = total.astype(bf16)

        compute((t, "finish"), from_others, finish, prio, 0.06)

        def there(*where, **more):
            return lambda: cs1.at[p, j, late_rows(*where, **more), wide]

        begin = [(t, "finish")]
        paired = ((t, "P"), lambda: cs1.at[p, j, pl.ds(0, half_of), wide])
        other = 1 - c
        send((t, "A", "+"), "x+", begin, there(0), there(0), there(-1), size, prio, sent_x)
        send((t, "A", "-"), "x-", begin, there(0), there(0), there(1), size, prio, sent_x)
        if direct:
            send((t, "A", "x2"), "x2", begin, there(0), there(0), there(2), size, prio, sent_x)
            far = [(t, "A", "x2")]
        else:
            both = ((t, "B"), there(2))
            for d, off in (("+", 0), ("-", own_block // 2)):
                piece = dict(rows=own_block // 2, off=off)
                b = there(-sign[d], **piece)
                send((t, "B", d), "x" + d, [(t, "A", d)], b, b, there(2, **piece), size // 2, prio, sent_x, both)
            far = [(t, "B", "+"), (t, "B", "-")]
        for dx, after in ((0, begin), (-1, [(t, "A", "+")]), (1, [(t, "A", "-")]), (2, far)):
            send((t, "P", dx), "c", after, there(dx), there(dx), there(dx, other), size, prio, sent_c, paired)

        def count():
            def step(i, _):
                here = pl.ds(pl.multiple_of(i * 64, 64), 64)
                rows = pl.ds(pl.multiple_of(p * PART + i * 64, 64), 64)
                shift, one, two = stats[0, rows, :], stats[1, rows, :], stats[2, rows, :]
                for at, cols in enumerate(columns):
                    value = (residual_scale * first[rows, cols].astype(f32)
                             + cs1[p, j, here, at * GROUP:(at + 1) * GROUP].astype(f32))
                    val[rows, cols] = value
                    for lanes in range(0, GROUP, 128):
                        part = value[:, lanes:lanes + 128] - shift
                        one, two = one + part, two + part * part
                stats[1, rows, :], stats[2, rows, :] = one, two
                return 0

            lax.fori_loop(0, PART // 64, step, 0)

        compute((t, "count"), begin + far + [("stats", p)] + [(t, "P", dx) for dx in (0, -1, 1, 2)],
                count, prio + 1, 0.15 * len(dists))

    def begin_stats(p):
        def emit():
            rows = pl.ds(p * PART, PART)
            shift = residual_scale * first[rows, 0:128].astype(f32)[:, 0:1]
            stats[0, rows, :] = jnp.broadcast_to(shift, (PART, 128))
            stats[1, rows, :] = jnp.zeros((PART, 128), f32)
            stats[2, rows, :] = jnp.zeros((PART, 128), f32)

        compute(("stats", p), [("hidden", p, 1)], emit, 6, 0.1)

    for p in range(PARTS):
        begin_stats(p)
        for j, dists in enumerate(LATE):
            late_chunk(p, j, dists, DIRECT[j], 2 + 0.5 * p + 0.05 * j)

    def finish_norm(p):
        def step(i, _):
            rows = pl.ds(pl.multiple_of(p * PART + i * 64, 64), 64)
            off = jnp.sum(stats[1, rows, :], -1, keepdims=True) * (1.0 / WIDTH)
            square = jnp.sum(stats[2, rows, :], -1, keepdims=True) * (1.0 / WIDTH)
            scale = lax.rsqrt(jnp.maximum(square - off * off, 0.0) + norm_epsilon)
            centered = val[rows, :] - (stats[0, rows, 0:1] + off)
            res[rows, :] = (centered * scale * cgain[...] + cshift[...]).astype(bf16)
            return 0

        lax.fori_loop(0, PART // 64, step, 0)

    for p in range(PARTS):
        compute(("finish_norm", p), [(("late", p, j), "count") for j in range(len(LATE))],
                functools.partial(finish_norm, p), 6, 1.05)

    for tag, way, _, _ in PIECES:
        for op in ops:
            if isinstance(op.name, tuple) and op.name[0] == tag:
                op.earliest = EARLIEST.get(tag[0] + way, 0.0)
    order, done = plan(ops)
    if report is not None:
        report(order, done, len(send_groups), len(recv_groups), len(loads))
    assert (len(send_groups), len(recv_groups), len(loads)) == (N_SENDS, N_RECVS, N_LOADS), (
        len(send_groups), len(recv_groups), len(loads))

    for start_load in loads:
        start_load()
    barrier = pltpu.get_barrier_semaphore()
    for link in peer:
        pl.semaphore_signal(barrier, inc=1, device_id=peer[link], device_id_type=pl.DeviceIdType.MESH)
    pl.semaphore_wait(barrier, len(peer))

    by_name = {op.name: op for op in ops}
    waited = set()

    def need(name):
        op = by_name[name]
        key = op.group or name
        if op.wait is not None and key not in waited:
            waited.add(key)
            op.wait()

    for _, op in order:
        for name in op.deps:
            need(name)
        op.emit()
    for op in ops:
        need(op.name)
    for wait in sends.values():
        wait()


N_SENDS, N_RECVS, N_LOADS = 46, 250, 7


def local(tokens, gate_outer, gate_inner, conv_input, mixer_output, conv_taps, mixer_gain,
          mixer_shift, up_weight, down_weight, channel_gain, channel_shift):
    bf16, f32 = jnp.bfloat16, jnp.float32
    vmem, hbm = pl.BlockSpec(memory_space=pltpu.VMEM), pl.BlockSpec(memory_space=pl.ANY)
    return pl.pallas_call(
        layer_kernel,
        out_shape=pltpu.VMEM((SEQ, WIDTH), bf16),
        in_specs=[hbm] * 7 + [vmem] * 5,
        out_specs=vmem,
        scratch_shapes=[
            pltpu.VMEM((SEQ, WIDTH), bf16),
            pltpu.VMEM((NZ, GROUP, 512), bf16),
            pltpu.VMEM((NZ, GROUP, 1024), bf16),
            pltpu.VMEM((NZ, GROUP, 1024), bf16),
            pltpu.VMEM((SEQ, 384), f32),
            pltpu.VMEM((SEQ + 8, 128), f32),
            pltpu.VMEM((SEQ, 128), bf16),
            pltpu.VMEM((1, PARTS, CHUNKS, PART, CHUNK), bf16),
            pltpu.VMEM((1, PARTS, CHUNKS, CORE_ROWS, CHUNK), bf16),
            pltpu.VMEM((1, PARTS, CHUNKS, CORE_ROWS, CHUNK), bf16),
            pltpu.VMEM((1, PARTS, CHUNKS, OWN, CHUNK), bf16),
            pltpu.VMEM((1, PARTS, CHUNKS, OWN, CHUNK), bf16),
            pltpu.VMEM((1, PARTS, CHUNKS, OWN, CHUNK), bf16),
            pltpu.VMEM((PARTS, OWN, WIDTH), f32),
            pltpu.VMEM((SEQ, WIDTH), bf16),
            pltpu.VMEM((SEQ, 1024), bf16),
            pltpu.VMEM((PARTS, len(LATE), PART, CHUNK), bf16),
            pltpu.VMEM((PARTS, len(LATE), CORE_ROWS, CHUNK), bf16),
            pltpu.VMEM((PARTS, len(LATE), CORE_ROWS, CHUNK), bf16),
            pltpu.VMEM((PARTS, len(LATE), 3, OWN, CHUNK), bf16),
            pltpu.VMEM((PARTS, len(LATE), PART, CHUNK), bf16),
            pltpu.VMEM((SEQ, WIDTH), f32),
            pltpu.VMEM((3, SEQ, 128), f32),
            pltpu.SemaphoreType.DMA((N_SENDS,)),
            pltpu.SemaphoreType.DMA((N_RECVS,)),
            pltpu.SemaphoreType.DMA((N_LOADS,)),
        ],
        compiler_params=pltpu.CompilerParams(
            collective_id=0, has_side_effects=True, vmem_limit_bytes=56 * 2**20),
    )(tokens, gate_outer, gate_inner, conv_input, mixer_output, up_weight, down_weight, conv_taps,
      mixer_gain.reshape(1, -1), mixer_shift.reshape(1, -1), channel_gain.reshape(1, -1),
      channel_shift.reshape(1, -1))


def solution(mesh):
    weights = P("fs", "tp")
    in_specs = (
        P(("rep", "fs"), None), weights, weights, weights, weights, P(None, "tp"), P(), P(),
        weights, weights, P(), P(),
    )
    out_specs = P(("rep", "fs"), None)
    return jax.shard_map(local, mesh=mesh, in_specs=in_specs, out_specs=out_specs, check_vma=False)
```

```python
import functools

import jax
import jax.numpy as jnp
from jax import lax
from jax.experimental import pallas as pl
from jax.experimental.pallas import tpu as pltpu
from jax.sharding import PartitionSpec as P

residual_scale = 8.0**0.25
norm_epsilon = 1e-05

NZ, NY, NX = 8, 4, 4
SEQ, WIDTH = 512, 2048
ROWS = 64
GROUP = 256
PARTS = 2
PART = SEQ // PARTS
CORE_ROWS, OWN = PART // 2, PART // 8
CHUNKS, CHUNK = 4, 512
NEAR = ("+", "-")
ARRIVAL = (0, 1, -1, 2, -2, 3, -3, 4)
LATE = ((0, 1), (-1, 2), (-2, 3), (-3, 4))
DIRECT = (False, False, False, False)

LINK_RATE, LINK_LAT = 45.0e3, 2.1
PAIR_RATE, PAIR_LAT = 400e3, 1.6
BACKLOG = 1.9
PATHS = {"c": (PAIR_RATE, PAIR_LAT), "x+": (LINK_RATE, 2.6), "x-": (LINK_RATE, 2.6)}


PIECES = (
    ("m0", "y", 128, 1),
    ("m2", "z", 384, 1),
    ("u0", "y", 128, 4),
    ("u1", "y", 256, 4),
    ("u2", "z", 384, 4),
    ("u3", "z", 256, 4),
    ("d0", "y", 256, 5),
    ("d1", "y", 256, 5),
    ("d2", "z", 512, 5),
)
HOPS = {
    "m": {"y": (0.76, 3.57), "yz": (5.4, 4.91, 3.59, 6),
          "z": (0.75, 4.7, 5.55, 2.49), "zy": (6, 4.33, 6, 3.75, 3.57)},
    "u": {"y": (3.62, 4.53), "yz": (3.69, 1.44, 4.5, 2.13),
          "z": (1.42, 1.1, 0.76, 3.22), "zy": (0.3, 0.99, 3.35, 3.91, 1.5)},
    "d": {"y": (5.22, 3.72), "yz": (6, 1.71, 5.65, 1.31),
          "z": (1.86, 2.09, 0.83, 2.25), "zy": (2.19, 0.3, 1.5, 2.04, 2.99)},
}
EARLIEST = {"uy": 3.8, "uz": 11.0, "dy": 15.3, "dz": 0.1}


class Op:
    def __init__(self, name, deps, emit, prio, dur=0.0, link=None, nbytes=0, wait=None, latency=0.0):
        self.name, self.deps, self.emit, self.prio = name, deps, emit, prio
        self.dur, self.link, self.nbytes, self.wait = dur, link, nbytes, wait
        self.latency, self.group, self.earliest = latency, None, 0.0


def plan(ops):
    done, link_free, order, now = {}, {}, [], 0.0
    members = {}
    for op in ops:
        if op.group is not None:
            members.setdefault(op.group, []).append(op.name)
    group_of = {op.name: members[op.group] for op in ops if op.group is not None}
    for op in ops:
        op.deps = list(dict.fromkeys(m for d in op.deps for m in group_of.get(d, [d])))
    left = list(ops)
    while left:
        best = None
        for at, op in enumerate(left):
            if any(d not in done for d in op.deps):
                continue
            ready = max([done[d] for d in op.deps] + [op.earliest])
            if op.link is not None:
                ready = max(ready, link_free.get(op.link, 0.0) - (BACKLOG if op.prio >= 3 else 0.94 * BACKLOG))
            key = (max(ready, now), op.prio, at)
            if best is None or key < best[0]:
                best = (key, op)
        (start, _, _), op = best
        left.remove(op)
        now = start + (op.dur if op.link is None else 0.03)
        if op.link is None:
            done[op.name] = now + op.latency
        else:
            rate, lat = PATHS.get(op.link, (LINK_RATE, LINK_LAT))
            begin = max(now, link_free.get(op.link, 0.0))
            link_free[op.link] = begin + op.nbytes / rate
            done[op.name] = link_free[op.link] + lat
        order.append((start, op))
    return order, done


def layer_kernel(
    tok_hbm, go_hbm, gi_hbm, ci_hbm, mo_hbm, up_hbm, dn_hbm, taps, mgain, mshift, cgain, cshift,
    res,
    tok, wm, wu, wd, proj, prod, conv, pp, so, dr, rl, fr, fd, v, first, hid,
    pp1, dr1, so1, in1, cs1, val, stats, send_sems, recv_sems, load_sems,
    report=None,
):
    f32, bf16 = jnp.float32, jnp.bfloat16
    rep, fs, tp = lax.axis_index("rep"), lax.axis_index("fs"), lax.axis_index("tp")
    zl, y = lax.div(fs, NY), lax.rem(fs, NY)
    x, c = lax.div(tp, 2), lax.rem(tp, 2)
    z = rep * NZ + zl

    def mod(v, n):
        return lax.rem(v + 2 * n, n)

    def device(dz=0, dy=0, dx=0, dc=0):
        zz = mod(z + dz, 2 * NZ)
        return (
            lax.div(zz, NZ),
            lax.rem(zz, NZ) * NY + mod(y + dy, NY),
            mod(x + dx, NX) * 2 + lax.rem(c + dc, 2),
        )

    peer = {
        "z+": device(dz=1), "z-": device(dz=-1), "y+": device(dy=1), "y-": device(dy=-1),
        "x+": device(dx=1), "x-": device(dx=-1), "c": device(dc=1),
    }
    if any(DIRECT):
        peer["x2"] = device(dx=2)
    sign = {"+": 1, "-": -1}

    ops = []
    sends = {}

    send_groups, recv_groups = {}, {}

    def send(name, link, deps, src, dst, landed, nbytes, prio, sent, group=None):
        send_at = send_groups.setdefault(sent[0], len(send_groups))
        recv_at = recv_groups.setdefault(group[0] if group else name, len(recv_groups))

        def copy(s, d):
            return pltpu.make_async_remote_copy(
                src_ref=s, dst_ref=d, send_sem=send_sems.at[send_at], recv_sem=recv_sems.at[recv_at],
                device_id=peer[link], device_id_type=pl.DeviceIdType.MESH,
            )

        all_here = group[1] if group else landed
        sends.setdefault(sent[0], lambda: copy(sent[1](), sent[1]()).wait_send())
        op = Op(
            name, deps, lambda: copy(src(), dst()).start(), prio,
            link="x+" if link == "x2" else link, nbytes=2 * nbytes if link == "x2" else nbytes,
            wait=lambda: copy(all_here(), all_here()).wait_recv(),
        )
        op.group = group[0] if group else None
        ops.append(op)

    def compute(name, deps, emit, prio, dur):
        ops.append(Op(name, deps, emit, prio, dur=dur))

    loads = []

    def load(name, src, dst):
        index = len(loads)
        op = Op(name, [], lambda: None, 0, latency=0.5)
        op.wait = lambda: pltpu.make_async_copy(src(), dst(), load_sems.at[index]).wait()
        loads.append(lambda: pltpu.make_async_copy(src(), dst(), load_sems.at[index]).start())
        ops.append(op)

    def own(w, c0, n):
        return lambda: w.at[zl, pl.ds(pl.multiple_of(y * ROWS, ROWS), ROWS), pl.ds(c0, n)]

    load("load.m0", lambda: go_hbm, own(wm, 0, 128))
    load("load.m1", lambda: gi_hbm, own(wm, 128, 128))
    load("load.m2", lambda: ci_hbm, own(wm, 256, 128))
    load("load.m3", lambda: mo_hbm, own(wm, 384, 128))
    load("load.u", lambda: up_hbm, own(wu, 0, 1024))
    load("load.d", lambda: dn_hbm, own(wd, 0, 1024))
    load("load.t", lambda: tok_hbm, lambda: tok)

    def block(w, dz, dy, c0, n, half=None):
        rows, off = (ROWS, 0) if half is None else (ROWS // 2, half * ROWS // 2)

        def view():
            start = pl.multiple_of(mod(y + dy, NY) * ROWS + off, ROWS // 2)
            return w.at[mod(zl + dz, NZ), pl.ds(start, rows), pl.ds(c0, n)]

        return view

    def slab(w, dz, c0, n, half=None):
        rows, off = (GROUP, 0) if half is None else (GROUP // 2, half * GROUP // 2)
        return lambda: w.at[mod(zl + dz, NZ), pl.ds(off, rows), pl.ds(c0, n)]

    ready = {}

    def y_first(tag, w, c0, n, deps, prio):
        size = ROWS * n * 2
        part_of = lambda zs, rows: (lambda: w.at[zs, rows, pl.ds(c0, n)])
        sent_y = ((tag, "Y"), part_of(0, pl.ds(0, 3 * ROWS)))
        sent_z = ((tag, "Z"), part_of(pl.ds(0, 7), pl.ds(0, GROUP)))
        second = ((tag, "Y", 2), part_of(0, pl.ds(0, ROWS)))
        fourth = ((tag, "Z", 4), part_of(0, pl.ds(0, GROUP)))
        for d in "+-":
            s = sign[d]
            b = block(w, 0, 0, c0, n)
            send((tag, "Y", 1, d), "y" + d, deps, b, b, block(w, 0, -s, c0, n), size,
                 HOPS[tag[0]]["y"][0], sent_y)
        for d, half in (("+", 0), ("-", 1)):
            s = sign[d]
            b = block(w, 0, -s, c0, n, half)
            send((tag, "Y", 2, d), "y" + d, [(tag, "Y", 1, d)], b, b, block(w, 0, -2 * s, c0, n, half), size // 2,
                 HOPS[tag[0]]["y"][1], sent_y, second)
        group = [(tag, "Y", h, d) for h in (1, 2) for d in "+-"]
        ready[tag[0], 0] = ready.get((tag[0], 0), []) + group
        for d, half in (("+", 0), ("-", 1)):
            s = sign[d]
            for h in (1, 2, 3, 4):
                part = half if h == 4 else None
                b = slab(w, -s * (h - 1), c0, n, part)
                before = deps + group if h == 1 else [(tag, "Z", h - 1, d)]
                send((tag, "Z", h, d), "z" + d, before, b, b, slab(w, -s * h, c0, n, part),
                     NY * size // (1 if part is None else 2), HOPS[tag[0]]["yz"][h - 1],
                     sent_z, fourth if h == 4 else None)
                dist = 4 if h == 4 else -s * h
                ready[tag[0], dist] = ready.get((tag[0], dist), []) + [(tag, "Z", h, d)]

    def z_first(tag, w, c0, n, deps, prio):
        size = ROWS * n * 2
        part_of = lambda zs, rows: (lambda: w.at[zs, rows, pl.ds(c0, n)])
        sent_z = part_of(0, pl.ds(0, 7 * ROWS // 2))
        sent_y = ((tag, "Y"), part_of(pl.ds(0, 6), pl.ds(0, GROUP)))
        fourth = ((tag, "Z", 4), part_of(0, pl.ds(0, ROWS)))
        for d, half in (("+", 0), ("-", 1)):
            s = sign[d]
            for h in (1, 2, 3, 4):
                part = half if h == 4 else None
                b = block(w, -s * (h - 1), 0, c0, n, part)
                before = deps if h == 1 else [(tag, "Z", h - 1, d)]
                send((tag, "Z", h, d), "z" + d, before, b, b, block(w, -s * h, 0, c0, n, part),
                     size // (1 if part is None else 2), HOPS[tag[0]]["z"][h - 1],
                     ((tag, "Z", d), sent_z), fourth if h == 4 else None)
        late = {dist: j for j, dists in enumerate(LATE) for dist in dists}
        for at, dist in enumerate(ARRIVAL):
            here = {0: deps, 4: [(tag, "Z", 4, "+"), (tag, "Z", 4, "-")]}.get(
                dist, [(tag, "Z", abs(dist), NEAR[dist > 0])])
            second = {
                "m": ((tag, "Y", 2, at), part_of(0, pl.ds(0, ROWS))),
                "u": ((tag, "Y", 2), part_of(pl.ds(0, 2), pl.ds(0, GROUP))),
                "d": ((tag, "Y", 2, late[dist]), part_of(0, pl.ds(0, ROWS * len(LATE[late[dist]])))),
            }[tag[0]]
            for d, half in (("+", 0), ("-", 1)):
                s = sign[d]
                b = block(w, dist, 0, c0, n)
                send((tag, "Y", 1, d, dist), "y" + d, here, b, b, block(w, dist, -s, c0, n), size,
                     HOPS[tag[0]]["zy"][abs(dist)], sent_y)
                b = block(w, dist, -s, c0, n, half)
                send((tag, "Y", 2, d, dist), "y" + d, [(tag, "Y", 1, d, dist)], b, b,
                     block(w, dist, -2 * s, c0, n, half), size // 2,
                     HOPS[tag[0]]["zy"][abs(dist)], sent_y, second)
            names = here + [(tag, "Y", h, d, dist) for h in (1, 2) for d in "+-"]
            ready[tag[0], dist] = ready.get((tag[0], dist), []) + names

    seen = []
    mixer_loads = ["load.m0", "load.m1", "load.m2", "load.m3"]
    column, loads_of = 0, {"m": mixer_loads, "u": ["load.u"], "d": ["load.d"]}
    for tag, way, n, prio in PIECES:
        w = {"m": wm, "u": wu, "d": wd}[tag[0]]
        if tag[0] not in [t[0] for t in seen]:
            column = 0
        seen.append(tag)
        way = y_first if way == "y" else z_first
        way(tag, w, column, n, loads_of[tag[0]], prio)
        column += n

    def project(first_one, dists):
        def emit():
            for at, dist in enumerate(dists):
                g = mod(zl + dist, NZ)
                term = jnp.dot(
                    tok[:, pl.ds(pl.multiple_of(g * GROUP, GROUP), GROUP)], wm[g, :, 0:384],
                    preferred_element_type=f32)
                if first_one and at == 0:
                    proj[...] = term
                else:
                    proj[...] += term

        return emit

    def convolve():
        prod[0:8, :] = jnp.zeros((8, 128), f32)
        prod[8:, :] = proj[:, 128:256] * proj[:, 256:384]
        total = taps[0:1, :] * prod[6:6 + SEQ, :]
        total = total + taps[1:2, :] * prod[7:7 + SEQ, :]
        total = total + taps[2:3, :] * prod[8:8 + SEQ, :]
        conv[...] = (proj[:, 0:128] * total).astype(bf16)

    compute_after = ["load.t"] + mixer_loads
    for dist in ARRIVAL:
        compute_after = compute_after + ready["m", dist]
        compute(("project", dist), compute_after, project(dist == 0, [dist]), 0, 0.35)
        compute_after = [("project", dist)]
    compute("convolve", compute_after, convolve, 0, 0.7)

    nt = (((1,), (1,)), ((), ()))

    def product(phase, p, k, left, rights):
        for at, right in enumerate(rights):
            pp[phase, p, k, :, at * GROUP:(at + 1) * GROUP] = lax.dot_general(
                left[p * PART:(p + 1) * PART, :], right(), nt, preferred_element_type=f32).astype(bf16)

    def rows_of(dx):
        return pl.ds(pl.multiple_of(mod(x + dx, NX) * OWN, OWN), OWN)

    def core_rows(core):
        return pl.ds(pl.multiple_of(core * CORE_ROWS, CORE_ROWS), CORE_ROWS)

    def seq_rows(p, dx=0, core=None):
        core = c if core is None else core
        return pl.ds(pl.multiple_of(p * PART + core * CORE_ROWS + mod(x + dx, NX) * OWN, OWN), OWN)

    def sum_chunk(phase, p, k, groups, residual, prio):
        t = ("s", phase, p, k)
        d, e = ("+", "-") if k % 2 == 0 else ("-", "+")
        s = sign[d]
        send((t, "pair"), "c", [(t, "product")], lambda: pp.at[phase, p, k, core_rows(1 - c), :],
             lambda: dr.at[phase, p, k], lambda: dr.at[phase, p, k], CORE_ROWS * CHUNK * 2, prio,
             (("s", phase, p, "pair"), lambda: dr.at[phase, p]))

        def add_pair():
            so[phase, p, k] = (
                pp[phase, p, k, core_rows(c), :].astype(f32) + dr[phase, p, k].astype(f32)).astype(bf16)

        compute((t, "add"), [(t, "product"), (t, "pair")], add_pair, prio, 0.06)
        size = OWN * CHUNK * 2
        at = lambda dx: (lambda: so.at[phase, p, k, rows_of(dx), :])
        slot = lambda ref: (lambda: ref.at[phase, p, k])
        sent = (("s", phase, p, "x"), lambda: so.at[phase, p, pl.ds(0, CHUNKS - 1)])
        last = ((t, "last"), lambda: so.at[phase, p, k, pl.ds(0, 2 * OWN), :])
        send((t, "relay"), "x" + d, [(t, "add")], at(2), slot(rl), slot(rl), size, prio, sent)
        send((t, "direct"), "x" + e, [(t, "add")], at(-s), slot(fd), slot(fd), size, prio + 0.5,
             sent, last)

        def add_relay():
            so[phase, p, k, rows_of(s), :] = (
                so[phase, p, k, rows_of(s), :].astype(f32) + rl[phase, p, k].astype(f32)).astype(bf16)

        compute((t, "radd"), [(t, "add"), (t, "relay")], add_relay, prio, 0.03)
        send((t, "final"), "x" + d, [(t, "radd")], at(s), slot(fr), slot(fr), size, prio, sent, last)

        def finish():
            total = so[phase, p, k, rows_of(0), :].astype(f32) + fr[phase, p, k].astype(f32)
            total = total + fd[phase, p, k].astype(f32)
            for at, group in enumerate(groups):
                columns = pl.ds(pl.multiple_of(group() * GROUP, GROUP), GROUP)
                v[p, :, columns] = (residual_scale * residual[seq_rows(p), columns].astype(f32)
                                    + total[:, at * GROUP:(at + 1) * GROUP])

        compute((t, "finish"), [(t, "add"), (t, "final"), (t, "direct")], finish, prio, 0.04)

    def norm(phase, p, gain, shift, dest, prio):
        def emit():
            values = v[p]
            mean = jnp.mean(values, -1, keepdims=True)
            centered = values - mean
            variance = jnp.mean(centered * centered, -1, keepdims=True)
            scaled = centered * lax.rsqrt(variance + norm_epsilon)
            dest[seq_rows(p), :] = (scaled * gain[...] + shift[...]).astype(bf16)

        compute(("norm", phase, p), [(("s", phase, p, k), "finish") for k in range(CHUNKS)], emit, prio, 0.25)

    HALF = WIDTH // 2

    def place(p, dx, h, other=False):
        def view(ref):
            rows = seq_rows(p, dx, 1 - c if other else c)
            return ref.at[rows, :] if h is None else ref.at[rows, pl.ds(h * HALF, HALF)]
        return view

    def gather(phase, p, ref, prio):
        def at(*where):
            return lambda: place(p, *where)(ref)

        t, size, landed = ("g", phase, p), OWN * HALF * 2, []
        start = [("norm", phase, p)]
        first_rows = lambda rows: (lambda: ref.at[pl.ds(0, rows), :])
        sent_x, sent_c = ((t, "x"), first_rows(3 * OWN)), ((t, "c"), first_rows(4 * OWN))
        if phase == 0:
            pairs = [((t, "P"), first_rows(4 * OWN))] * 4
        else:
            pairs = [((t, "P", i), first_rows(rows)) for i, rows in enumerate((OWN, OWN, OWN, OWN))]
        for d, first_half in (("+", 0), ("-", 1)):
            for h in (first_half, 1 - first_half):
                send((t, "A", d, h), "x" + d, start, at(0, h), at(0, h), at(-sign[d], h), size, prio, sent_x)
                landed.append(((t, "A", d, h), (-sign[d], h)))
        send((t, "P"), "c", start, at(0, None), at(0, None), at(0, None, True), 2 * size, prio, sent_c, pairs[0])
        landed.append(((t, "P"), (0, None, True)))
        for d, h in (("+", 0), ("-", 1)):
            b = at(-sign[d], h)
            send((t, "B", d), "x" + d, [(t, "A", d, h)], b, b, at(2, h), size, prio, sent_x)
            landed.append(((t, "B", d), (2, h)))
        for i, (name, dx, h) in enumerate((
                ((t, "A", "+", 0), -1, 0), ((t, "A", "-", 1), 1, 1), ((t, "A", "+", 1), -1, 1),
                ((t, "A", "-", 0), 1, 0), ((t, "B", "+"), 2, 0), ((t, "B", "-"), 2, 1))):
            send((name, "P"), "c", [name], at(dx, h), at(dx, h), at(dx, h, True), size, prio,
                 sent_c, pairs[1 + i // 2])
            landed.append(((name, "P"), (dx, h, True)))
        return landed

    def hidden(p, n):
        rows = pl.ds(p * PART, PART)
        for at in (2 * n, 2 * n + 1):
            columns = pl.ds(at * 256, 256)
            up = jnp.dot(first[rows, :], wu[:, :, columns].reshape(WIDTH, 256), preferred_element_type=f32)
            hid[rows, columns] = jnp.square(jnp.maximum(up, 0.0)).astype(bf16)

    up_ready = ["load.u"] + [n for dist in ARRIVAL for n in ready["u", dist]]
    for p in range(PARTS):
        for k in range(CHUNKS):
            pair = (2 * k, 2 * k + 1)
            compute((("s", 0, p, k), "product"), ["convolve"],
                    functools.partial(product, 0, p, k, conv, [lambda g=g: wm[g, :, 384:512] for g in pair]),
                    0 + p, 0.25)
            sum_chunk(0, p, k, [lambda g=g: g for g in pair], tok, 0 + p)
        norm(0, p, mgain, mshift, first, 0 + p)
        landed = gather(0, p, first, 0 + p)
        for n in range(2):
            compute(("hidden", p, n), [("norm", 0, p)] + [name for name, _ in landed] + up_ready,
                    functools.partial(hidden, p, n), 2 + p, 0.75)

    own_block, half_of = OWN, CORE_ROWS

    def late_rows(dx=0, core=None, rows=own_block, off=0):
        core = c if core is None else core
        start = core * half_of + mod(x + dx, NX) * own_block + off
        return pl.ds(pl.multiple_of(start, own_block // 2), rows)

    def late_half(core):
        return pl.ds(pl.multiple_of(core * half_of, half_of), half_of)

    def in_half(dx):
        return pl.ds(pl.multiple_of(mod(x + dx, NX) * own_block, own_block), own_block)

    def late_chunk(p, j, dists, direct, prio):
        t, width = ("late", p, j), GROUP * len(dists)
        wide = pl.ds(0, width)
        groups = [mod(zl + dist, NZ) for dist in dists]
        columns = [pl.ds(pl.multiple_of(g * GROUP, GROUP), GROUP) for g in groups]
        arrived = [name for dist in dists for name in ready["d", dist]]

        def multiply():
            for at, g in enumerate(groups):
                for r in range(1, -1, -1) if len(groups) == 1 else (None,):
                    size, start = (PART, 0) if r is None else (half_of, r * half_of)
                    pp1[p, j, pl.ds(start, size), at * GROUP:(at + 1) * GROUP] = lax.dot_general(
                        hid[pl.ds(p * PART + start, size), :], wd[g], nt, preferred_element_type=f32).astype(bf16)

        compute((t, "product"), [("hidden", p, n) for n in range(2)] + ["load.d"] + arrived,
                multiply, prio, 0.25 * len(dists))
        sent_x = ((t, "x"), lambda: cs1.at[p, j, pl.ds(0, 6 * own_block), wide])
        sent_c = ((t, "c"), lambda: cs1.at[p, j, :, wide])
        size = own_block * width * 2
        send((t, "pair"), "c", [(t, "product")], lambda: pp1.at[p, j, late_half(1 - c), wide],
             lambda: dr1.at[p, j, :, wide], lambda: dr1.at[p, j, :, wide], NX * size, prio, sent_c)

        def add_pair():
            so1[p, j, :, wide] = (
                pp1[p, j, late_half(c), wide].astype(f32) + dr1[p, j, :, wide].astype(f32)).astype(bf16)

        compute((t, "add"), [(t, "pair")], add_pair, prio, 0.1)
        at = lambda dx: (lambda: so1.at[p, j, in_half(dx), wide])
        slot = lambda i: (lambda: in1.at[p, j, i, :, wide])
        d, e = ("+", "-") if j % 2 == 0 else ("-", "+")
        s = sign[d]
        if direct:
            last = ((t, "last"), lambda: so1.at[p, j, pl.ds(0, 3 * own_block), wide])
            send((t, "far"), "x2", [(t, "add")], at(2), slot(0), slot(0), size, prio, sent_x, last)
            send((t, "plus"), "x+", [(t, "add")], at(1), slot(1), slot(1), size, prio, sent_x, last)
            send((t, "minus"), "x-", [(t, "add")], at(-1), slot(2), slot(2), size, prio, sent_x, last)
            terms, from_others = (0, 1, 2), [(t, "far"), (t, "plus"), (t, "minus")]
        else:
            last = ((t, "last"), lambda: so1.at[p, j, pl.ds(0, 2 * own_block), wide])
            send((t, "relay"), "x" + d, [(t, "add")], at(2), slot(0), slot(0), size, prio, sent_x)
            send((t, "direct"), "x" + e, [(t, "add")], at(-s), slot(2), slot(2), size, prio + 0.5, sent_x, last)

            def add_relay():
                so1[p, j, in_half(s), wide] = (
                    so1[p, j, in_half(s), wide].astype(f32) + in1[p, j, 0, :, wide].astype(f32)).astype(bf16)

            compute((t, "radd"), [(t, "relay")], add_relay, prio, 0.05)
            send((t, "final"), "x" + d, [(t, "radd")], at(s), slot(1), slot(1), size, prio, sent_x, last)
            terms, from_others = (1, 2), [(t, "final"), (t, "direct")]

        def finish():
            total = so1[p, j, in_half(0), wide].astype(f32)
            for i in terms:
                total = total + in1[p, j, i, :, wide].astype(f32)
            cs1[p, j, late_rows(), wide] = total.astype(bf16)

        compute((t, "finish"), from_others, finish, prio, 0.06)

        def there(*where, **more):
            return lambda: cs1.at[p, j, late_rows(*where, **more), wide]

        begin = [(t, "finish")]
        paired = ((t, "P"), lambda: cs1.at[p, j, pl.ds(0, half_of), wide])
        other = 1 - c
        send((t, "A", "+"), "x+", begin, there(0), there(0), there(-1), size, prio, sent_x)
        send((t, "A", "-"), "x-", begin, there(0), there(0), there(1), size, prio, sent_x)
        if direct:
            send((t, "A", "x2"), "x2", begin, there(0), there(0), there(2), size, prio, sent_x)
            far = [(t, "A", "x2")]
        else:
            both = ((t, "B"), there(2))
            for d, off in (("+", 0), ("-", own_block // 2)):
                piece = dict(rows=own_block // 2, off=off)
                b = there(-sign[d], **piece)
                send((t, "B", d), "x" + d, [(t, "A", d)], b, b, there(2, **piece), size // 2, prio, sent_x, both)
            far = [(t, "B", "+"), (t, "B", "-")]
        for dx, after in ((0, begin), (-1, [(t, "A", "+")]), (1, [(t, "A", "-")]), (2, far)):
            send((t, "P", dx), "c", after, there(dx), there(dx), there(dx, other), size, prio, sent_c, paired)

        def count():
            def step(i, _):
                here = pl.ds(pl.multiple_of(i * 64, 64), 64)
                rows = pl.ds(pl.multiple_of(p * PART + i * 64, 64), 64)
                shift, one, two = stats[0, rows, :], stats[1, rows, :], stats[2, rows, :]
                for at, cols in enumerate(columns):
                    value = (residual_scale * first[rows, cols].astype(f32)
                             + cs1[p, j, here, at * GROUP:(at + 1) * GROUP].astype(f32))
                    val[rows, cols] = value
                    for lanes in range(0, GROUP, 128):
                        part = value[:, lanes:lanes + 128] - shift
                        one, two = one + part, two + part * part
                stats[1, rows, :], stats[2, rows, :] = one, two
                return 0

            lax.fori_loop(0, PART // 64, step, 0)

        compute((t, "count"), begin + far + [("stats", p)] + [(t, "P", dx) for dx in (0, -1, 1, 2)],
                count, prio + 1, 0.15 * len(dists))

    def begin_stats(p):
        def emit():
            rows = pl.ds(p * PART, PART)
            shift = residual_scale * first[rows, 0:128].astype(f32)[:, 0:1]
            stats[0, rows, :] = jnp.broadcast_to(shift, (PART, 128))
            stats[1, rows, :] = jnp.zeros((PART, 128), f32)
            stats[2, rows, :] = jnp.zeros((PART, 128), f32)

        compute(("stats", p), [("hidden", p, 1)], emit, 6, 0.1)

    for p in range(PARTS):
        begin_stats(p)
        for j, dists in enumerate(LATE):
            late_chunk(p, j, dists, DIRECT[j], 2 + 0.5 * p + 0.05 * j)

    def finish_norm(p):
        def step(i, _):
            rows = pl.ds(pl.multiple_of(p * PART + i * 64, 64), 64)
            off = jnp.sum(stats[1, rows, :], -1, keepdims=True) * (1.0 / WIDTH)
            square = jnp.sum(stats[2, rows, :], -1, keepdims=True) * (1.0 / WIDTH)
            scale = lax.rsqrt(jnp.maximum(square - off * off, 0.0) + norm_epsilon)
            centered = val[rows, :] - (stats[0, rows, 0:1] + off)
            res[rows, :] = (centered * scale * cgain[...] + cshift[...]).astype(bf16)
            return 0

        lax.fori_loop(0, PART // 64, step, 0)

    for p in range(PARTS):
        compute(("finish_norm", p), [(("late", p, j), "count") for j in range(len(LATE))],
                functools.partial(finish_norm, p), 6, 1.05)

    for tag, way, _, _ in PIECES:
        for op in ops:
            if isinstance(op.name, tuple) and op.name[0] == tag:
                op.earliest = EARLIEST.get(tag[0] + way, 0.0)
    order, done = plan(ops)
    if report is not None:
        report(order, done, len(send_groups), len(recv_groups), len(loads))
    assert (len(send_groups), len(recv_groups), len(loads)) == (N_SENDS, N_RECVS, N_LOADS), (
        len(send_groups), len(recv_groups), len(loads))

    for start_load in loads:
        start_load()
    barrier = pltpu.get_barrier_semaphore()
    for link in peer:
        pl.semaphore_signal(barrier, inc=1, device_id=peer[link], device_id_type=pl.DeviceIdType.MESH)
    pl.semaphore_wait(barrier, len(peer))

    by_name = {op.name: op for op in ops}
    waited = set()

    def need(name):
        op = by_name[name]
        key = op.group or name
        if op.wait is not None and key not in waited:
            waited.add(key)
            op.wait()

    for _, op in order:
        for name in op.deps:
            need(name)
        op.emit()
    for op in ops:
        need(op.name)
    for wait in sends.values():
        wait()


N_SENDS, N_RECVS, N_LOADS = 46, 250, 7


def local(tokens, gate_outer, gate_inner, conv_input, mixer_output, conv_taps, mixer_gain,
          mixer_shift, up_weight, down_weight, channel_gain, channel_shift):
    bf16, f32 = jnp.bfloat16, jnp.float32
    vmem, hbm = pl.BlockSpec(memory_space=pltpu.VMEM), pl.BlockSpec(memory_space=pl.ANY)
    return pl.pallas_call(
        layer_kernel,
        out_shape=pltpu.VMEM((SEQ, WIDTH), bf16),
        in_specs=[hbm] * 7 + [vmem] * 5,
        out_specs=vmem,
        scratch_shapes=[
            pltpu.VMEM((SEQ, WIDTH), bf16),
            pltpu.VMEM((NZ, GROUP, 512), bf16),
            pltpu.VMEM((NZ, GROUP, 1024), bf16),
            pltpu.VMEM((NZ, GROUP, 1024), bf16),
            pltpu.VMEM((SEQ, 384), f32),
            pltpu.VMEM((SEQ + 8, 128), f32),
            pltpu.VMEM((SEQ, 128), bf16),
            pltpu.VMEM((1, PARTS, CHUNKS, PART, CHUNK), bf16),
            pltpu.VMEM((1, PARTS, CHUNKS, CORE_ROWS, CHUNK), bf16),
            pltpu.VMEM((1, PARTS, CHUNKS, CORE_ROWS, CHUNK), bf16),
            pltpu.VMEM((1, PARTS, CHUNKS, OWN, CHUNK), bf16),
            pltpu.VMEM((1, PARTS, CHUNKS, OWN, CHUNK), bf16),
            pltpu.VMEM((1, PARTS, CHUNKS, OWN, CHUNK), bf16),
            pltpu.VMEM((PARTS, OWN, WIDTH), f32),
            pltpu.VMEM((SEQ, WIDTH), bf16),
            pltpu.VMEM((SEQ, 1024), bf16),
            pltpu.VMEM((PARTS, len(LATE), PART, CHUNK), bf16),
            pltpu.VMEM((PARTS, len(LATE), CORE_ROWS, CHUNK), bf16),
            pltpu.VMEM((PARTS, len(LATE), CORE_ROWS, CHUNK), bf16),
            pltpu.VMEM((PARTS, len(LATE), 3, OWN, CHUNK), bf16),
            pltpu.VMEM((PARTS, len(LATE), PART, CHUNK), bf16),
            pltpu.VMEM((SEQ, WIDTH), f32),
            pltpu.VMEM((3, SEQ, 128), f32),
            pltpu.SemaphoreType.DMA((N_SENDS,)),
            pltpu.SemaphoreType.DMA((N_RECVS,)),
            pltpu.SemaphoreType.DMA((N_LOADS,)),
        ],
        compiler_params=pltpu.CompilerParams(
            collective_id=0, has_side_effects=True, vmem_limit_bytes=56 * 2**20),
    )(tokens, gate_outer, gate_inner, conv_input, mixer_output, up_weight, down_weight, conv_taps,
      mixer_gain.reshape(1, -1), mixer_shift.reshape(1, -1), channel_gain.reshape(1, -1),
      channel_shift.reshape(1, -1))


def solution(mesh):
    weights = P("fs", "tp")
    in_specs = (
        P(("rep", "fs"), None), weights, weights, weights, weights, P(None, "tp"), P(), P(),
        weights, weights, P(), P(),
    )
    out_specs = P(("rep", "fs"), None)
    return jax.shard_map(local, mesh=mesh, in_specs=in_specs, out_specs=out_specs, check_vma=False)
```
